128 devices in a mesh: sp: 32 (over z, y, core), tp: 4 (over x).
Axes of the slice: x: 4, y: 4, z: 4, core: 2. Of those that a mesh axis runs over, the one named last changes fastest.
Arguments:
- residual: bfloat16 [32768, 2048], P('sp'), may hold values from -6 to 6
- small_heads: bfloat16 [32768, 1024], P('sp', 'tp'), may hold values from -6 to 6
- large_heads: bfloat16 [32768, 1024], P('sp', 'tp'), may hold values from -6 to 6
- state_keys: bfloat16 [32768, 8, 128], P('sp', 'tp'), may hold values from -6 to 6
- state_queries: bfloat16 [32768, 8, 128], P('sp', 'tp'), may hold values from -6 to 6
- small_gate: bfloat16 [32768, 1024], P('sp', 'tp'), may hold values from -6 to 6
- large_gate: bfloat16 [32768, 1024], P('sp', 'tp'), may hold values from -6 to 6
- small_step: float32 [32768, 16], P('sp', 'tp'), may hold values from -3 to 2
- large_step: float32 [32768, 8], P('sp', 'tp'), may hold values from -3 to 2
- small_taps: bfloat16 [4, 1024], P(None, 'tp'), may hold values from -3 to 3
- large_taps: bfloat16 [4, 1024], P(None, 'tp'), may hold values from -3 to 3
- key_taps: bfloat16 [4, 8, 128], P(None, 'tp'), may hold values from -3 to 3
- query_taps: bfloat16 [4, 8, 128], P(None, 'tp'), may hold values from -3 to 3
- small_decay: float32 [16], P('tp'), may hold values from -12 to -2, as said below
- large_decay: float32 [8], P('tp'), may hold values from -12 to -2, as said below
- small_gain: bfloat16 [1024], P('tp'), may hold values from 0.099609375 to 1.8984375
- large_gain: bfloat16 [1024], P('tp'), may hold values from 0.099609375 to 1.8984375
- small_out: bfloat16 [1024, 2048], P('tp'), may hold values from -0.125 to 0.125
- large_out: bfloat16 [1024, 2048], P('tp'), may hold values from -0.125 to 0.125
- mixer_gain: bfloat16 [2048], replicated, may hold values from 0.099609375 to 1.8984375
- ffn_in_gain: bfloat16 [2048], replicated, may hold values from 0.099609375 to 1.8984375
- gate_proj: bfloat16 [2048, 5632], P('sp', 'tp'), may hold values from -0.125 to 0.125
- up_proj: bfloat16 [2048, 5632], P('sp', 'tp'), may hold values from -0.125 to 0.125
- down_proj: bfloat16 [2048, 5632], P('sp', 'tp'), may hold values from -0.078125 to 0.078125
- ffn_out_gain: bfloat16 [2048], replicated, may hold values from 0.099609375 to 1.8984375
Outputs:
- updated: bfloat16 [32768, 2048], P(('sp', 'tp'))
The draws below stay inside these ranges and needn't reach their ends.
Inputs may be any that keep to these rules, and one draw needn't show every extreme that they name: `small_decay`: log decay rates of the first group. `large_decay`: log decay rates of the second group.
All inputs are finite; a program needn't handle non-finite values.
Results may differ from the reference program's by a relative error of at most 0.014.
Values may be sent and summed in bfloat16 or wider, within the bound.
A program may use at most 192 MiB of HBM per device.

```python
import jax
import jax.numpy as jnp
from jax import lax

D = 2048
FF = 5632
HA = 16
PA = 64
HB = 8
PB = 128
GROUPS = 8
STATE = 128
CONV = 4
BLOCK = 128
TOK_DEV = 1024
TOKENS = 32768
HEAD_BLOCKS = 4


def step_law(key, heads, salt):
    rows = jnp.arange(TOKENS, dtype=jnp.int32) // TOK_DEV
    offset_key = jax.random.fold_in(key, 101)
    jitter_key = jax.random.fold_in(key, salt)
    offsets = jax.random.uniform(offset_key, (TOKENS // TOK_DEV,), jnp.float32, -1.5, 0.5)
    jitter = jnp.clip(0.5 * jax.random.normal(jitter_key, (TOKENS, heads), jnp.float32), -1.5, 1.5)
    return offsets[rows][:, None] + jitter


def decay_law(key, heads, salt):
    base_key = jax.random.fold_in(key, salt)
    order_key, slow_key, fast_key = jax.random.split(base_key, 3)
    fast_count = heads // 2
    ranks = jax.random.permutation(order_key, heads)
    slow_values = jnp.log(jax.random.uniform(slow_key, (heads,), jnp.float32, 0.25, 1.5) / TOKENS)
    fast_values = jnp.log(jax.random.uniform(fast_key, (heads,), jnp.float32, 1.0 / 60.0, 1.0 / 20.0))
    return jnp.where(ranks < fast_count, fast_values, slow_values)


def draw_small_step(key, part):
    return step_law(key, HA, 11)


def draw_large_step(key, part):
    return step_law(key, HB, 12)


def draw_small_decay(key, part):
    return decay_law(key, HA, 21)


def draw_large_decay(key, part):
    return decay_law(key, HB, 22)


def shard_levels(rng, shape, pieces, low, top_value):
    def one(position, parts):
        draws = jax.random.uniform(jax.random.fold_in(jax.random.fold_in(rng, 6), position), (parts,), jnp.float32, low / len(pieces), top_value / len(pieces))
        return jnp.repeat(jnp.exp(draws), shape[position] // parts).reshape((-1,) + (1,) * (len(shape) - position - 1))

    loudness = one(*pieces[0])
    for cut in pieces[1:]:
        loudness = loudness * one(*cut)
    return loudness


def scatter_about(rng, shape, width, bound, cuts=(), kind=jnp.bfloat16):
    level = shard_levels(rng, shape, cuts, -0.22, 0.18) if cuts else 1.0
    drawn = jax.random.normal(rng, shape, jnp.float32) * width * level
    return jnp.minimum(jnp.maximum(drawn, -bound), bound).astype(kind)


def setup_inputs(seed: int = 0) -> dict:
    arg_keys = jax.random.split(jax.random.key(seed), 26)
    return {
        "residual": scatter_about(arg_keys[0], (TOKENS, D), 1.0, 6.0, ((0, 32),)),
        "small_heads": scatter_about(arg_keys[1], (TOKENS, HA * PA), 1.0, 6.0, ((0, 32), (1, 4))),
        "large_heads": scatter_about(arg_keys[2], (TOKENS, HB * PB), 1.0, 6.0, ((0, 32), (1, 4))),
        "state_keys": scatter_about(arg_keys[3], (TOKENS, GROUPS, STATE), 1.0, 6.0, ((0, 32), (1, 4))),
        "state_queries": scatter_about(arg_keys[4], (TOKENS, GROUPS, STATE), 1.0, 6.0, ((0, 32), (1, 4))),
        "small_gate": scatter_about(arg_keys[5], (TOKENS, HA * PA), 1.0, 6.0, ((0, 32), (1, 4))),
        "large_gate": scatter_about(arg_keys[6], (TOKENS, HB * PB), 1.0, 6.0, ((0, 32), (1, 4))),
        "small_step": draw_small_step(jax.random.fold_in(arg_keys[25], 71), 0),
        "large_step": draw_large_step(jax.random.fold_in(arg_keys[25], 71), 0),
        "small_taps": scatter_about(arg_keys[9], (CONV, HA * PA), CONV ** -0.5, 3.0, ((1, 4),)),
        "large_taps": scatter_about(arg_keys[10], (CONV, HB * PB), CONV ** -0.5, 3.0, ((1, 4),)),
        "key_taps": scatter_about(arg_keys[11], (CONV, GROUPS, STATE), CONV ** -0.5, 3.0, ((1, 4),)),
        "query_taps": scatter_about(arg_keys[12], (CONV, GROUPS, STATE), CONV ** -0.5, 3.0, ((1, 4),)),
        "small_decay": draw_small_decay(jax.random.fold_in(arg_keys[25], 71), 0),
        "large_decay": draw_large_decay(jax.random.fold_in(arg_keys[25], 71), 0),
        "small_gain": jnp.clip(1.0 + 0.18 * jax.random.normal(arg_keys[15], (HA * PA,), jnp.float32), 0.099609375, 1.8984375).astype(jnp.bfloat16),
        "large_gain": jnp.clip(1.0 + 0.18 * jax.random.normal(arg_keys[16], (HB * PB,), jnp.float32), 0.099609375, 1.8984375).astype(jnp.bfloat16),
        "small_out": scatter_about(arg_keys[17], (HA * PA, D), (HA * PA + HB * PB) ** -0.5, 0.125, ((0, 4),)),
        "large_out": scatter_about(arg_keys[18], (HB * PB, D), (HA * PA + HB * PB) ** -0.5, 0.125, ((0, 4),)),
        "mixer_gain": jnp.clip(1.0 + 0.18 * jax.random.normal(arg_keys[19], (D,), jnp.float32), 0.099609375, 1.8984375).astype(jnp.bfloat16),
        "ffn_in_gain": jnp.clip(1.0 + 0.18 * jax.random.normal(arg_keys[20], (D,), jnp.float32), 0.099609375, 1.8984375).astype(jnp.bfloat16),
        "gate_proj": scatter_about(arg_keys[21], (D, FF), D ** -0.5, 0.125, ((0, 32), (1, 4))),
        "up_proj": scatter_about(arg_keys[22], (D, FF), D ** -0.5, 0.125, ((0, 32), (1, 4))),
        "down_proj": scatter_about(arg_keys[23], (D, FF), FF ** -0.5, 0.078125, ((0, 32), (1, 4))),
        "ffn_out_gain": jnp.clip(1.0 + 0.18 * jax.random.normal(arg_keys[24], (D,), jnp.float32), 0.099609375, 1.8984375).astype(jnp.bfloat16),
    }


EPS = 1e-06

def rounded(values):
    return lax.optimization_barrier(values.astype(jnp.bfloat16)).astype(jnp.float32)

def causal_taps(extended, tap_weights, length):
    kernel_len = tap_weights.shape[0]
    summed = jnp.zeros((length,) + extended.shape[1:], jnp.float32)
    for offset in range(kernel_len):
        window_rows = extended[offset:offset + length].astype(jnp.float32)
        summed = summed + tap_weights[offset].astype(jnp.float32) * window_rows
    return jax.nn.silu(summed).astype(jnp.bfloat16)

def block_pass(values, key_rows, queries, step_sizes, decay_rates):
    length, groups, head_count, head_dim = values.shape
    block_count = length // BLOCK
    state_len = key_rows.shape[-1]
    log_decay = -step_sizes * decay_rates
    causal = jnp.tril(jnp.ones((BLOCK, BLOCK), dtype=bool))
    highest = lax.Precision.HIGHEST

    def one_block(carry_state, block):
        block_values, block_keys, block_queries, block_steps, block_decay = block
        values_wide = block_values.astype(jnp.float32)
        keys_wide = block_keys.astype(jnp.float32)
        queries_wide = block_queries.astype(jnp.float32)
        cumulative = jnp.cumsum(block_decay, axis=0)
        scores = jnp.einsum('lgn,sgn->gls', queries_wide, keys_wide, precision=highest)
        cum_heads = jnp.transpose(cumulative, (1, 2, 0))
        gap_matrix = cum_heads[:, :, :, None] - cum_heads[:, :, None, :]
        decays = jnp.exp(jnp.where(causal, gap_matrix, -jnp.inf))
        step_heads = jnp.transpose(block_steps, (1, 2, 0))[:, :, None, :]
        weights = rounded(scores[:, None] * decays * step_heads)
        inside = jnp.einsum('ghls,sghp->lghp', weights, values_wide, precision=highest)
        carried = jnp.einsum('lgn,ghpn->lghp', queries_wide, carry_state, precision=highest)
        carried = carried * jnp.exp(cumulative)[..., None]
        tail_sum = cumulative[-1]
        scaled = rounded(values_wide * (block_steps * jnp.exp(tail_sum - cumulative))[..., None])
        fresh_state = jnp.einsum('lghp,lgn->ghpn', scaled, keys_wide, precision=highest)
        next_state = carry_state * jnp.exp(tail_sum)[..., None, None] + fresh_state
        return (next_state, inside + carried)
    blocked = (values.reshape(block_count, BLOCK, groups, head_count, head_dim), key_rows.reshape(block_count, BLOCK, groups, state_len), queries.reshape(block_count, BLOCK, groups, state_len), step_sizes.reshape(block_count, BLOCK, groups, head_count), log_decay.reshape(block_count, BLOCK, groups, head_count))
    start_state = jnp.zeros((groups, head_count, head_dim, state_len), jnp.float32)
    end_state, outputs = lax.scan(one_block, start_state, blocked)
    return outputs.reshape(length, groups, head_count, head_dim)

def head_group(values, key_rows, queries, step_raw, decay_log):
    length = values.shape[0]
    head_count = step_raw.shape[1]
    groups = key_rows.shape[1]
    per_group = head_count // groups
    head_dim = values.shape[1] // head_count
    step_sizes = jax.nn.softplus(step_raw.astype(jnp.float32)).reshape(length, groups, per_group)
    decay_rates = jnp.exp(decay_log.astype(jnp.float32)).reshape(groups, per_group)
    return block_pass(values.reshape(length, groups, per_group, head_dim), key_rows, queries, step_sizes, decay_rates)

def unit_rms(values):
    return values * lax.rsqrt(lax.optimization_barrier(jnp.mean(values * values, axis=-1, keepdims=True)) + EPS)

def gate_and_norm(mixed_heads, gate_raw, gain):
    length, groups, per_group, head_dim = mixed_heads.shape
    gated = mixed_heads.reshape(length, -1) * jax.nn.silu(gate_raw.astype(jnp.float32))
    normed = unit_rms(gated.reshape(length, groups * per_group, head_dim))
    return (normed.reshape(length, -1) * gain.astype(jnp.float32)).astype(jnp.bfloat16)

def blockwise_sum(pairs, length, features):
    summed = jnp.zeros((length, features), jnp.float32)
    for index in range(HEAD_BLOCKS):
        partial_value = jnp.zeros((length, features), jnp.float32)
        for left, right in pairs:
            cols = left.shape[1] // HEAD_BLOCKS
            partial_value = partial_value + jnp.dot(left[:, index * cols:(index + 1) * cols], right[index * cols:(index + 1) * cols], preferred_element_type=jnp.float32)
        summed = summed + rounded(partial_value)
    return summed

def reference(residual, small_heads, large_heads, state_keys, state_queries, small_gate, large_gate, small_step, large_step, small_taps, large_taps, key_taps, query_taps, small_decay, large_decay, small_gain, large_gain, small_out, large_out, mixer_gain, ffn_in_gain, gate_proj, up_proj, down_proj, ffn_out_gain):
    length = residual.shape[0]
    halo_rows = small_taps.shape[0] - 1

    def extended(values):
        return jnp.concatenate([jnp.zeros((halo_rows,) + values.shape[1:], values.dtype), values], axis=0)
    small_conv = causal_taps(extended(small_heads), small_taps, length)
    large_conv = causal_taps(extended(large_heads), large_taps, length)
    key_conv = causal_taps(extended(state_keys), key_taps, length)
    query_conv = causal_taps(extended(state_queries), query_taps, length)
    small_mix = head_group(small_conv, key_conv[:, 0::2], query_conv[:, 0::2], small_step, small_decay)
    large_mix = head_group(large_conv, key_conv[:, 1::2], query_conv[:, 1::2], large_step, large_decay)
    small_normed = gate_and_norm(small_mix, small_gate, small_gain)
    large_normed = gate_and_norm(large_mix, large_gate, large_gain)
    mix = blockwise_sum([(small_normed, small_out), (large_normed, large_out)], length, D)
    mixed = residual.astype(jnp.float32) + unit_rms(mix) * mixer_gain.astype(jnp.float32)
    normed_in = (unit_rms(mixed) * ffn_in_gain.astype(jnp.float32)).astype(jnp.bfloat16)
    gate = jnp.dot(normed_in, gate_proj, preferred_element_type=jnp.float32)
    up_values = jnp.dot(normed_in, up_proj, preferred_element_type=jnp.float32)
    hidden = (jax.nn.silu(gate) * up_values).astype(jnp.bfloat16)
    ffn = blockwise_sum([(hidden, jnp.transpose(down_proj))], length, D)
    updated = mixed + 0.5 * unit_rms(ffn) * ffn_out_gain.astype(jnp.float32)
    return updated.astype(jnp.bfloat16)
```

```python
import functools

import jax
import jax.numpy as jnp
from jax import lax
from jax.experimental import pallas as pl
from jax.experimental.pallas import tpu as pltpu
from jax.sharding import PartitionSpec as P

BLOCK = 128
HALO = 16
LANES = 128
SLOTS = 8
TAIL = 16
SIDE = 4

EPS = 1e-06
FAR = -1e30
F32 = jnp.float32
BF16 = jnp.bfloat16
MESH = pl.DeviceIdType.MESH
VMEM_LIMIT = 66_000_000


def silu(x):
    return x / (1.0 + jnp.exp(-x))


def softplus(x):
    return jnp.maximum(x, 0.0) + jnp.log1p(jnp.exp(-jnp.abs(x)))


def exact_dot(a, b, dims=(((1,), (0,)), ((), ()))):
    return lax.dot_general(a, b, dims, precision=lax.Precision.HIGHEST, preferred_element_type=F32)


def lower(n):
    rows = lax.broadcasted_iota(jnp.int32, (n, n), 0)
    return rows >= lax.broadcasted_iota(jnp.int32, (n, n), 1)


def spread(columns, heads, dim):
    rows = columns.shape[0]
    parts = []
    if dim >= LANES:
        for h in heads:
            parts.append(jnp.broadcast_to(columns[:, h : h + 1], (rows, dim)))
    else:
        per = LANES // dim
        lane = lax.broadcasted_iota(jnp.int32, (rows, LANES), 1)
        for first in range(0, len(heads), per):
            part = jnp.broadcast_to(columns[:, heads[first] : heads[first] + 1], (rows, LANES))
            for j in range(1, per):
                h = heads[first + j]
                part = jnp.where(lane >= j * dim, columns[:, h : h + 1], part)
            parts.append(part)
    return jnp.concatenate(parts, axis=1)


def unit_rms(values):
    return values * lax.rsqrt(jnp.mean(values * values, axis=-1, keepdims=True) + EPS)


def pack(ref, slot, state, log):
    rows = state.shape[0]
    high = log.astype(BF16).astype(F32)
    row = lax.broadcasted_iota(jnp.int32, (TAIL, log.shape[1]), 0)
    both = jnp.where(row == 0, high, jnp.where(row == 1, log - high, 0.0))
    if slot is None:
        ref[:rows] = state.astype(BF16)
        ref[rows:] = both.astype(BF16)
    else:
        ref[slot, :rows] = state.astype(BF16)
        ref[slot, rows:] = both.astype(BF16)


def opened(packet, rows):
    log = packet[rows : rows + TAIL].astype(F32)
    return packet[:rows].astype(F32), log[0:1] + log[1:2]


class Counter:
    def __init__(self):
        self.n = 0

    def take(self, count=1):
        first = self.n
        self.n += count
        return first


def tile_list(width, tile):
    return [(s, min(tile, width - s)) for s in range(0, width, tile)]


def whole_kernel(
    sizes,
    res_in,
    small_in,
    large_in,
    key_in,
    query_in,
    small_gate,
    large_gate,
    steps,
    decay,
    taps,
    gain,
    small_out,
    large_out,
    mixer_gain,
    in_gain,
    out_gain,
    gate_in,
    up_in,
    down_in,
    out,
    xin,
    conv,
    dts,
    cums,
    logs,
    starts,
    inside,
    state,
    total,
    packet,
    from_partner,
    first_state,
    first_log,
    along_y,
    along_z,
    row_state,
    row_log,
    entering,
    for_partner,
    w,
    o,
    heads,
    res,
    mixbuf,
    ownmix,
    ninbuf,
    hidden,
    parts,
    ra,
    rb,
    rc,
    rd,
    send,
    recv,
    local,
):
    (heads_a, dim_a), (heads_b, dim_b), state_len, blocks = sizes
    head_list_a = list(range(heads_a))
    head_list_b = list(range(heads_a, heads_a + heads_b))
    width_a = heads_a * dim_a
    width_b = heads_b * dim_b
    width = width_a + width_b
    groups = (
        (head_list_a, dim_a, width_a, 0),
        (head_list_b, dim_b, width_b, width_a),
    )

    sp = lax.axis_index("sp")
    x = lax.axis_index("tp")
    c = lax.rem(sp, 2)
    y = lax.rem(sp // 2, SIDE)
    z = sp // (2 * SIDE)
    count_sp = lax.axis_size("sp")

    def turn(v, d):
        return lax.rem(v + d + SIDE, SIDE)

    def at_chip(zz, yy, xx):
        return ((zz * SIDE + yy) * 2 + c, xx)

    partner = (sp + 1 - 2 * c, x)
    xs = {d: (sp, turn(x, d)) for d in (1, -1)}
    ys = {d: at_chip(z, turn(y, d), x) for d in (1, -1, 2)}
    zs = {d: at_chip(turn(z, d), y, x) for d in (1, -1, 2)}
    after = (lax.rem(sp + 1, count_sp), x)
    prior = (lax.rem(sp + count_sp - 1, count_sp), x)

    counter = Counter()
    issued = []

    def message(src, dst, landing, target, index):
        copy = pltpu.make_async_remote_copy(
            src_ref=src,
            dst_ref=dst,
            send_sem=send.at[index],
            recv_sem=recv.at[index],
            device_id=target,
            device_id_type=MESH,
        )
        arrival = pltpu.make_async_remote_copy(
            src_ref=landing,
            dst_ref=landing,
            send_sem=send.at[index],
            recv_sem=recv.at[index],
            device_id=target,
            device_id_type=MESH,
        )
        return copy, arrival

    barrier = pltpu.get_barrier_semaphore()
    greeted = [partner, xs[1], xs[-1], ys[1], ys[-1], ys[2], zs[1], zs[-1], zs[2], after, prior]
    for peer in greeted:
        pl.semaphore_signal(barrier, inc=1, device_id=peer, device_id_type=MESH)

    loads = []

    def load(src, dst):
        copy = pltpu.make_async_copy(src, dst, local.at[len(loads)])
        copy.start()
        loads.append(copy)
        return copy

    length = small_in.shape[0]
    weight_loads = [
        load(ref, w.at[m, z, y, c]) for m, ref in enumerate((gate_in, up_in, down_in))
    ]
    conv_loads = [
        load(ref, xin.at[g, pl.ds(HALO, length)])
        for g, ref in enumerate((small_in, large_in, key_in, query_in))
    ]
    out_loads = [
        load(small_out, o.at[pl.ds(x * width, width_a)]),
        load(large_out, o.at[pl.ds(x * width + width_a, width_b)]),
    ]
    res_loads = [load(res_in.at[:, k], res.at[k]) for k in range(SIDE)]

    pl.semaphore_wait(barrier, len(greeted))

    halo = []
    for g, ref in enumerate((small_in, large_in, key_in, query_in)):
        first = xin.at[g, pl.ds(0, HALO)]
        copy, arrival = message(
            ref.at[pl.ds(length - HALO, HALO)], first, first, after, counter.take()
        )
        copy.start()
        issued.append(copy)
        halo.append(arrival)

    half_rows = gate_in.shape[0] // 2
    quarter_rows = half_rows // 2

    def wline(h, first_axis, offset, q=None):
        rows = (
            pl.ds(half_rows * h, half_rows)
            if q is None
            else pl.ds(half_rows * h + quarter_rows * q, quarter_rows)
        )
        if first_axis:
            if h == 0:
                return w.at[:, z, turn(y, offset), c, rows]
            return w.at[:, turn(z, offset), y, c, rows]
        if h == 0:
            return w.at[:, turn(z, offset), :, c, rows]
        return w.at[:, :, turn(y, offset), c, rows]

    def wtarget(h, first_axis, d):
        return (ys if (h == 0) == first_axis else zs)[d]

    def wmirror(h, offset):
        rows = pl.ds(half_rows * h, half_rows)
        if h == 0:
            return w.at[:, turn(z, offset), :, 1 - c, rows]
        return w.at[:, :, turn(y, offset), 1 - c, rows]

    def spread_weights(first_axis):
        sent = []
        for h in (0, 1):
            for d in (1, -1):
                src = wline(h, first_axis, 0)
                copy, arrival = message(
                    src, src, wline(h, first_axis, -d), wtarget(h, first_axis, d), counter.take()
                )
                copy.start()
                issued.append(copy)
                sent.append(arrival)
        return sent

    def forward_weights(first_axis):
        sent = []
        for h in (0, 1):
            for d, q in ((1, 0), (-1, 1)):
                src = wline(h, first_axis, -d, q)
                copy, arrival = message(
                    src,
                    src,
                    wline(h, first_axis, -2 * d, q),
                    wtarget(h, first_axis, d),
                    counter.take(),
                )
                copy.start()
                issued.append(copy)
                sent.append(arrival)
        return sent

    def mirror_weights(offsets):
        sent = []
        for h in (0, 1):
            for offset in offsets:
                src = wline(h, False, offset)
                copy, arrival = message(src, src, wmirror(h, offset), partner, counter.take())
                copy.start()
                issued.append(copy)
                sent.append(arrival)
        return sent

    def wait_all(arrivals):
        for arrival in arrivals:
            arrival.wait_recv()

    for copy in weight_loads:
        copy.wait()
    w_first = spread_weights(True)
    progress = {"w_first": w_first}

    o_half = width // 2

    def orows(offset, core, q=None):
        base = turn(x, offset) * width + core * o_half
        if q is None:
            return o.at[pl.ds(base, o_half)]
        return o.at[pl.ds(base + q * (o_half // 2), o_half // 2)]

    for copy in out_loads:
        copy.wait()
    o_first = []
    for d in (1, -1):
        src = orows(0, c)
        copy, arrival = message(src, src, orows(-d, c), xs[d], counter.take())
        copy.start()
        issued.append(copy)
        o_first.append(arrival)

    def forward_out():
        wait_all(o_first)
        second, mirrored = [], []
        for d, q in ((1, 0), (-1, 1)):
            src = orows(-d, c, q)
            copy, arrival = message(src, src, orows(-2 * d, c, q), xs[d], counter.take())
            copy.start()
            issued.append(copy)
            second.append(arrival)
        for d in (1, -1):
            src = orows(d, c)
            copy, arrival = message(src, src, orows(d, 1 - c), partner, counter.take())
            copy.start()
            issued.append(copy)
            mirrored.append(arrival)
        progress["o_second"] = second
        progress["o_mirrored"] = mirrored

    def mirror_out():
        wait_all(progress["o_second"])
        src = orows(2, c)
        copy, arrival = message(src, src, orows(2, 1 - c), partner, counter.take())
        copy.start()
        issued.append(copy)
        progress["o_mirrored"].append(arrival)

    for copy in conv_loads:
        copy.wait()
    wait_all(halo)
    for g in range(4):
        edge = xin[g, :HALO].astype(F32)
        xin[g, :HALO] = jnp.where(sp == 0, 0.0, edge).astype(BF16)
    state[...] = jnp.zeros_like(state)
    total[...] = jnp.zeros_like(total)
    kernel_len = taps.shape[0]

    def convolve(i, carry):
        at = pl.multiple_of(i * BLOCK, BLOCK)
        rows = pl.ds(at, BLOCK)
        column = 0
        for g in range(4):
            for first_lane in range(0, xin.shape[2], LANES):
                here = pl.ds(column, LANES)
                extended = xin[g, pl.ds(at, BLOCK + HALO), pl.ds(first_lane, LANES)].astype(F32)
                summed = None
                for k in range(kernel_len):
                    first = HALO - kernel_len + 1 + k
                    term = taps[k : k + 1, here] * extended[first : first + BLOCK]
                    summed = term if summed is None else summed + term
                conv[rows, here] = silu(summed).astype(BF16)
                column += LANES
        dt = softplus(steps[rows])
        cum = exact_dot(lower(BLOCK).astype(F32), -dt * jnp.exp(decay[...]))
        dts[rows] = dt
        cums[rows] = cum
        tail = cum[BLOCK - 1 : BLOCK]
        scale = dt * jnp.exp(tail - cum)
        kept = jnp.exp(tail)
        before = total[...]
        logs[i] = jnp.concatenate(
            [spread(before, head_list_a, dim_a), spread(before, head_list_b, dim_b)], axis=1
        )
        for which, (head_list, dim, wide, offset) in enumerate(groups):
            key_at = width + which * state_len
            columns = slice(offset, offset + wide)
            xv = conv[rows, columns].astype(F32)
            u = (xv * spread(scale, head_list, dim)).astype(BF16)
            k = conv[rows, key_at : key_at + state_len]
            fresh = lax.dot_general(k, u, (((0,), (0,)), ((), ())), preferred_element_type=F32)
            old = state[:, columns]
            starts[i, :, columns] = old
            state[:, columns] = old * spread(kept, head_list, dim) + fresh
        total[...] = before + tail
        return carry

    lax.fori_loop(0, blocks // 2, convolve, 0)
    wait_all(w_first)
    w_second = forward_weights(True)
    lax.fori_loop(blocks // 2, blocks, convolve, 0)

    half = width // 2

    def half_of(core):
        return pl.ds(pl.multiple_of(core * half, half), half)

    final_log = jnp.concatenate(
        [spread(total[...], head_list_a, dim_a), spread(total[...], head_list_b, dim_b)], axis=1
    )
    pack(packet, None, state[...], final_log)
    copy, swapped = message(
        packet.at[:, half_of(1 - c)], from_partner, from_partner, partner, counter.take()
    )
    copy.start()
    issued.append(copy)

    wait_all(w_second)
    w_third = spread_weights(False)
    w_mirrored = mirror_weights((0,))

    def mix_inside(i, carry):
        at = pl.multiple_of(i * BLOCK, BLOCK)
        rows = pl.ds(at, BLOCK)
        causal = lower(BLOCK)
        row_id = lax.broadcasted_iota(jnp.int32, (BLOCK, BLOCK), 0)
        eye = (row_id == lax.broadcasted_iota(jnp.int32, (BLOCK, BLOCK), 1)).astype(F32)
        flip = (((0,), (0,)), ((), ()))
        dt_across = exact_dot(dts[rows], eye, flip)
        cum = cums[rows]
        cum_across = exact_dot(cum, eye, flip)
        lane = lax.broadcasted_iota(jnp.int32, (BLOCK, LANES), 1)
        for which, (head_list, dim, wide, offset) in enumerate(groups):
            key_at = width + which * state_len
            query_at = key_at + 2 * state_len
            k = conv[rows, key_at : key_at + state_len]
            q = conv[rows, query_at : query_at + state_len]
            scores = lax.dot_general(q, k, (((1,), (1,)), ((), ())), preferred_element_type=F32)
            span = max(dim, LANES)
            per = span // dim
            for first in range(0, len(head_list), per):
                columns = slice(offset + first * dim, offset + first * dim + span)
                x_part = conv[rows, columns]
                part = None
                for j in range(per):
                    h = head_list[first + j]
                    gap = cum[:, h : h + 1] - cum_across[h : h + 1]
                    decays = jnp.exp(jnp.where(causal, gap, FAR))
                    weight = (scores * decays * dt_across[h : h + 1]).astype(BF16)
                    got = jnp.dot(weight, x_part, preferred_element_type=F32)
                    part = got if part is None else jnp.where(lane >= j * dim, got, part)
                inside[rows, columns] = part
        return carry

    def send_along(buffer, targets):
        arrivals = []
        for d, slot in ((1, 1), (2, 2), (-1, 3)):
            copy, arrival = message(
                buffer.at[0], buffer.at[slot], buffer.at[slot], targets[d], counter.take()
            )
            copy.start()
            issued.append(copy)
            arrivals.append(arrival)
        return arrivals

    def fold(buffer, place, number):
        zero = jnp.zeros((state_len, half), F32)
        every, every_log = zero, jnp.zeros((1, half), F32)
        ahead, ahead_log = every, every_log
        for p in range(number):
            slot = turn(place, -p)
            one, log = opened(buffer[slot], state_len)
            counts = p < place
            ahead = jnp.where(counts, ahead * jnp.exp(log) + one, ahead)
            ahead_log = jnp.where(counts, ahead_log + log, ahead_log)
            every = every * jnp.exp(log) + one
            every_log = every_log + log
        return every, every_log, ahead, ahead_log

    lax.fori_loop(0, 1, mix_inside, 0)
    swapped.wait_recv()
    mine, mine_log = opened(packet[:, half_of(c)], state_len)
    theirs, theirs_log = opened(from_partner[...], state_len)
    even = c == 0
    a_state = jnp.where(even, mine, theirs)
    a_log = jnp.where(even, mine_log, theirs_log)
    b_state = jnp.where(even, theirs, mine)
    b_log = jnp.where(even, theirs_log, mine_log)
    first_state[...] = a_state
    first_log[...] = a_log
    pack(along_y, 0, a_state * jnp.exp(b_log) + b_state, a_log + b_log)
    y_arrivals = send_along(along_y, ys)

    lax.fori_loop(1, 4, mix_inside, 0)
    wait_all(y_arrivals)
    row_all, row_all_log, row_ahead, row_ahead_log = fold(along_y, y, SIDE)
    row_state[...] = row_ahead
    row_log[...] = row_ahead_log
    pack(along_z, 0, row_all, row_all_log)
    z_arrivals = send_along(along_z, zs)

    lax.fori_loop(4, 7, mix_inside, 0)
    wait_all(z_arrivals)
    _, _, plane_ahead, _ = fold(along_z, z, SIDE - 1)
    chip = plane_ahead * jnp.exp(row_log[...]) + row_state[...]
    second = chip * jnp.exp(first_log[...]) + first_state[...]
    entering[:, half_of(c)] = jnp.where(even, chip, second)
    for_partner[...] = jnp.where(even, second, chip)
    copy, entered = message(
        for_partner,
        entering.at[:, half_of(c)],
        entering.at[:, half_of(1 - c)],
        partner,
        counter.take(),
    )
    copy.start()
    issued.append(copy)
    lax.fori_loop(7, blocks, mix_inside, 0)
    entered.wait_recv()

    sub = length // (SIDE * SIDE)
    lane = lax.broadcasted_iota(jnp.int32, (BLOCK, LANES), 1)

    def carry_block(n, carry):
        stage = n // SIDE
        d = lax.rem(n, SIDE)
        i = 2 * d + stage
        rows = pl.ds(pl.multiple_of(i * BLOCK, BLOCK), BLOCK)
        grown = jnp.exp(cums[rows])
        for which, (head_list, dim, wide, offset) in enumerate(groups):
            columns = slice(offset, offset + wide)
            query_at = width + (2 + which) * state_len
            q = conv[rows, query_at : query_at + state_len]
            old = starts[i, :, columns] + entering[:, columns] * jnp.exp(logs[i, :, columns])
            carried = jnp.dot(q, old.astype(BF16), preferred_element_type=F32)
            mixed = inside[rows, columns] + carried * spread(grown, head_list, dim)
            gate = (small_gate, large_gate)[which]
            gated = mixed * silu(gate[rows].astype(F32))
            squares = gated * gated
            span = max(dim, LANES)
            per = span // dim
            normed = []
            for first in range(0, len(head_list), per):
                at = first * dim
                part = squares[:, at : at + span]
                means = None
                for j in range(per):
                    if per == 1:
                        means = jnp.sum(part, axis=1, keepdims=True)
                    else:
                        ours = (lane >= j * dim) & (lane < (j + 1) * dim)
                        one = jnp.sum(jnp.where(ours, part, 0.0), axis=1, keepdims=True)
                        means = one if means is None else jnp.where(lane >= j * dim, one, means)
                normed.append(gated[:, at : at + span] * lax.rsqrt(means * (1.0 / dim) + EPS))
            normed = (jnp.concatenate(normed, axis=1) * gain[:, columns]).astype(BF16)
            place = pl.ds(pl.multiple_of(x * width + offset, LANES), wide)
            spot = pl.ds(pl.multiple_of(d * sub, sub), sub)
            heads[2 * stage, spot, place] = normed[:sub]
            heads[2 * stage + 1, spot, place] = normed[sub:]
        return carry

    def hcols(offset):
        return pl.ds(pl.multiple_of(turn(x, offset) * width, LANES), width)

    step_rows = heads.shape[1]
    g1 = {d: counter.take(SIDE) for d in (1, -1)}
    g2 = {d: counter.take(SIDE) for d in (1, -1)}

    def heads_message(k, d):
        src = heads.at[k, :, hcols(0)]
        return message(src, src, heads.at[k, :, hcols(-d)], xs[d], g1[d] + k)

    def heads_forward(k, d):
        rows = pl.ds(0 if d == 1 else step_rows // 2, step_rows // 2)
        src = heads.at[k, rows, hcols(-d)]
        return message(src, src, heads.at[k, rows, hcols(-2 * d)], xs[d], g2[d] + k)

    def start_heads(k):
        for d in (1, -1):
            heads_message(k, d)[0].start()

    def forward_heads(k):
        for d in (1, -1):
            heads_message(k, d)[1].wait_recv()
        for d in (1, -1):
            heads_forward(k, d)[0].start()

    lax.fori_loop(0, SIDE, carry_block, 0)
    start_heads(0)
    start_heads(1)
    forward_out()
    lax.fori_loop(SIDE, 2 * SIDE, carry_block, 0)
    start_heads(2)
    start_heads(3)
    wait_all(w_third)
    w_fourth = forward_weights(False)
    w_mirrored += mirror_weights((1, -1))
    mirror_out()
    forward_heads(0)
    forward_heads(1)
    for copy in res_loads:
        copy.wait()
    wait_all(progress["o_mirrored"])
    wait_all(w_fourth)
    w_mirrored += mirror_weights((2,))
    wait_all(w_mirrored)

    features = res.shape[3]
    hid = hidden.shape[1]
    side_half = features // 2
    r1 = {d: counter.take(SIDE) for d in (1, -1)}
    r2 = {d: counter.take(SIDE) for d in (1, -1)}

    def prow(offset):
        return pl.ds(pl.multiple_of(turn(x, offset) * sub, sub), sub)

    def far_message(k, d):
        lanes = pl.ds(0 if d == 1 else side_half, side_half)
        landing = (ra if d == 1 else rb).at[k]
        return message(parts.at[k, prow(2), lanes], landing, landing, xs[d], r1[d] + k)

    def near_message(k, d):
        landing = (rc if d == 1 else rd).at[k]
        return message(parts.at[k, prow(d)], landing, landing, xs[d], r2[d] + k)

    def pass_on(k):
        for d in (1, -1):
            far_message(k, d)[1].wait_recv()
            lanes = slice(0, side_half) if d == 1 else slice(side_half, features)
            extra = (ra if d == 1 else rb)[k].astype(F32)
            mine = parts[k, prow(d), lanes].astype(F32)
            parts[k, prow(d), lanes] = (mine + extra).astype(BF16)
            near_message(k, d)[0].start()

    def channel_mix(k, carry):
        for d in (1, -1):
            heads_forward(k, d)[1].wait_recv()
        left = heads[k]
        for first, size in tile_list(features, 512):
            mixbuf[:, first : first + size] = jnp.dot(
                left, o[:, first : first + size], preferred_element_type=F32
            )

        @pl.when(k < 2)
        def _():
            forward_heads(k + 2)

        for d in range(SIDE):
            rows = slice(d * sub, (d + 1) * sub)
            mixed = res[k, d].astype(F32) + unit_rms(mixbuf[rows]) * mixer_gain[...].astype(F32)
            mixbuf[rows] = mixed
            ninbuf[rows] = (unit_rms(mixed) * in_gain[...].astype(F32)).astype(BF16)
        ownmix[k] = mixbuf[prow(0)]

        @pl.when(k > 0)
        def _():
            pass_on(k - 1)

        nin = ninbuf[...]
        for first, size in tile_list(hid, 512):
            wg = w[0, :, :, :, :, first : first + size].reshape(features, size)
            wu = w[1, :, :, :, :, first : first + size].reshape(features, size)
            gate = jnp.dot(nin, wg, preferred_element_type=F32)
            up = jnp.dot(nin, wu, preferred_element_type=F32)
            hidden[:, first : first + size] = (silu(gate) * up).astype(BF16)
        hv = hidden[...]
        tile = features // SIDE
        for n in range(SIDE):
            wd = w[2, n].reshape(tile, hid)
            got = lax.dot_general(hv, wd, (((1,), (1,)), ((), ())), preferred_element_type=F32)
            parts[k, :, n * tile : (n + 1) * tile] = got.astype(BF16)
        for d in (1, -1):
            far_message(k, d)[0].start()
        return carry

    lax.fori_loop(0, SIDE, channel_mix, 0)

    def finish(k):
        for d in (1, -1):
            near_message(k, d)[1].wait_recv()
        ffn = parts[k, prow(0)].astype(F32) + rc[k].astype(F32) + rd[k].astype(F32)
        updated = ownmix[k] + 0.5 * unit_rms(ffn) * out_gain[...].astype(F32)
        out[k * sub : (k + 1) * sub] = updated.astype(BF16)

    for k in range(SIDE - 1):
        finish(k)
    pass_on(SIDE - 1)
    finish(SIDE - 1)

    for copy in issued:
        copy.wait_send()

    def drain(k, carry):
        for d in (1, -1):
            heads_message(k, d)[0].wait_send()
            heads_forward(k, d)[0].wait_send()
            far_message(k, d)[0].wait_send()
            near_message(k, d)[0].wait_send()
        return carry

    lax.fori_loop(0, SIDE, drain, 0)


def local_program(
    residual,
    small_heads,
    large_heads,
    state_keys,
    state_queries,
    small_gate,
    large_gate,
    small_step,
    large_step,
    small_taps,
    large_taps,
    key_taps,
    query_taps,
    small_decay,
    large_decay,
    small_gain,
    large_gain,
    small_out,
    large_out,
    mixer_gain,
    ffn_in_gain,
    gate_proj,
    up_proj,
    down_proj,
    ffn_out_gain,
):
    length, features = residual.shape
    state_len = state_keys.shape[-1]
    key_rows = state_keys.reshape(length, -1)
    query_rows = state_queries.reshape(length, -1)
    heads_a = small_step.shape[1]
    heads_b = large_step.shape[1]
    heads = heads_a + heads_b
    width_a = small_heads.shape[1]
    width_b = large_heads.shape[1]
    width = width_a + width_b
    everything = width + key_rows.shape[1] + query_rows.shape[1]
    blocks = length // BLOCK
    sizes = ((heads_a, width_a // heads_a), (heads_b, width_b // heads_b), state_len, blocks)
    steps = jnp.pad(
        jnp.concatenate([small_step, large_step], axis=1), ((0, 0), (0, SLOTS - heads))
    )
    decay = jnp.pad(jnp.concatenate([small_decay, large_decay]), (0, SLOTS - heads))[None]
    kernel_len = small_taps.shape[0]
    taps = jnp.concatenate(
        [
            small_taps,
            large_taps,
            key_taps.reshape(kernel_len, -1),
            query_taps.reshape(kernel_len, -1),
        ],
        axis=1,
    ).astype(F32)
    gain = jnp.concatenate([small_gain, large_gain]).astype(F32)[None]
    sub = length // (SIDE * SIDE)
    step_rows = SIDE * sub
    wrows, hid = gate_proj.shape
    half = width // 2
    packet_rows = state_len + TAIL
    any_space = pl.BlockSpec(memory_space=pl.ANY)
    vmem = pl.BlockSpec(memory_space=pltpu.VMEM)
    messages = 128

    return pl.pallas_call(
        functools.partial(whole_kernel, sizes),
        in_specs=[any_space] * 5 + [vmem] * 6 + [any_space] * 2 + [vmem] * 3 + [any_space] * 3,
        out_specs=vmem,
        out_shape=jax.ShapeDtypeStruct((length // SIDE, features), BF16),
        scratch_shapes=[
            pltpu.VMEM((4, HALO + length, width_a), BF16),
            pltpu.VMEM((length, everything), BF16),
            pltpu.VMEM((length, SLOTS), F32),
            pltpu.VMEM((length, SLOTS), F32),
            pltpu.VMEM((blocks, 1, width), F32),
            pltpu.VMEM((blocks, state_len, width), F32),
            pltpu.VMEM((length, width), F32),
            pltpu.VMEM((state_len, width), F32),
            pltpu.VMEM((1, SLOTS), F32),
            pltpu.VMEM((packet_rows, width), BF16),
            pltpu.VMEM((packet_rows, half), BF16),
            pltpu.VMEM((state_len, half), F32),
            pltpu.VMEM((1, half), F32),
            pltpu.VMEM((SIDE, packet_rows, half), BF16),
            pltpu.VMEM((SIDE, packet_rows, half), BF16),
            pltpu.VMEM((state_len, half), F32),
            pltpu.VMEM((1, half), F32),
            pltpu.VMEM((state_len, width), F32),
            pltpu.VMEM((state_len, half), F32),
            pltpu.VMEM((3, SIDE, SIDE, 2, wrows, hid), BF16),
            pltpu.VMEM((SIDE * width, features), BF16),
            pltpu.VMEM((SIDE, step_rows, SIDE * width), BF16),
            pltpu.VMEM((SIDE, SIDE, sub, features), BF16),
            pltpu.VMEM((step_rows, features), F32),
            pltpu.VMEM((SIDE, sub, features), F32),
            pltpu.VMEM((step_rows, features), BF16),
            pltpu.VMEM((step_rows, hid), BF16),
            pltpu.VMEM((SIDE, step_rows, features), BF16),
            pltpu.VMEM((SIDE, sub, features // 2), BF16),
            pltpu.VMEM((SIDE, sub, features // 2), BF16),
            pltpu.VMEM((SIDE, sub, features), BF16),
            pltpu.VMEM((SIDE, sub, features), BF16),
            pltpu.SemaphoreType.DMA((messages,)),
            pltpu.SemaphoreType.DMA((messages,)),
            pltpu.SemaphoreType.DMA((16,)),
        ],
        compiler_params=pltpu.CompilerParams(
            collective_id=0, has_side_effects=True, vmem_limit_bytes=VMEM_LIMIT
        ),
        cost_estimate=pl.CostEstimate(
            flops=40_000_000_000, bytes_accessed=60_000_000, transcendentals=0
        ),
        name="layer",
    )(
        residual.reshape(SIDE, SIDE, sub, features),
        small_heads,
        large_heads,
        key_rows,
        query_rows,
        small_gate,
        large_gate,
        steps,
        decay,
        taps,
        gain,
        small_out,
        large_out,
        mixer_gain[None],
        ffn_in_gain[None],
        ffn_out_gain[None],
        gate_proj,
        up_proj,
        down_proj,
    )


def solution(mesh):
    placed = (
        P("sp", None),
        P("sp", "tp"),
        P("sp", "tp"),
        P("sp", "tp", None),
        P("sp", "tp", None),
        P("sp", "tp"),
        P("sp", "tp"),
        P("sp", "tp"),
        P("sp", "tp"),
        P(None, "tp"),
        P(None, "tp"),
        P(None, "tp", None),
        P(None, "tp", None),
        P("tp"),
        P("tp"),
        P("tp"),
        P("tp"),
        P("tp", None),
        P("tp", None),
        P(),
        P(),
        P("sp", "tp"),
        P("sp", "tp"),
        P("sp", "tp"),
        P(),
    )
    return jax.shard_map(
        local_program, mesh=mesh, in_specs=placed, out_specs=P(("sp", "tp"), None), check_vma=False
    )
```

```python
import functools

import jax
import jax.numpy as jnp
from jax import lax
from jax.experimental import pallas as pl
from jax.experimental.pallas import tpu as pltpu
from jax.sharding import PartitionSpec as P

BLOCK = 128
HALO = 16
LANES = 128
SLOTS = 8
TAIL = 16
SIDE = 4

EPS = 1e-06
FAR = -1e30
F32 = jnp.float32
BF16 = jnp.bfloat16
MESH = pl.DeviceIdType.MESH
scope = jax.named_scope
VMEM_LIMIT = 66_000_000


def silu(x):
    return x / (1.0 + jnp.exp(-x))


def softplus(x):
    return jnp.maximum(x, 0.0) + jnp.log1p(jnp.exp(-jnp.abs(x)))


def exact_dot(a, b, dims=(((1,), (0,)), ((), ()))):
    return lax.dot_general(a, b, dims, precision=lax.Precision.HIGHEST, preferred_element_type=F32)


def lower(n):
    rows = lax.broadcasted_iota(jnp.int32, (n, n), 0)
    return rows >= lax.broadcasted_iota(jnp.int32, (n, n), 1)


def spread(columns, heads, dim):
    rows = columns.shape[0]
    parts = []
    if dim >= LANES:
        for h in heads:
            parts.append(jnp.broadcast_to(columns[:, h : h + 1], (rows, dim)))
    else:
        per = LANES // dim
        lane = lax.broadcasted_iota(jnp.int32, (rows, LANES), 1)
        for first in range(0, len(heads), per):
            part = jnp.broadcast_to(columns[:, heads[first] : heads[first] + 1], (rows, LANES))
            for j in range(1, per):
                h = heads[first + j]
                part = jnp.where(lane >= j * dim, columns[:, h : h + 1], part)
            parts.append(part)
    return jnp.concatenate(parts, axis=1)


def unit_rms(values):
    return values * lax.rsqrt(jnp.mean(values * values, axis=-1, keepdims=True) + EPS)


def pack(ref, slot, state, log):
    rows = state.shape[0]
    high = log.astype(BF16).astype(F32)
    row = lax.broadcasted_iota(jnp.int32, (TAIL, log.shape[1]), 0)
    both = jnp.where(row == 0, high, jnp.where(row == 1, log - high, 0.0))
    if slot is None:
        ref[:rows] = state.astype(BF16)
        ref[rows:] = both.astype(BF16)
    else:
        ref[slot, :rows] = state.astype(BF16)
        ref[slot, rows:] = both.astype(BF16)


def opened(packet, rows):
    log = packet[rows : rows + TAIL].astype(F32)
    return packet[:rows].astype(F32), log[0:1] + log[1:2]


class Counter:
    def __init__(self):
        self.n = 0

    def take(self, count=1):
        first = self.n
        self.n += count
        return first


def tile_list(width, tile):
    return [(s, min(tile, width - s)) for s in range(0, width, tile)]


def whole_kernel(
    sizes,
    res_in,
    small_in,
    large_in,
    key_in,
    query_in,
    small_gate,
    large_gate,
    small_step,
    large_step,
    small_decay,
    large_decay,
    small_taps,
    large_taps,
    key_taps,
    query_taps,
    small_gain,
    large_gain,
    small_out,
    large_out,
    mixer_gain,
    in_gain,
    out_gain,
    gate_in,
    up_in,
    down_in,
    out,
    xin,
    conv,
    taps,
    gain,
    dt_rows,
    cum_rows,
    cums,
    logs,
    starts,
    inside,
    state,
    total,
    packet,
    from_partner,
    first_state,
    first_log,
    along_y,
    along_z,
    row_state,
    row_log,
    entering,
    for_partner,
    w,
    ox,
    oy,
    heads,
    res,
    mixbuf,
    ownmix,
    ninbuf,
    hidden,
    parts,
    ra,
    rb,
    rc,
    rd,
    send,
    recv,
    local,
):
    (heads_a, dim_a), (heads_b, dim_b), state_len, blocks = sizes
    head_list_a = list(range(heads_a))
    head_list_b = list(range(heads_a, heads_a + heads_b))
    width_a = heads_a * dim_a
    width_b = heads_b * dim_b
    width = width_a + width_b
    groups = (
        (head_list_a, dim_a, width_a, 0),
        (head_list_b, dim_b, width_b, width_a),
    )

    sp = lax.axis_index("sp")
    x = lax.axis_index("tp")
    c = lax.rem(sp, 2)
    y = lax.rem(sp // 2, SIDE)
    z = sp // (2 * SIDE)
    zy = sp // 2
    count_sp = lax.axis_size("sp")

    def turn(v, d):
        return lax.rem(v + d + SIDE, SIDE)

    def at_chip(zz, yy):
        return ((zz * SIDE + yy) * 2 + c, x)

    partner = (sp + 1 - 2 * c, x)
    xs = {d: (sp, turn(x, d)) for d in (1, -1, 2)}
    ys = {d: at_chip(z, turn(y, d)) for d in (1, -1, 2)}
    zs = {d: at_chip(turn(z, d), y) for d in (1, -1, 2)}
    after = (lax.rem(sp + 1, count_sp), x)
    prior = (lax.rem(sp + count_sp - 1, count_sp), x)

    barrier = pltpu.get_barrier_semaphore()
    greeted = [partner, after, prior] + [v[d] for v in (xs, ys, zs) for d in (1, -1, 2)]
    for peer in greeted:
        pl.semaphore_signal(barrier, inc=1, device_id=peer, device_id_type=MESH)

    counter = Counter()
    issued = []

    def message(src, dst, target, index):
        return pltpu.make_async_remote_copy(
            src_ref=src,
            dst_ref=dst,
            send_sem=send.at[index],
            recv_sem=recv.at[index],
            device_id=target,
            device_id_type=MESH,
        )

    def post(src, dst, landing, target):
        index = counter.take()
        copy = message(src, dst, target, index)
        copy.start()
        issued.append(copy)
        return message(landing, landing, target, index)

    def wait_all(arrivals, name="wait"):
        with scope(name):
            for arrival in arrivals:
                arrival.wait_recv()

    def run(name, first, last, body):
        with scope(name):
            lax.fori_loop(first, last, body, 0)

    loads = []

    def load(src, dst):
        copy = pltpu.make_async_copy(src, dst, local.at[len(loads)])
        copy.start()
        loads.append(copy)
        return copy

    length = small_in.shape[0]
    orows, ocols = oy.shape[4], oy.shape[5]
    weight_loads = [
        load(ref, w.at[m, z, y, c]) for m, ref in enumerate((gate_in, up_in, down_in))
    ]
    out_load = load(
        large_out.at[
            pl.ds(pl.multiple_of(zy * orows, orows), orows),
            pl.ds(pl.multiple_of(c * ocols, ocols), ocols),
        ],
        oy.at[x, c, z, y],
    )
    conv_loads = [
        load(ref, xin.at[g, pl.ds(HALO, length)])
        for g, ref in enumerate((small_in, large_in, key_in, query_in))
    ]
    small_load = load(small_out, ox.at[pl.ds(pl.multiple_of(x * width_a, width_a), width_a)])
    res_loads = [load(res_in.at[:, k], res.at[k]) for k in range(SIDE)]

    with scope("barrier"):
        pl.semaphore_wait(barrier, len(greeted))

    halo = []
    for g, ref in enumerate((small_in, large_in, key_in, query_in)):
        first = xin.at[g, pl.ds(0, HALO)]
        halo.append(post(ref.at[pl.ds(length - HALO, HALO)], first, first, after))

    def cell(kind, h, first_axis, offset, q=None, m=None, core=c):
        if first_axis:
            zz, yy = (z, turn(y, offset)) if h == 0 else (turn(z, offset), y)
        else:
            zz, yy = (turn(z, offset), slice(None)) if h == 0 else (slice(None), turn(y, offset))
        extent = w.shape[4] if kind == "w" else ocols
        if q is None:
            part = pl.ds(h * (extent // 2), extent // 2)
        else:
            part = pl.ds(h * (extent // 2) + q * (extent // 4), extent // 4)
        if kind == "w":
            return w.at[slice(None) if m is None else m, zz, yy, core, part]
        return oy.at[slice(None), core, zz, yy, slice(None), part]

    def target_of(h, first_axis, d):
        return (ys if (h == 0) == first_axis else zs)[d]

    def spread_over(kind, first_axis, hs=(0, 1), m=None):
        arrivals = []
        for h in hs:
            for d in (1, -1):
                src = cell(kind, h, first_axis, 0, m=m)
                landing = cell(kind, h, first_axis, -d, m=m)
                arrivals.append(post(src, src, landing, target_of(h, first_axis, d)))
        return arrivals

    def forward_over(kind, first_axis, m=None):
        arrivals = []
        for h in (0, 1):
            for d, q in ((1, 0), (-1, 1)):
                src = cell(kind, h, first_axis, -d, q, m)
                landing = cell(kind, h, first_axis, -2 * d, q, m)
                arrivals.append(post(src, src, landing, target_of(h, first_axis, d)))
        return arrivals

    def mirror_over(kind, offsets, m=None):
        arrivals = []
        for h in (0, 1):
            for offset in offsets:
                src = cell(kind, h, False, offset, m=m)
                landing = cell(kind, h, False, offset, m=m, core=1 - c)
                arrivals.append(post(src, src, landing, partner))
        return arrivals

    with scope("out_load"):
        out_load.wait()
    mine_out = oy.at[x, c, z, y]
    o_entry = [
        post(mine_out, mine_out, oy.at[turn(x, -d), c, z, y], xs[d]) for d in (1, -1, 2)
    ]
    with scope("w_loads"):
        for copy in weight_loads:
            copy.wait()
    w_first = spread_over("w", True)

    o_half = width_a // 2

    def xrows(offset, core, q=None):
        base = turn(x, offset) * width_a + core * o_half
        if q is None:
            return ox.at[pl.ds(pl.multiple_of(base, o_half), o_half)]
        quarter = o_half // 2
        return ox.at[pl.ds(pl.multiple_of(base + q * quarter, quarter), quarter)]

    with scope("small_load"):
        small_load.wait()
    x_first = [post(xrows(0, c), xrows(0, c), xrows(-d, c), xs[d]) for d in (1, -1)]

    kernel_len = small_taps.shape[0]
    taps[:, :width_a] = small_taps[...].astype(F32)
    taps[:, width_a:width] = large_taps[...].astype(F32)
    for g, ref in enumerate((key_taps, query_taps)):
        for j in range(ref.shape[1]):
            at = width + (2 * g + j) * state_len
            taps[:, at : at + state_len] = ref[:, j].astype(F32)
    gain[:, :width_a] = small_gain[...].astype(F32).reshape(1, width_a)
    gain[:, width_a:] = large_gain[...].astype(F32).reshape(1, width_b)
    dt_rows[...] = jnp.zeros_like(dt_rows)
    dt_rows[:heads_a] = softplus(small_step[...])
    dt_rows[heads_a : heads_a + heads_b] = softplus(large_step[...])
    head_row = lax.broadcasted_iota(jnp.int32, (SLOTS, BLOCK), 0)
    rate = jnp.zeros((SLOTS, BLOCK), F32)
    for h in range(heads_a + heads_b):
        value = small_decay[h] if h < heads_a else large_decay[h - heads_a]
        rate = jnp.where(head_row == h, value, rate)
    rate = jnp.exp(rate)
    state[...] = jnp.zeros_like(state)
    total[...] = jnp.zeros_like(total)
    row_id = lax.broadcasted_iota(jnp.int32, (BLOCK, BLOCK), 0)
    col_id = lax.broadcasted_iota(jnp.int32, (BLOCK, BLOCK), 1)

    with scope("conv_loads"):
        for copy in conv_loads:
            copy.wait()
    wait_all(o_entry, "o_entry")
    o_first = spread_over("o", True)
    wait_all(halo, "halo")
    for g in range(4):
        edge = xin[g, :HALO].astype(F32)
        xin[g, :HALO] = jnp.where(sp == 0, 0.0, edge).astype(BF16)

    def convolve(g, at):
        for first_lane in range(0, xin.shape[2], LANES):
            here = pl.ds(g * xin.shape[2] + first_lane, LANES)
            extended = xin[g, pl.ds(at, BLOCK + HALO), pl.ds(first_lane, LANES)].astype(F32)
            summed = None
            for k in range(kernel_len):
                first = HALO - kernel_len + 1 + k
                term = taps[k : k + 1, here] * extended[first : first + BLOCK]
                summed = term if summed is None else summed + term
            conv[pl.ds(at, BLOCK), here] = silu(summed).astype(BF16)

    def states(i, carry):
        at = pl.multiple_of(i * BLOCK, BLOCK)
        rows = pl.ds(at, BLOCK)
        for g in range(3):
            convolve(g, at)
        dt = dt_rows[:, rows]
        upper = (row_id <= col_id).astype(F32)
        cum = exact_dot(-dt * rate, upper)
        cum_rows[:, rows] = cum
        tail = cum[:, BLOCK - 1 : BLOCK]
        scale_rows = dt * jnp.exp(tail - cum)
        eye = (row_id == col_id).astype(F32)
        both = exact_dot(
            eye, jnp.concatenate([cum, scale_rows], axis=0), (((1,), (1,)), ((), ()))
        )
        cums[rows] = both[:, :SLOTS]
        scale = both[:, SLOTS:]
        tail_columns = both[BLOCK - 1 : BLOCK, :SLOTS]
        kept = jnp.exp(tail_columns)
        before = total[...]
        logs[i] = jnp.concatenate(
            [spread(before, head_list_a, dim_a), spread(before, head_list_b, dim_b)], axis=1
        )
        for which, (head_list, dim, wide, offset) in enumerate(groups):
            key_at = width + which * state_len
            columns = slice(offset, offset + wide)
            xv = conv[rows, columns].astype(F32)
            u = (xv * spread(scale, head_list, dim)).astype(BF16)
            k = conv[rows, key_at : key_at + state_len]
            fresh = lax.dot_general(k, u, (((0,), (0,)), ((), ())), preferred_element_type=F32)
            old = state[:, columns]
            starts[i, :, columns] = old
            state[:, columns] = old * spread(kept, head_list, dim) + fresh
        total[...] = before + tail_columns
        return carry

    run("conv1", 0, 4, states)
    wait_all(w_first, "w_first")
    w_second = forward_over("w", True)
    wait_all(o_first, "o_first")
    o_second = forward_over("o", True)
    run("conv2", 4, blocks, states)

    half = width // 2

    def half_of(core):
        return pl.ds(pl.multiple_of(core * half, half), half)

    final_log = jnp.concatenate(
        [spread(total[...], head_list_a, dim_a), spread(total[...], head_list_b, dim_b)], axis=1
    )
    pack(packet, None, state[...], final_log)
    swapped = post(packet.at[:, half_of(1 - c)], from_partner, from_partner, partner)

    def queries(i, carry):
        convolve(3, pl.multiple_of(i * BLOCK, BLOCK))
        return carry

    def mix_inside(i, carry):
        at = pl.multiple_of(i * BLOCK, BLOCK)
        rows = pl.ds(at, BLOCK)
        causal = row_id >= col_id
        dt_across = dt_rows[:, rows]
        cum = cums[rows]
        cum_across = cum_rows[:, rows]
        lane = lax.broadcasted_iota(jnp.int32, (BLOCK, LANES), 1)
        for which, (head_list, dim, wide, offset) in enumerate(groups):
            key_at = width + which * state_len
            query_at = key_at + 2 * state_len
            k = conv[rows, key_at : key_at + state_len]
            q = conv[rows, query_at : query_at + state_len]
            scores = lax.dot_general(q, k, (((1,), (1,)), ((), ())), preferred_element_type=F32)
            span = max(dim, LANES)
            per = span // dim
            for first in range(0, len(head_list), per):
                columns = slice(offset + first * dim, offset + first * dim + span)
                x_part = conv[rows, columns]
                part = None
                for j in range(per):
                    h = head_list[first + j]
                    gap = cum[:, h : h + 1] - cum_across[h : h + 1]
                    decays = jnp.exp(jnp.where(causal, gap, FAR))
                    weight = (scores * decays * dt_across[h : h + 1]).astype(BF16)
                    got = jnp.dot(weight, x_part, preferred_element_type=F32)
                    part = got if part is None else jnp.where(lane >= j * dim, got, part)
                inside[rows, columns] = part
        return carry

    def send_along(buffer, targets):
        arrivals = []
        for d, slot in ((1, 1), (-1, 3), (2, 2)):
            landing = buffer.at[slot]
            arrivals.append(post(buffer.at[0], landing, landing, targets[d]))
        return arrivals

    def fold(buffer, place, number):
        zero = jnp.zeros((state_len, half), F32)
        every, every_log = zero, jnp.zeros((1, half), F32)
        ahead, ahead_log = every, every_log
        for p in range(number):
            slot = turn(place, -p)
            one, log = opened(buffer[slot], state_len)
            counts = p < place
            ahead = jnp.where(counts, ahead * jnp.exp(log) + one, ahead)
            ahead_log = jnp.where(counts, ahead_log + log, ahead_log)
            every = every * jnp.exp(log) + one
            every_log = every_log + log
        return every, every_log, ahead, ahead_log

    run("queries", 0, 4, queries)
    wait_all([swapped], "swap_wait")
    mine, mine_log = opened(packet[:, half_of(c)], state_len)
    theirs, theirs_log = opened(from_partner[...], state_len)
    even = c == 0
    a_state = jnp.where(even, mine, theirs)
    a_log = jnp.where(even, mine_log, theirs_log)
    b_state = jnp.where(even, theirs, mine)
    b_log = jnp.where(even, theirs_log, mine_log)
    first_state[...] = a_state
    first_log[...] = a_log
    pack(along_y, 0, a_state * jnp.exp(b_log) + b_state, a_log + b_log)
    y_arrivals = send_along(along_y, ys)
    wait_all(w_second, "w_second")
    wait_all(o_second, "o_second")
    o_third = spread_over("o", False, (1, 0))
    w_third = {m: spread_over("w", False, (1,), m) for m in range(3)}
    o_mirrored = mirror_over("o", (0,))
    w_mirrored = {m: mirror_over("w", (0,), m) for m in range(3)}

    run("queries", 4, blocks, queries)
    run("mix0", 0, 4, mix_inside)
    wait_all(y_arrivals, "y_wait")
    row_all, row_all_log, row_ahead, row_ahead_log = fold(along_y, y, SIDE)
    row_state[...] = row_ahead
    row_log[...] = row_ahead_log
    pack(along_z, 0, row_all, row_all_log)
    z_arrivals = send_along(along_z, zs)
    for m in range(3):
        w_third[m] += spread_over("w", False, (0,), m)
    wait_all(x_first, "x_first")
    x_second, x_mirrored = [], []
    for d, q in ((1, 0), (-1, 1)):
        src = xrows(-d, c, q)
        x_second.append(post(src, src, xrows(-2 * d, c, q), xs[d]))
    for d in (1, -1):
        src = xrows(d, c)
        x_mirrored.append(post(src, src, xrows(d, 1 - c), partner))

    run("mix4", 4, blocks, mix_inside)
    wait_all(z_arrivals, "z_wait")
    _, _, plane_ahead, _ = fold(along_z, z, SIDE - 1)
    chip = plane_ahead * jnp.exp(row_log[...]) + row_state[...]
    second = chip * jnp.exp(first_log[...]) + first_state[...]
    entering[:, half_of(c)] = jnp.where(even, chip, second)
    for_partner[...] = jnp.where(even, second, chip)
    entered = post(
        for_partner, entering.at[:, half_of(c)], entering.at[:, half_of(1 - c)], partner
    )
    wait_all([entered], "enter_wait")

    sub = length // (SIDE * SIDE)
    lane = lax.broadcasted_iota(jnp.int32, (BLOCK, LANES), 1)

    def carry_block(n, carry):
        stage = n // SIDE
        d = lax.rem(n, SIDE)
        i = 2 * d + stage
        rows = pl.ds(pl.multiple_of(i * BLOCK, BLOCK), BLOCK)
        grown = jnp.exp(cums[rows])
        for which, (head_list, dim, wide, offset) in enumerate(groups):
            columns = slice(offset, offset + wide)
            query_at = width + (2 + which) * state_len
            q = conv[rows, query_at : query_at + state_len]
            old = starts[i, :, columns] + entering[:, columns] * jnp.exp(logs[i, :, columns])
            carried = jnp.dot(q, old.astype(BF16), preferred_element_type=F32)
            mixed = inside[rows, columns] + carried * spread(grown, head_list, dim)
            gate = (small_gate, large_gate)[which]
            gated = mixed * silu(gate[rows].astype(F32))
            squares = gated * gated
            span = max(dim, LANES)
            per = span // dim
            normed = []
            for first in range(0, len(head_list), per):
                at = first * dim
                part = squares[:, at : at + span]
                means = None
                for j in range(per):
                    if per == 1:
                        means = jnp.sum(part, axis=1, keepdims=True)
                    else:
                        ours = (lane >= j * dim) & (lane < (j + 1) * dim)
                        one = jnp.sum(jnp.where(ours, part, 0.0), axis=1, keepdims=True)
                        means = one if means is None else jnp.where(lane >= j * dim, one, means)
                normed.append(gated[:, at : at + span] * lax.rsqrt(means * (1.0 / dim) + EPS))
            normed = (jnp.concatenate(normed, axis=1) * gain[:, columns]).astype(BF16)
            place = pl.ds(pl.multiple_of(x * wide, LANES), wide)
            spot = pl.ds(pl.multiple_of(d * sub, sub), sub)
            heads[2 * stage, which, spot, place] = normed[:sub]
            heads[2 * stage + 1, which, spot, place] = normed[sub:]
        return carry

    def hcols(offset):
        return pl.ds(pl.multiple_of(turn(x, offset) * width_a, LANES), width_a)

    step_rows = heads.shape[2]
    g1 = {d: counter.take(SIDE) for d in (1, -1)}
    g2 = {d: counter.take(SIDE) for d in (1, -1)}

    def heads_out(k, d):
        src = heads.at[k, :, :, hcols(0)]
        return message(src, src, xs[d], g1[d] + k)

    def heads_in(k, d):
        landing = heads.at[k, :, :, hcols(-d)]
        return message(landing, landing, xs[d], g1[d] + k)

    def far_rows(d):
        return pl.ds(0 if d == 1 else step_rows // 2, step_rows // 2)

    def heads_on(k, d):
        src = heads.at[k, :, far_rows(d), hcols(-d)]
        return message(src, src, xs[d], g2[d] + k)

    def heads_far(k, d):
        landing = heads.at[k, :, far_rows(d), hcols(-2 * d)]
        return message(landing, landing, xs[d], g2[d] + k)

    def start_heads(k):
        for d in (1, -1):
            heads_out(k, d).start()

    def forward_heads(k):
        with scope("heads_in"):
            for d in (1, -1):
                heads_in(k, d).wait_recv()
        for d in (1, -1):
            heads_on(k, d).start()

    features = res.shape[3]
    hid = hidden.shape[1]
    side_half = features // 2
    r1 = {d: counter.take(SIDE) for d in (1, -1)}
    r2 = {d: counter.take(SIDE) for d in (1, -1)}

    def prow(offset):
        return pl.ds(pl.multiple_of(turn(x, offset) * sub, sub), sub)

    def project(k):
        with scope("heads_far"):
            for d in (1, -1):
                heads_far(k, d).wait_recv()
        with scope("out_dot"):
            left_a = heads[k, 0]
            left_b = heads[k, 1]
            depth_b = SIDE * SIDE * SIDE * orows
            for first, size in tile_list(features, 512):
                got = jnp.dot(left_a, ox[:, first : first + size], preferred_element_type=F32)
                inner = first % ocols
                right = oy[:, first // ocols, :, :, :, inner : inner + size]
                got = got + jnp.dot(
                    left_b, right.reshape(depth_b, size), preferred_element_type=F32
                )
                mixbuf[:, first : first + size] = got
        with scope("norms"):
            outer = mixer_gain[...].astype(F32).reshape(1, features)
            inner = in_gain[...].astype(F32).reshape(1, features)
            for d in range(SIDE):
                rows = slice(d * sub, (d + 1) * sub)
                mixed = res[k, d].astype(F32) + unit_rms(mixbuf[rows]) * outer
                mixbuf[rows] = mixed
                ninbuf[(k % 2), rows] = (unit_rms(mixed) * inner).astype(BF16)
            ownmix[k] = mixbuf[prow(0)]

    run("carry1", 0, SIDE, carry_block)
    start_heads(0)
    start_heads(1)
    wait_all(o_third, "o_third")
    o_fourth = forward_over("o", False)
    o_mirrored += mirror_over("o", (1, -1))
    wait_all(x_second, "x_second")
    src = xrows(2, c)
    x_mirrored.append(post(src, src, xrows(2, 1 - c), partner))
    run("carry2", SIDE, 2 * SIDE, carry_block)
    w_fourth = {}

    def pass_weights(m):
        wait_all(w_third[m], "w_third")
        w_fourth[m] = forward_over("w", False, m)
        w_mirrored[m] += mirror_over("w", (1, -1), m)

    def settle_weights(m):
        wait_all(w_fourth[m], "w_fourth")
        w_mirrored[m] += mirror_over("w", (2,), m)

    forward_heads(0)
    start_heads(2)
    wait_all(o_fourth, "o_fourth")
    o_mirrored += mirror_over("o", (2,))
    pass_weights(0)
    forward_heads(1)
    start_heads(3)
    pass_weights(1)
    for copy in res_loads:
        copy.wait()
    wait_all(x_mirrored, "x_mirrored")
    wait_all(o_mirrored, "o_mirrored")
    project(0)
    pass_weights(2)
    forward_heads(2)
    settle_weights(0)
    project(1)
    forward_heads(3)
    settle_weights(1)
    wait_all(w_mirrored[0] + w_mirrored[1], "w_mirrored")

    def far_out(k, d):
        lanes = pl.ds(0 if d == 1 else side_half, side_half)
        landing = (ra if d == 1 else rb).at[k]
        return message(parts.at[k, prow(2), lanes], landing, xs[d], r1[d] + k)

    def near_out(k, d):
        landing = (rc if d == 1 else rd).at[k]
        return message(parts.at[k, prow(d)], landing, xs[d], r2[d] + k)

    def pass_on(k):
        for d in (1, -1):
            with scope("far_wait"):
                far_out(k, d).wait_recv()
            lanes = slice(0, side_half) if d == 1 else slice(side_half, features)
            extra = (ra if d == 1 else rb)[k].astype(F32)
            mine = parts[k, prow(d), lanes].astype(F32)
            parts[k, prow(d), lanes] = (mine + extra).astype(BF16)
            near_out(k, d).start()

    def gate_up(k):
        with scope("gate_up"):
            nin = ninbuf[(k % 2)]
            for first, size in tile_list(hid, 512):
                wg = w[0, :, :, :, :, first : first + size].reshape(features, size)
                wu = w[1, :, :, :, :, first : first + size].reshape(features, size)
                gate = jnp.dot(nin, wg, preferred_element_type=F32)
                up = jnp.dot(nin, wu, preferred_element_type=F32)
                hidden[:, first : first + size] = (silu(gate) * up).astype(BF16)

    def down(k):
        with scope("down"):
            hv = hidden[...]
            tile = features // SIDE
            for n in range(SIDE):
                wd = w[2, n].reshape(tile, hid)
                got = lax.dot_general(hv, wd, (((1,), (1,)), ((), ())), preferred_element_type=F32)
                parts[k, :, n * tile : (n + 1) * tile] = got.astype(BF16)
            for d in (1, -1):
                far_out(k, d).start()

    def channel_mix(k, carry):
        down(k)

        @pl.when(k < 2)
        def _():
            project(k + 2)

        @pl.when(k < SIDE - 1)
        def _():
            gate_up(k + 1)
            pass_on(k)

        return carry

    gate_up(0)
    settle_weights(2)
    wait_all(w_mirrored[2], "w_mirrored2")
    lax.fori_loop(0, SIDE, channel_mix, 0)
    outer = 0.5 * out_gain[...].astype(F32).reshape(1, features)

    def finish(k):
        with scope("near_wait"):
            for d in (1, -1):
                near_out(k, d).wait_recv()
        ffn = parts[k, prow(0)].astype(F32) + rc[k].astype(F32) + rd[k].astype(F32)
        updated = ownmix[k] + unit_rms(ffn) * outer
        out[k * sub : (k + 1) * sub] = updated.astype(BF16)

    finish(0)
    finish(1)
    pass_on(SIDE - 1)
    finish(2)
    finish(SIDE - 1)

    with scope("drain"):
        for copy in issued:
            copy.wait_send()

    def drain(k, carry):
        for d in (1, -1):
            heads_out(k, d).wait_send()
            heads_on(k, d).wait_send()
            far_out(k, d).wait_send()
            near_out(k, d).wait_send()
        return carry

    lax.fori_loop(0, SIDE, drain, 0)


def local_program(
    residual,
    small_heads,
    large_heads,
    state_keys,
    state_queries,
    small_gate,
    large_gate,
    small_step,
    large_step,
    small_taps,
    large_taps,
    key_taps,
    query_taps,
    small_decay,
    large_decay,
    small_gain,
    large_gain,
    small_out,
    large_out,
    mixer_gain,
    ffn_in_gain,
    gate_proj,
    up_proj,
    down_proj,
    ffn_out_gain,
):
    length, features = residual.shape
    state_len = state_keys.shape[-1]
    key_rows = state_keys.reshape(length, -1)
    query_rows = state_queries.reshape(length, -1)
    heads_a = small_step.shape[1]
    heads_b = large_step.shape[1]
    heads = heads_a + heads_b
    width_a = small_heads.shape[1]
    width_b = large_heads.shape[1]
    width = width_a + width_b
    everything = width + key_rows.shape[1] + query_rows.shape[1]
    blocks = length // BLOCK
    sizes = ((heads_a, width_a // heads_a), (heads_b, width_b // heads_b), state_len, blocks)
    kernel_len = small_taps.shape[0]
    sub = length // (SIDE * SIDE)
    step_rows = SIDE * sub
    wrows, hid = gate_proj.shape
    half = width // 2
    packet_rows = state_len + TAIL
    any_space = pl.BlockSpec(memory_space=pl.ANY)
    vmem = pl.BlockSpec(memory_space=pltpu.VMEM)
    smem = pl.BlockSpec(memory_space=pltpu.SMEM)
    messages = 160

    return pl.pallas_call(
        functools.partial(whole_kernel, sizes),
        in_specs=[any_space] * 5
        + [vmem] * 4
        + [smem] * 2
        + [vmem] * 6
        + [any_space] * 2
        + [vmem] * 3
        + [any_space] * 3,
        out_specs=vmem,
        out_shape=jax.ShapeDtypeStruct((length // SIDE, features), BF16),
        scratch_shapes=[
            pltpu.VMEM((4, HALO + length, width_a), BF16),
            pltpu.VMEM((length, everything), BF16),
            pltpu.VMEM((kernel_len, everything), F32),
            pltpu.VMEM((1, width), F32),
            pltpu.VMEM((SLOTS, length), F32),
            pltpu.VMEM((SLOTS, length), F32),
            pltpu.VMEM((length, SLOTS), F32),
            pltpu.VMEM((blocks, 1, width), F32),
            pltpu.VMEM((blocks, state_len, width), F32),
            pltpu.VMEM((length, width), F32),
            pltpu.VMEM((state_len, width), F32),
            pltpu.VMEM((1, SLOTS), F32),
            pltpu.VMEM((packet_rows, width), BF16),
            pltpu.VMEM((packet_rows, half), BF16),
            pltpu.VMEM((state_len, half), F32),
            pltpu.VMEM((1, half), F32),
            pltpu.VMEM((SIDE, packet_rows, half), BF16),
            pltpu.VMEM((SIDE, packet_rows, half), BF16),
            pltpu.VMEM((state_len, half), F32),
            pltpu.VMEM((1, half), F32),
            pltpu.VMEM((state_len, width), F32),
            pltpu.VMEM((state_len, half), F32),
            pltpu.VMEM((3, SIDE, SIDE, 2, wrows, hid), BF16),
            pltpu.VMEM((SIDE * width_a, features), BF16),
            pltpu.VMEM(
                (SIDE, 2, SIDE, SIDE, width_b // (SIDE * SIDE), features // 2), BF16
            ),
            pltpu.VMEM((SIDE, 2, step_rows, SIDE * width_a), BF16),
            pltpu.VMEM((SIDE, SIDE, sub, features), BF16),
            pltpu.VMEM((step_rows, features), F32),
            pltpu.VMEM((SIDE, sub, features), F32),
            pltpu.VMEM((2, step_rows, features), BF16),
            pltpu.VMEM((step_rows, hid), BF16),
            pltpu.VMEM((SIDE, step_rows, features), BF16),
            pltpu.VMEM((SIDE, sub, features // 2), BF16),
            pltpu.VMEM((SIDE, sub, features // 2), BF16),
            pltpu.VMEM((SIDE, sub, features), BF16),
            pltpu.VMEM((SIDE, sub, features), BF16),
            pltpu.SemaphoreType.DMA((messages,)),
            pltpu.SemaphoreType.DMA((messages,)),
            pltpu.SemaphoreType.DMA((16,)),
        ],
        compiler_params=pltpu.CompilerParams(
            collective_id=0, has_side_effects=True, vmem_limit_bytes=VMEM_LIMIT
        ),
        cost_estimate=pl.CostEstimate(
            flops=40_000_000_000, bytes_accessed=60_000_000, transcendentals=0
        ),
        name="layer",
    )(
        residual.reshape(SIDE, SIDE, sub, features),
        small_heads,
        large_heads,
        key_rows,
        query_rows,
        small_gate,
        large_gate,
        small_step.T,
        large_step.T,
        small_decay,
        large_decay,
        small_taps,
        large_taps,
        key_taps,
        query_taps,
        small_gain,
        large_gain,
        small_out,
        large_out,
        mixer_gain,
        ffn_in_gain,
        ffn_out_gain,
        gate_proj,
        up_proj,
        down_proj,
    )


def solution(mesh):
    placed = (
        P("sp", None),
        P("sp", "tp"),
        P("sp", "tp"),
        P("sp", "tp", None),
        P("sp", "tp", None),
        P("sp", "tp"),
        P("sp", "tp"),
        P("sp", "tp"),
        P("sp", "tp"),
        P(None, "tp"),
        P(None, "tp"),
        P(None, "tp", None),
        P(None, "tp", None),
        P("tp"),
        P("tp"),
        P("tp"),
        P("tp"),
        P("tp", None),
        P("tp", None),
        P(),
        P(),
        P("sp", "tp"),
        P("sp", "tp"),
        P("sp", "tp"),
        P(),
    )
    return jax.shard_map(
        local_program, mesh=mesh, in_specs=placed, out_specs=P(("sp", "tp"), None), check_vma=False
    )
```

```python
import functools

import jax
import jax.numpy as jnp
from jax import lax
from jax.experimental import pallas as pl
from jax.experimental.pallas import tpu as pltpu
from jax.sharding import PartitionSpec as P

BLOCK = 128
HALO = 16
LANES = 128
SLOTS = 8
TAIL = 16
SIDE = 4

EPS = 1e-06
FAR = -1e30
F32 = jnp.float32
BF16 = jnp.bfloat16
MESH = pl.DeviceIdType.MESH
scope = jax.named_scope
VMEM_LIMIT = 66_000_000


def silu(x):
    return x / (1.0 + jnp.exp(-x))


def softplus(x):
    return jnp.maximum(x, 0.0) + jnp.log1p(jnp.exp(-jnp.abs(x)))


def exact_dot(a, b, dims=(((1,), (0,)), ((), ()))):
    return lax.dot_general(a, b, dims, precision=lax.Precision.HIGHEST, preferred_element_type=F32)


def lower(n):
    rows = lax.broadcasted_iota(jnp.int32, (n, n), 0)
    return rows >= lax.broadcasted_iota(jnp.int32, (n, n), 1)


def spread(columns, heads, dim):
    rows = columns.shape[0]
    parts = []
    if dim >= LANES:
        for h in heads:
            parts.append(jnp.broadcast_to(columns[:, h : h + 1], (rows, dim)))
    else:
        per = LANES // dim
        lane = lax.broadcasted_iota(jnp.int32, (rows, LANES), 1)
        for first in range(0, len(heads), per):
            part = jnp.broadcast_to(columns[:, heads[first] : heads[first] + 1], (rows, LANES))
            for j in range(1, per):
                h = heads[first + j]
                part = jnp.where(lane >= j * dim, columns[:, h : h + 1], part)
            parts.append(part)
    return jnp.concatenate(parts, axis=1)


def unit_rms(values):
    return values * lax.rsqrt(jnp.mean(values * values, axis=-1, keepdims=True) + EPS)


def pack(ref, slot, state, log):
    rows = state.shape[0]
    high = log.astype(BF16).astype(F32)
    row = lax.broadcasted_iota(jnp.int32, (TAIL, log.shape[1]), 0)
    both = jnp.where(row == 0, high, jnp.where(row == 1, log - high, 0.0))
    if slot is None:
        ref[:rows] = state.astype(BF16)
        ref[rows:] = both.astype(BF16)
    else:
        ref[slot, :rows] = state.astype(BF16)
        ref[slot, rows:] = both.astype(BF16)


def opened(packet, rows):
    log = packet[rows : rows + TAIL].astype(F32)
    return packet[:rows].astype(F32), log[0:1] + log[1:2]


class Counter:
    def __init__(self):
        self.n = 0

    def take(self, count=1):
        first = self.n
        self.n += count
        return first


def tile_list(width, tile):
    return [(s, min(tile, width - s)) for s in range(0, width, tile)]


def whole_kernel(
    sizes,
    res_in,
    small_in,
    large_in,
    key_in,
    query_in,
    small_gate,
    large_gate,
    small_step,
    large_step,
    small_decay,
    large_decay,
    small_taps,
    large_taps,
    key_taps,
    query_taps,
    small_gain,
    large_gain,
    small_out,
    large_out,
    mixer_gain,
    in_gain,
    out_gain,
    gate_in,
    up_in,
    down_in,
    out,
    xin,
    conv,
    taps,
    gain,
    dt_rows,
    cum_rows,
    cums,
    logs,
    tails,
    starts,
    inside,
    state,
    total,
    packet,
    from_partner,
    first_state,
    first_log,
    along_y,
    along_z,
    row_state,
    row_log,
    entering,
    for_partner,
    w,
    o,
    heads,
    res,
    mixbuf,
    ninbuf,
    hidden,
    parts,
    ra,
    rb,
    rc,
    rd,
    send,
    recv,
    local,
):
    (heads_a, dim_a), (heads_b, dim_b), state_len, blocks = sizes
    head_list_a = list(range(heads_a))
    head_list_b = list(range(heads_a, heads_a + heads_b))
    width_a = heads_a * dim_a
    width_b = heads_b * dim_b
    width = width_a + width_b
    groups = (
        (head_list_a, dim_a, width_a, 0),
        (head_list_b, dim_b, width_b, width_a),
    )

    sp = lax.axis_index("sp")
    x = lax.axis_index("tp")
    c = lax.rem(sp, 2)
    y = lax.rem(sp // 2, SIDE)
    z = sp // (2 * SIDE)
    zy = sp // 2
    count_sp = lax.axis_size("sp")

    def turn(v, d):
        return lax.rem(v + d + SIDE, SIDE)

    def at_chip(zz, yy):
        return ((zz * SIDE + yy) * 2 + c, x)

    partner = (sp + 1 - 2 * c, x)
    xs = {d: (sp, turn(x, d)) for d in (1, -1, 2)}
    ys = {d: at_chip(z, turn(y, d)) for d in (1, -1, 2)}
    zs = {d: at_chip(turn(z, d), y) for d in (1, -1, 2)}
    after = (lax.rem(sp + 1, count_sp), x)
    prior = (lax.rem(sp + count_sp - 1, count_sp), x)

    barrier = pltpu.get_barrier_semaphore()
    greeted = [partner, after, prior] + [v[d] for v in (xs, ys, zs) for d in (1, -1, 2)]
    for peer in greeted:
        pl.semaphore_signal(barrier, inc=1, device_id=peer, device_id_type=MESH)

    counter = Counter()
    issued = []

    def message(src, dst, target, index):
        return pltpu.make_async_remote_copy(
            src_ref=src,
            dst_ref=dst,
            send_sem=send.at[index],
            recv_sem=recv.at[index],
            device_id=target,
            device_id_type=MESH,
        )

    def post(src, dst, landing, target):
        index = counter.take()
        copy = message(src, dst, target, index)
        copy.start()
        issued.append(copy)
        return message(landing, landing, target, index)

    def wait_all(arrivals, name="wait"):
        with scope(name):
            for arrival in arrivals:
                arrival.wait_recv()

    def run(name, first, last, body):
        with scope(name):
            lax.fori_loop(first, last, body, 0)

    loads = []

    def load(src, dst):
        copy = pltpu.make_async_copy(src, dst, local.at[len(loads)])
        copy.start()
        loads.append(copy)
        return copy

    length = small_in.shape[0]
    weight_loads = [
        load(ref, w.at[m, z, y, c]) for m, ref in enumerate((gate_in, up_in, down_in))
    ]
    conv_loads = [
        load(ref, xin.at[g, pl.ds(HALO, length)])
        for g, ref in enumerate((small_in, large_in, key_in, query_in))
    ]
    out_loads = [
        load(ref, o.at[pl.ds(pl.multiple_of(x * width + first, width_a), width_a)])
        for ref, first in ((small_out, 0), (large_out, width_a))
    ]
    res_loads = [load(res_in.at[:, k], res.at[k]) for k in range(SIDE)]

    with scope("barrier"):
        pl.semaphore_wait(barrier, len(greeted))

    halo = []
    for g, ref in enumerate((small_in, large_in, key_in, query_in)):
        first = xin.at[g, pl.ds(0, HALO)]
        halo.append(post(ref.at[pl.ds(length - HALO, HALO)], first, first, after))

    def cell(h, first_axis, offset, q=None, m=None, core=c):
        if first_axis:
            zz, yy = (z, turn(y, offset)) if h == 0 else (turn(z, offset), y)
        else:
            zz, yy = (turn(z, offset), slice(None)) if h == 0 else (slice(None), turn(y, offset))
        extent = w.shape[4]
        if q is None:
            part = pl.ds(h * (extent // 2), extent // 2)
        else:
            part = pl.ds(h * (extent // 2) + q * (extent // 4), extent // 4)
        return w.at[slice(None) if m is None else m, zz, yy, core, part]

    def target_of(h, first_axis, d):
        return (ys if (h == 0) == first_axis else zs)[d]

    def spread_over(first_axis, hs=(0, 1), m=None):
        arrivals = []
        for h in hs:
            for d in (1, -1):
                src = cell(h, first_axis, 0, m=m)
                landing = cell(h, first_axis, -d, m=m)
                arrivals.append(post(src, src, landing, target_of(h, first_axis, d)))
        return arrivals

    def forward_over(first_axis, m=None, hs=(0, 1)):
        arrivals = []
        for h in hs:
            for d, q in ((1, 0), (-1, 1)):
                src = cell(h, first_axis, -d, q, m)
                landing = cell(h, first_axis, -2 * d, q, m)
                arrivals.append(post(src, src, landing, target_of(h, first_axis, d)))
        return arrivals

    def mirror_over(offsets, m=None):
        arrivals = []
        for h in (0, 1):
            for offset in offsets:
                src = cell(h, False, offset, m=m)
                landing = cell(h, False, offset, m=m, core=1 - c)
                arrivals.append(post(src, src, landing, partner))
        return arrivals

    with scope("loads"):
        for copy in weight_loads + out_loads:
            copy.wait()
    w_first = spread_over(True)

    o_part = width // 4

    def orows(offset, core, q):
        base = turn(x, offset) * width + core * 2 * o_part
        if q is None:
            return o.at[pl.ds(pl.multiple_of(base, o_part), 2 * o_part)]
        return o.at[pl.ds(pl.multiple_of(base + q * o_part, o_part), o_part)]

    sides = ((1, 0), (-1, 1))
    o_first, o_rest = [], []
    for arrivals, flip in ((o_first, False), (o_rest, True)):
        for d, q in sides:
            part = 1 - q if flip else q
            arrivals.append(post(orows(0, c, part), orows(0, c, part), orows(-d, c, part), xs[d]))

    kernel_len = small_taps.shape[0]
    taps[:, :width_a] = small_taps[...].astype(F32)
    taps[:, width_a:width] = large_taps[...].astype(F32)
    for g, ref in enumerate((key_taps, query_taps)):
        for j in range(ref.shape[1]):
            at = width + (2 * g + j) * state_len
            taps[:, at : at + state_len] = ref[:, j].astype(F32)
    gain[:, :width_a] = small_gain[...].astype(F32).reshape(1, width_a)
    gain[:, width_a:] = large_gain[...].astype(F32).reshape(1, width_b)
    dt_rows[...] = jnp.zeros_like(dt_rows)
    dt_rows[:heads_a] = softplus(small_step[...])
    dt_rows[heads_a : heads_a + heads_b] = softplus(large_step[...])
    head_row = lax.broadcasted_iota(jnp.int32, (SLOTS, BLOCK), 0)
    rate = jnp.zeros((SLOTS, BLOCK), F32)
    for h in range(heads_a + heads_b):
        value = small_decay[h] if h < heads_a else large_decay[h - heads_a]
        rate = jnp.where(head_row == h, value, rate)
    rate = jnp.exp(rate)
    row_id = lax.broadcasted_iota(jnp.int32, (BLOCK, BLOCK), 0)
    col_id = lax.broadcasted_iota(jnp.int32, (BLOCK, BLOCK), 1)
    with scope("decays"):
        pieces = [dt_rows[:, i * BLOCK : (i + 1) * BLOCK] for i in range(blocks)]
        dt_all = jnp.concatenate(pieces, axis=0)
        rate_all = jnp.concatenate([rate] * blocks, axis=0)
        cum_all = exact_dot(-dt_all * rate_all, (row_id <= col_id).astype(F32))
        scale_all = dt_all * jnp.exp(cum_all[:, BLOCK - 1 : BLOCK] - cum_all)
        eye = (row_id == col_id).astype(F32)
        turned = exact_dot(
            eye, jnp.concatenate([cum_all, scale_all], axis=0), (((1,), (1,)), ((), ()))
        )
        before = jnp.zeros((1, SLOTS), F32)
        for i in range(blocks):
            rows = slice(i * BLOCK, (i + 1) * BLOCK)
            heads_at = slice(i * SLOTS, (i + 1) * SLOTS)
            scales_at = slice((blocks + i) * SLOTS, (blocks + i + 1) * SLOTS)
            cum_rows[:, rows] = cum_all[heads_at]
            cums[rows, :SLOTS] = turned[:, heads_at]
            cums[rows, SLOTS:] = turned[:, scales_at]
            tail = turned[BLOCK - 1 : BLOCK, heads_at]
            for buffer, value in ((logs, before), (tails, tail)):
                buffer[i] = jnp.concatenate(
                    [spread(value, head_list_a, dim_a), spread(value, head_list_b, dim_b)], axis=1
                )
            before = before + tail
        final_log = jnp.concatenate(
            [spread(before, head_list_a, dim_a), spread(before, head_list_b, dim_b)], axis=1
        )
        total[...] = final_log
    state[...] = jnp.zeros_like(state)

    with scope("conv_loads"):
        for copy in conv_loads:
            copy.wait()
    def convolve(g, at):
        for first_lane in range(0, xin.shape[2], LANES):
            here = pl.ds(g * xin.shape[2] + first_lane, LANES)
            extended = xin[g, pl.ds(at, BLOCK + HALO), pl.ds(first_lane, LANES)].astype(F32)
            summed = None
            for k in range(kernel_len):
                first = HALO - kernel_len + 1 + k
                term = taps[k : k + 1, here] * extended[first : first + BLOCK]
                summed = term if summed is None else summed + term
            conv[pl.ds(at, BLOCK), here] = silu(summed).astype(BF16)

    def convolve_three(i, carry):
        for g in range(3):
            convolve(g, pl.multiple_of(i * BLOCK, BLOCK))
        return carry

    def states(i, carry):
        at = pl.multiple_of(i * BLOCK, BLOCK)
        rows = pl.ds(at, BLOCK)
        scale = cums[rows, SLOTS:]
        kept = jnp.exp(tails[i])
        for which, (head_list, dim, wide, offset) in enumerate(groups):
            key_at = width + which * state_len
            columns = slice(offset, offset + wide)
            heads_here = list(range(len(head_list)))
            shifted = scale[:, head_list[0] : head_list[-1] + 1]
            xv = conv[rows, columns].astype(F32)
            u = (xv * spread(shifted, heads_here, dim)).astype(BF16)
            k = conv[rows, key_at : key_at + state_len]
            fresh = lax.dot_general(k, u, (((0,), (0,)), ((), ())), preferred_element_type=F32)
            old = state[:, columns]
            starts[i, :, columns] = old
            state[:, columns] = old * kept[:, columns] + fresh
        return carry

    run("conv1", 1, blocks, convolve_three)
    wait_all(halo, "halo")
    for g in range(4):
        edge = xin[g, :HALO].astype(F32)
        xin[g, :HALO] = jnp.where(sp == 0, 0.0, edge).astype(BF16)
    run("conv0", 0, 1, convolve_three)
    run("states", 0, blocks, states)

    half = width // 2

    def half_of(core):
        return pl.ds(pl.multiple_of(core * half, half), half)

    pack(packet, None, state[...], total[...])
    swapped = post(packet.at[:, half_of(1 - c)], from_partner, from_partner, partner)

    def queries(i, carry):
        convolve(3, pl.multiple_of(i * BLOCK, BLOCK))
        return carry

    def mix_inside(i, carry):
        at = pl.multiple_of(i * BLOCK, BLOCK)
        rows = pl.ds(at, BLOCK)
        causal = row_id >= col_id
        dt_across = dt_rows[:, rows]
        cum = cums[rows]
        cum_across = cum_rows[:, rows]
        lane = lax.broadcasted_iota(jnp.int32, (BLOCK, LANES), 1)
        for which, (head_list, dim, wide, offset) in enumerate(groups):
            key_at = width + which * state_len
            query_at = key_at + 2 * state_len
            k = conv[rows, key_at : key_at + state_len]
            q = conv[rows, query_at : query_at + state_len]
            scores = lax.dot_general(q, k, (((1,), (1,)), ((), ())), preferred_element_type=F32)
            span = max(dim, LANES)
            per = span // dim
            for first in range(0, len(head_list), per):
                columns = slice(offset + first * dim, offset + first * dim + span)
                x_part = conv[rows, columns]
                part = None
                for j in range(per):
                    h = head_list[first + j]
                    gap = cum[:, h : h + 1] - cum_across[h : h + 1]
                    decays = jnp.exp(jnp.where(causal, gap, FAR))
                    weight = (scores * decays * dt_across[h : h + 1]).astype(BF16)
                    got = jnp.dot(weight, x_part, preferred_element_type=F32)
                    part = got if part is None else jnp.where(lane >= j * dim, got, part)
                inside[rows, columns] = part
        return carry

    def send_along(buffer, targets):
        arrivals = []
        for d, slot in ((1, 1), (-1, 3), (2, 2)):
            landing = buffer.at[slot]
            arrivals.append(post(buffer.at[0], landing, landing, targets[d]))
        return arrivals

    def fold(buffer, place, number):
        zero = jnp.zeros((state_len, half), F32)
        every, every_log = zero, jnp.zeros((1, half), F32)
        ahead, ahead_log = every, every_log
        for p in range(number):
            slot = turn(place, -p)
            one, log = opened(buffer[slot], state_len)
            counts = p < place
            ahead = jnp.where(counts, ahead * jnp.exp(log) + one, ahead)
            ahead_log = jnp.where(counts, ahead_log + log, ahead_log)
            every = every * jnp.exp(log) + one
            every_log = every_log + log
        return every, every_log, ahead, ahead_log

    wait_all(w_first[2:], "w_first_z")
    w_second_z = forward_over(True, hs=(1,))
    run("queries", 0, blocks, queries)
    wait_all([swapped], "swap_wait")
    mine, mine_log = opened(packet[:, half_of(c)], state_len)
    theirs, theirs_log = opened(from_partner[...], state_len)
    even = c == 0
    a_state = jnp.where(even, mine, theirs)
    a_log = jnp.where(even, mine_log, theirs_log)
    b_state = jnp.where(even, theirs, mine)
    b_log = jnp.where(even, theirs_log, mine_log)
    first_state[...] = a_state
    first_log[...] = a_log
    pack(along_y, 0, a_state * jnp.exp(b_log) + b_state, a_log + b_log)
    y_arrivals = send_along(along_y, ys)
    wait_all(w_first[:2], "w_first_y")
    w_second_y = forward_over(True, hs=(0,))
    run("mix0", 0, 4, mix_inside)
    wait_all(w_second_z, "w_second_z")
    w_third = {m: spread_over(False, (1,), m) for m in (0, 1)}
    wait_all(o_first, "o_first")
    o_second = []
    for d, q in sides:
        src = orows(-d, c, q)
        o_second.append(post(src, src, orows(-2 * d, c, q), xs[d]))
    wait_all(y_arrivals, "y_wait")
    row_all, row_all_log, row_ahead, row_ahead_log = fold(along_y, y, SIDE)
    row_state[...] = row_ahead
    row_log[...] = row_ahead_log
    pack(along_z, 0, row_all, row_all_log)
    z_arrivals = send_along(along_z, zs)
    run("mix4", 4, 6, mix_inside)
    wait_all(w_second_y, "w_second_y")
    for m in (0, 1):
        w_third[m] += spread_over(False, (0,), m)
    run("mix6", 6, blocks, mix_inside)
    wait_all(z_arrivals, "z_wait")
    _, _, plane_ahead, _ = fold(along_z, z, SIDE - 1)
    chip = plane_ahead * jnp.exp(row_log[...]) + row_state[...]
    second = chip * jnp.exp(first_log[...]) + first_state[...]
    entering[:, half_of(c)] = jnp.where(even, chip, second)
    for_partner[...] = jnp.where(even, second, chip)
    entered = post(
        for_partner, entering.at[:, half_of(c)], entering.at[:, half_of(1 - c)], partner
    )
    w_mirrored = {m: mirror_over((0,), m) for m in range(3)}

    sub = length // (SIDE * SIDE)
    lane = lax.broadcasted_iota(jnp.int32, (BLOCK, LANES), 1)

    def carry_block(n, carry):
        stage = n // SIDE
        d = lax.rem(n, SIDE)
        i = 2 * d + stage
        rows = pl.ds(pl.multiple_of(i * BLOCK, BLOCK), BLOCK)
        grown = jnp.exp(cums[rows])
        for which, (head_list, dim, wide, offset) in enumerate(groups):
            columns = slice(offset, offset + wide)
            query_at = width + (2 + which) * state_len
            q = conv[rows, query_at : query_at + state_len]
            old = starts[i, :, columns] + entering[:, columns] * jnp.exp(logs[i, :, columns])
            carried = jnp.dot(q, old.astype(BF16), preferred_element_type=F32)
            mixed = inside[rows, columns] + carried * spread(grown, head_list, dim)
            gate = (small_gate, large_gate)[which]
            gated = mixed * silu(gate[rows].astype(F32))
            squares = gated * gated
            span = max(dim, LANES)
            per = span // dim
            normed = []
            for first in range(0, len(head_list), per):
                at = first * dim
                part = squares[:, at : at + span]
                means = None
                for j in range(per):
                    if per == 1:
                        means = jnp.sum(part, axis=1, keepdims=True)
                    else:
                        ours = (lane >= j * dim) & (lane < (j + 1) * dim)
                        one = jnp.sum(jnp.where(ours, part, 0.0), axis=1, keepdims=True)
                        means = one if means is None else jnp.where(lane >= j * dim, one, means)
                normed.append(gated[:, at : at + span] * lax.rsqrt(means * (1.0 / dim) + EPS))
            normed = (jnp.concatenate(normed, axis=1) * gain[:, columns]).astype(BF16)
            place = pl.ds(pl.multiple_of(x * width + offset, LANES), wide)
            spot = pl.ds(pl.multiple_of(d * sub, sub), sub)
            heads[2 * stage, spot, place] = normed[:sub]
            heads[2 * stage + 1, spot, place] = normed[sub:]
        return carry

    def hcols(offset):
        return pl.ds(pl.multiple_of(turn(x, offset) * width, LANES), width)

    step_rows = heads.shape[1]
    g1 = {d: counter.take(SIDE) for d in (1, -1)}
    g2 = {d: counter.take(SIDE) for d in (1, -1)}

    def heads_out(k, d):
        src = heads.at[k, :, hcols(0)]
        return message(src, src, xs[d], g1[d] + k)

    def heads_in(k, d):
        landing = heads.at[k, :, hcols(-d)]
        return message(landing, landing, xs[d], g1[d] + k)

    def far_rows(d):
        return pl.ds(0 if d == 1 else step_rows // 2, step_rows // 2)

    def heads_on(k, d):
        src = heads.at[k, far_rows(d), hcols(-d)]
        return message(src, src, xs[d], g2[d] + k)

    def heads_far(k, d):
        landing = heads.at[k, far_rows(d), hcols(-2 * d)]
        return message(landing, landing, xs[d], g2[d] + k)

    def start_heads(k):
        for d in (1, -1):
            heads_out(k, d).start()

    def forward_heads(k):
        with scope("heads_in"):
            for d in (1, -1):
                heads_in(k, d).wait_recv()
        for d in (1, -1):
            heads_on(k, d).start()

    features = res.shape[3]
    hid = hidden.shape[1]
    side_half = features // 2
    r1 = {d: counter.take(SIDE) for d in (1, -1)}
    r2 = {d: counter.take(SIDE) for d in (1, -1)}

    def prow(offset):
        return pl.ds(pl.multiple_of(turn(x, offset) * sub, sub), sub)

    def project(k):
        with scope("heads_far"):
            for d in (1, -1):
                heads_far(k, d).wait_recv()
        with scope("out_dot"):
            left = heads[k]
            for first, size in tile_list(features, 512):
                mixbuf[:, first : first + size] = jnp.dot(
                    left, o[:, first : first + size], preferred_element_type=F32
                )
        with scope("norms"):
            outer = mixer_gain[...].astype(F32).reshape(1, features)
            inner = in_gain[...].astype(F32).reshape(1, features)
            for d in range(SIDE):
                rows = slice(d * sub, (d + 1) * sub)
                mixed = res[k, d].astype(F32) + unit_rms(mixbuf[rows]) * outer
                mixbuf[rows] = mixed
                ninbuf[k, rows] = (unit_rms(mixed) * inner).astype(BF16)
            for j in range(SIDE):
                spot = slice((j % 2) * sub, (j % 2 + 1) * sub)
                cols = slice(j * width, (j + 1) * width)
                starts[2 * k + j // 2, spot] = mixbuf[prow(0), cols]

    w_fourth = {}

    def pass_weights(m):
        wait_all(w_third[m], "w_third")
        w_fourth[m] = forward_over(False, m)
        w_mirrored[m] += mirror_over((1, -1), m)

    def settle_weights(m):
        wait_all(w_fourth[m], "w_fourth")
        w_mirrored[m] += mirror_over((2,), m)

    wait_all([entered], "enter_wait")
    run("carry1", 0, SIDE, carry_block)
    start_heads(0)
    start_heads(1)
    run("carry2", SIDE, 2 * SIDE, carry_block)
    wait_all(o_rest, "o_rest")
    o_mirrored = []
    for d in (1, -1):
        src = orows(d, c, None)
        o_mirrored.append(post(src, src, orows(d, 1 - c, None), partner))
    pass_weights(0)
    w_third[2] = spread_over(False, (1, 0), 2)
    wait_all(o_second, "o_second")
    src = orows(2, c, None)
    o_mirrored.append(post(src, src, orows(2, 1 - c, None), partner))
    pass_weights(1)
    forward_heads(0)
    start_heads(2)
    forward_heads(1)
    start_heads(3)
    for copy in res_loads:
        copy.wait()
    wait_all(o_mirrored, "o_mirrored")
    project(0)
    pass_weights(2)
    settle_weights(0)
    forward_heads(2)
    settle_weights(1)
    project(1)
    settle_weights(2)
    forward_heads(3)
    wait_all(w_mirrored[0] + w_mirrored[1], "w_mirrored")

    def far_out(k, d):
        lanes = pl.ds(0 if d == 1 else side_half, side_half)
        landing = (ra if d == 1 else rb).at[k]
        return message(parts.at[k, prow(2), lanes], landing, xs[d], r1[d] + k)

    def near_out(k, d):
        landing = (rc if d == 1 else rd).at[k]
        return message(parts.at[k, prow(d)], landing, xs[d], r2[d] + k)

    def pass_on(k):
        for d in (1, -1):
            with scope("far_wait"):
                far_out(k, d).wait_recv()
            lanes = slice(0, side_half) if d == 1 else slice(side_half, features)
            extra = (ra if d == 1 else rb)[k].astype(F32)
            mine = parts[k, prow(d), lanes].astype(F32)
            parts[k, prow(d), lanes] = (mine + extra).astype(BF16)
            near_out(k, d).start()

    def gate_up(k):
        with scope("gate_up"):
            nin = ninbuf[k]
            for first, size in tile_list(hid, 512):
                wg = w[0, :, :, :, :, first : first + size].reshape(features, size)
                wu = w[1, :, :, :, :, first : first + size].reshape(features, size)
                gate = jnp.dot(nin, wg, preferred_element_type=F32)
                up = jnp.dot(nin, wu, preferred_element_type=F32)
                hidden[:, first : first + size] = (silu(gate) * up).astype(BF16)

    def down(k):
        with scope("down"):
            hv = hidden[...]
            tile = features // SIDE
            for n in range(SIDE):
                wd = w[2, n].reshape(tile, hid)
                got = lax.dot_general(hv, wd, (((1,), (1,)), ((), ())), preferred_element_type=F32)
                parts[k, :, n * tile : (n + 1) * tile] = got.astype(BF16)
            for d in (1, -1):
                far_out(k, d).start()

    def channel_mix(k, carry):
        down(k)

        @pl.when(k < 2)
        def _():
            project(k + 2)

        @pl.when(k < SIDE - 1)
        def _():
            pass_on(k)
            gate_up(k + 1)

        return carry

    gate_up(0)
    wait_all(w_mirrored[2], "w_mirrored2")
    lax.fori_loop(0, SIDE, channel_mix, 0)
    outer = 0.5 * out_gain[...].astype(F32).reshape(1, features)

    def finish(k):
        with scope("near_wait"):
            for d in (1, -1):
                near_out(k, d).wait_recv()
        ffn = parts[k, prow(0)].astype(F32) + rc[k].astype(F32) + rd[k].astype(F32)
        kept = [
            starts[2 * k + j // 2, (j % 2) * sub : (j % 2 + 1) * sub] for j in range(SIDE)
        ]
        updated = jnp.concatenate(kept, axis=1) + unit_rms(ffn) * outer
        out[k * sub : (k + 1) * sub] = updated.astype(BF16)

    finish(0)
    finish(1)
    pass_on(SIDE - 1)
    finish(2)
    finish(SIDE - 1)

    with scope("drain"):
        for copy in issued:
            copy.wait_send()

    def drain(k, carry):
        for d in (1, -1):
            heads_out(k, d).wait_send()
            heads_on(k, d).wait_send()
            far_out(k, d).wait_send()
            near_out(k, d).wait_send()
        return carry

    lax.fori_loop(0, SIDE, drain, 0)


def local_program(
    residual,
    small_heads,
    large_heads,
    state_keys,
    state_queries,
    small_gate,
    large_gate,
    small_step,
    large_step,
    small_taps,
    large_taps,
    key_taps,
    query_taps,
    small_decay,
    large_decay,
    small_gain,
    large_gain,
    small_out,
    large_out,
    mixer_gain,
    ffn_in_gain,
    gate_proj,
    up_proj,
    down_proj,
    ffn_out_gain,
):
    length, features = residual.shape
    state_len = state_keys.shape[-1]
    key_rows = state_keys.reshape(length, -1)
    query_rows = state_queries.reshape(length, -1)
    heads_a = small_step.shape[1]
    heads_b = large_step.shape[1]
    heads = heads_a + heads_b
    width_a = small_heads.shape[1]
    width_b = large_heads.shape[1]
    width = width_a + width_b
    everything = width + key_rows.shape[1] + query_rows.shape[1]
    blocks = length // BLOCK
    sizes = ((heads_a, width_a // heads_a), (heads_b, width_b // heads_b), state_len, blocks)
    kernel_len = small_taps.shape[0]
    sub = length // (SIDE * SIDE)
    step_rows = SIDE * sub
    wrows, hid = gate_proj.shape
    half = width // 2
    packet_rows = state_len + TAIL
    any_space = pl.BlockSpec(memory_space=pl.ANY)
    vmem = pl.BlockSpec(memory_space=pltpu.VMEM)
    smem = pl.BlockSpec(memory_space=pltpu.SMEM)
    messages = 160

    return pl.pallas_call(
        functools.partial(whole_kernel, sizes),
        in_specs=[any_space] * 5
        + [vmem] * 4
        + [smem] * 2
        + [vmem] * 6
        + [any_space] * 2
        + [vmem] * 3
        + [any_space] * 3,
        out_specs=vmem,
        out_shape=jax.ShapeDtypeStruct((length // SIDE, features), BF16),
        scratch_shapes=[
            pltpu.VMEM((4, HALO + length, width_a), BF16),
            pltpu.VMEM((length, everything), BF16),
            pltpu.VMEM((kernel_len, everything), F32),
            pltpu.VMEM((1, width), F32),
            pltpu.VMEM((SLOTS, length), F32),
            pltpu.VMEM((SLOTS, length), F32),
            pltpu.VMEM((length, 2 * SLOTS), F32),
            pltpu.VMEM((blocks, 1, width), F32),
            pltpu.VMEM((blocks, 1, width), F32),
            pltpu.VMEM((blocks, state_len, width), F32),
            pltpu.VMEM((length, width), F32),
            pltpu.VMEM((state_len, width), F32),
            pltpu.VMEM((1, width), F32),
            pltpu.VMEM((packet_rows, width), BF16),
            pltpu.VMEM((packet_rows, half), BF16),
            pltpu.VMEM((state_len, half), F32),
            pltpu.VMEM((1, half), F32),
            pltpu.VMEM((SIDE, packet_rows, half), BF16),
            pltpu.VMEM((SIDE, packet_rows, half), BF16),
            pltpu.VMEM((state_len, half), F32),
            pltpu.VMEM((1, half), F32),
            pltpu.VMEM((state_len, width), F32),
            pltpu.VMEM((state_len, half), F32),
            pltpu.VMEM((3, SIDE, SIDE, 2, wrows, hid), BF16),
            pltpu.VMEM((SIDE * width, features), BF16),
            pltpu.VMEM((SIDE, step_rows, SIDE * width), BF16),
            pltpu.VMEM((SIDE, SIDE, sub, features), BF16),
            pltpu.VMEM((step_rows, features), F32),
            pltpu.VMEM((SIDE, step_rows, features), BF16),
            pltpu.VMEM((step_rows, hid), BF16),
            pltpu.VMEM((SIDE, step_rows, features), BF16),
            pltpu.VMEM((SIDE, sub, features // 2), BF16),
            pltpu.VMEM((SIDE, sub, features // 2), BF16),
            pltpu.VMEM((SIDE, sub, features), BF16),
            pltpu.VMEM((SIDE, sub, features), BF16),
            pltpu.SemaphoreType.DMA((messages,)),
            pltpu.SemaphoreType.DMA((messages,)),
            pltpu.SemaphoreType.DMA((16,)),
        ],
        compiler_params=pltpu.CompilerParams(
            collective_id=0, has_side_effects=True, vmem_limit_bytes=VMEM_LIMIT
        ),
        cost_estimate=pl.CostEstimate(
            flops=40_000_000_000, bytes_accessed=60_000_000, transcendentals=0
        ),
        name="layer",
    )(
        residual.reshape(SIDE, SIDE, sub, features),
        small_heads,
        large_heads,
        key_rows,
        query_rows,
        small_gate,
        large_gate,
        small_step.T,
        large_step.T,
        small_decay,
        large_decay,
        small_taps,
        large_taps,
        key_taps,
        query_taps,
        small_gain,
        large_gain,
        small_out,
        large_out,
        mixer_gain,
        ffn_in_gain,
        ffn_out_gain,
        gate_proj,
        up_proj,
        down_proj,
    )


def solution(mesh):
    placed = (
        P("sp", None),
        P("sp", "tp"),
        P("sp", "tp"),
        P("sp", "tp", None),
        P("sp", "tp", None),
        P("sp", "tp"),
        P("sp", "tp"),
        P("sp", "tp"),
        P("sp", "tp"),
        P(None, "tp"),
        P(None, "tp"),
        P(None, "tp", None),
        P(None, "tp", None),
        P("tp"),
        P("tp"),
        P("tp"),
        P("tp"),
        P("tp", None),
        P("tp", None),
        P(),
        P(),
        P("sp", "tp"),
        P("sp", "tp"),
        P("sp", "tp"),
        P(),
    )
    return jax.shard_map(
        local_program, mesh=mesh, in_specs=placed, out_specs=P(("sp", "tp"), None), check_vma=False
    )
```

```python
import functools

import jax
import jax.numpy as jnp
from jax import lax
from jax.experimental import pallas as pl
from jax.experimental.pallas import tpu as pltpu
from jax.sharding import PartitionSpec as P

BLOCK = 128
HALO = 16
LANES = 128
SLOTS = 8
TAIL = 16
SIDE = 4

EPS = 1e-06
FAR = -1e30
F32 = jnp.float32
BF16 = jnp.bfloat16
MESH = pl.DeviceIdType.MESH
scope = jax.named_scope
VMEM_LIMIT = 66_000_000


def silu(x):
    return x / (1.0 + jnp.exp(-x))


def softplus(x):
    return jnp.maximum(x, 0.0) + jnp.log1p(jnp.exp(-jnp.abs(x)))


def exact_dot(a, b, dims=(((1,), (0,)), ((), ()))):
    return lax.dot_general(a, b, dims, precision=lax.Precision.HIGHEST, preferred_element_type=F32)


def lower(n):
    rows = lax.broadcasted_iota(jnp.int32, (n, n), 0)
    return rows >= lax.broadcasted_iota(jnp.int32, (n, n), 1)


def spread(columns, heads, dim):
    rows = columns.shape[0]
    parts = []
    if dim >= LANES:
        for h in heads:
            parts.append(jnp.broadcast_to(columns[:, h : h + 1], (rows, dim)))
    else:
        per = LANES // dim
        lane = lax.broadcasted_iota(jnp.int32, (rows, LANES), 1)
        for first in range(0, len(heads), per):
            part = jnp.broadcast_to(columns[:, heads[first] : heads[first] + 1], (rows, LANES))
            for j in range(1, per):
                h = heads[first + j]
                part = jnp.where(lane >= j * dim, columns[:, h : h + 1], part)
            parts.append(part)
    return jnp.concatenate(parts, axis=1)


def unit_rms(values):
    return values * lax.rsqrt(jnp.mean(values * values, axis=-1, keepdims=True) + EPS)


def pack(ref, slot, state, log):
    rows = state.shape[0]
    high = log.astype(BF16).astype(F32)
    row = lax.broadcasted_iota(jnp.int32, (TAIL, log.shape[1]), 0)
    both = jnp.where(row == 0, high, jnp.where(row == 1, log - high, 0.0))
    if slot is None:
        ref[:rows] = state.astype(BF16)
        ref[rows:] = both.astype(BF16)
    else:
        ref[slot, :rows] = state.astype(BF16)
        ref[slot, rows:] = both.astype(BF16)


def opened(packet, rows):
    log = packet[rows : rows + TAIL].astype(F32)
    return packet[:rows].astype(F32), log[0:1] + log[1:2]


class Counter:
    def __init__(self):
        self.n = 0

    def take(self, count=1):
        first = self.n
        self.n += count
        return first


def tile_list(width, tile):
    return [(s, min(tile, width - s)) for s in range(0, width, tile)]


def whole_kernel(
    sizes,
    res_in,
    small_in,
    large_in,
    key_in,
    query_in,
    small_gate_in,
    large_gate_in,
    small_step,
    large_step,
    small_decay,
    large_decay,
    small_taps,
    large_taps,
    key_taps,
    query_taps,
    small_gain,
    large_gain,
    small_out,
    large_out,
    mixer_gain,
    in_gain,
    out_gain,
    gate_in,
    up_in,
    down_in,
    out,
    xin,
    kin,
    gates,
    woven,
    conv,
    taps,
    pattern,
    gain,
    dt_rows,
    cum_rows,
    cums,
    logs,
    tails,
    starts,
    inside,
    state,
    total,
    packet,
    from_partner,
    first_state,
    first_log,
    along_y,
    along_z,
    row_state,
    row_log,
    entering,
    for_partner,
    w,
    o,
    heads,
    res,
    mixbuf,
    ninbuf,
    hidden,
    parts,
    ra,
    rb,
    rc,
    rd,
    send,
    recv,
    local,
):
    (heads_a, dim_a), (heads_b, dim_b), state_len, blocks = sizes
    head_list_a = list(range(heads_a))
    head_list_b = list(range(heads_a, heads_a + heads_b))
    width_a = heads_a * dim_a
    width_b = heads_b * dim_b
    width = width_a + width_b
    groups = (
        (head_list_a, dim_a, width_a, 0),
        (head_list_b, dim_b, width_b, width_a),
    )

    sp = lax.axis_index("sp")
    x = lax.axis_index("tp")
    c = lax.rem(sp, 2)
    y = lax.rem(sp // 2, SIDE)
    z = sp // (2 * SIDE)
    zy = sp // 2
    count_sp = lax.axis_size("sp")

    def turn(v, d):
        return lax.rem(v + d + SIDE, SIDE)

    def at_chip(zz, yy):
        return ((zz * SIDE + yy) * 2 + c, x)

    partner = (sp + 1 - 2 * c, x)
    xs = {d: (sp, turn(x, d)) for d in (1, -1, 2)}
    ys = {d: at_chip(z, turn(y, d)) for d in (1, -1, 2)}
    zs = {d: at_chip(turn(z, d), y) for d in (1, -1, 2)}
    after = (lax.rem(sp + 1, count_sp), x)
    prior = (lax.rem(sp + count_sp - 1, count_sp), x)

    barrier = pltpu.get_barrier_semaphore()
    greeted = [partner, after, prior] + [v[d] for v in (xs, ys, zs) for d in (1, -1, 2)]
    for peer in greeted:
        pl.semaphore_signal(barrier, inc=1, device_id=peer, device_id_type=MESH)

    counter = Counter()
    issued = []

    def message(src, dst, target, index):
        return pltpu.make_async_remote_copy(
            src_ref=src,
            dst_ref=dst,
            send_sem=send.at[index],
            recv_sem=recv.at[index],
            device_id=target,
            device_id_type=MESH,
        )

    def post(src, dst, landing, target):
        index = counter.take()
        copy = message(src, dst, target, index)
        copy.start()
        issued.append(copy)
        return message(landing, landing, target, index)

    def wait_all(arrivals, name="wait"):
        with scope(name):
            for arrival in arrivals:
                arrival.wait_recv()

    def run(name, first, last, body):
        with scope(name):
            lax.fori_loop(first, last, body, 0)

    loads = []

    def load(src, dst):
        copy = pltpu.make_async_copy(src, dst, local.at[len(loads)])
        copy.start()
        loads.append(copy)
        return copy

    length = small_in.shape[0]
    weight_loads = [
        load(ref, w.at[m, z, y, c]) for m, ref in enumerate((gate_in, up_in, down_in))
    ]
    conv_loads = [
        load(ref, xin.at[g, pl.ds(HALO, length)]) for g, ref in enumerate((small_in, large_in))
    ]
    conv_loads += [
        load(ref, kin.at[g, pl.ds(2 * HALO, 2 * length)])
        for g, ref in enumerate((key_in, query_in))
    ]
    out_loads = [
        load(ref, o.at[x, pl.ds(first, SIDE // 2)])
        for ref, first in ((small_out, 0), (large_out, SIDE // 2))
    ]
    gate_loads = [
        load(ref, gates.at[g]) for g, ref in enumerate((small_gate_in, large_gate_in))
    ]
    res_loads = [load(res_in.at[:, k], res.at[k]) for k in range(SIDE)]

    with scope("barrier"):
        pl.semaphore_wait(barrier, len(greeted))

    halo = []
    for g, ref in enumerate((small_in, large_in)):
        first = xin.at[g, pl.ds(0, HALO)]
        halo.append(post(ref.at[pl.ds(length - HALO, HALO)], first, first, after))
    for g, ref in enumerate((key_in, query_in)):
        first = kin.at[g, pl.ds(0, 2 * HALO)]
        halo.append(post(ref.at[pl.ds(2 * (length - HALO), 2 * HALO)], first, first, after))

    def cell(kind, h, first_axis, offset, q=None, m=None, core=c):
        if first_axis:
            zz, yy = (z, turn(y, offset)) if h == 0 else (turn(z, offset), y)
        else:
            zz, yy = (turn(z, offset), slice(None)) if h == 0 else (slice(None), turn(y, offset))
        extent = w.shape[4] if kind == "w" else o.shape[5]
        if q is None:
            part = pl.ds(h * (extent // 2), extent // 2)
        else:
            part = pl.ds(h * (extent // 2) + q * (extent // 4), extent // 4)
        if kind == "o":
            return o.at[turn(x, 2), zz, yy, core, slice(None), part]
        return w.at[slice(None) if m is None else m, zz, yy, core, part]

    def target_of(h, first_axis, d):
        return (ys if (h == 0) == first_axis else zs)[d]

    def spread_over(kind, first_axis, hs=(0, 1), m=None):
        arrivals = []
        for h in hs:
            for d in (1, -1):
                src = cell(kind, h, first_axis, 0, m=m)
                landing = cell(kind, h, first_axis, -d, m=m)
                arrivals.append(post(src, src, landing, target_of(h, first_axis, d)))
        return arrivals

    def forward_over(kind, first_axis, m=None, hs=(0, 1)):
        arrivals = []
        for h in hs:
            for d, q in ((1, 0), (-1, 1)):
                src = cell(kind, h, first_axis, -d, q, m)
                landing = cell(kind, h, first_axis, -2 * d, q, m)
                arrivals.append(post(src, src, landing, target_of(h, first_axis, d)))
        return arrivals

    def mirror_over(kind, offsets, m=None):
        arrivals = []
        for h in (0, 1):
            for offset in offsets:
                src = cell(kind, h, False, offset, m=m)
                landing = cell(kind, h, False, offset, m=m, core=1 - c)
                arrivals.append(post(src, src, landing, partner))
        return arrivals

    with scope("loads"):
        for copy in weight_loads + out_loads:
            copy.wait()
    mine_out = o.at[x, z, y, c]
    o_entry = [post(mine_out, mine_out, o.at[turn(x, 2), z, y, c], xs[2])]
    w_first = spread_over("w", True)

    def orows(offset, core):
        return o.at[turn(x, offset), pl.ds(core * (SIDE // 2), SIDE // 2)]

    o_near = [post(orows(0, c), orows(0, c), orows(-d, c), xs[d]) for d in (1, -1)]

    kernel_len = small_taps.shape[0]
    taps[:, :width_a] = small_taps[...].astype(F32)
    taps[:, width_a:width] = large_taps[...].astype(F32)
    pair_row = lax.broadcasted_iota(jnp.int32, (SLOTS, LANES), 0)
    for g, ref in enumerate((key_taps, query_taps)):
        for k in range(kernel_len):
            pattern[g, k] = jnp.where(
                pair_row % 2 == 0, ref[k, 0:1].astype(F32), ref[k, 1:2].astype(F32)
            )
    gain[:, :width_a] = small_gain[...].astype(F32).reshape(1, width_a)
    gain[:, width_a:] = large_gain[...].astype(F32).reshape(1, width_b)
    dt_rows[...] = jnp.zeros_like(dt_rows)
    dt_rows[:heads_a] = softplus(small_step[...])
    dt_rows[heads_a : heads_a + heads_b] = softplus(large_step[...])
    head_row = lax.broadcasted_iota(jnp.int32, (SLOTS, BLOCK), 0)
    rate = jnp.zeros((SLOTS, BLOCK), F32)
    for h in range(heads_a + heads_b):
        value = small_decay[h] if h < heads_a else large_decay[h - heads_a]
        rate = jnp.where(head_row == h, value, rate)
    rate = jnp.exp(rate)
    row_id = lax.broadcasted_iota(jnp.int32, (BLOCK, BLOCK), 0)
    col_id = lax.broadcasted_iota(jnp.int32, (BLOCK, BLOCK), 1)
    with scope("decays"):
        pieces = [dt_rows[:, i * BLOCK : (i + 1) * BLOCK] for i in range(blocks)]
        dt_all = jnp.concatenate(pieces, axis=0)
        rate_all = jnp.concatenate([rate] * blocks, axis=0)
        cum_all = exact_dot(-dt_all * rate_all, (row_id <= col_id).astype(F32))
        scale_all = dt_all * jnp.exp(cum_all[:, BLOCK - 1 : BLOCK] - cum_all)
        eye = (row_id == col_id).astype(F32)
        turned = exact_dot(
            eye, jnp.concatenate([cum_all, scale_all], axis=0), (((1,), (1,)), ((), ()))
        )
        before = jnp.zeros((1, SLOTS), F32)
        for i in range(blocks):
            rows = slice(i * BLOCK, (i + 1) * BLOCK)
            heads_at = slice(i * SLOTS, (i + 1) * SLOTS)
            scales_at = slice((blocks + i) * SLOTS, (blocks + i + 1) * SLOTS)
            cum_rows[:, rows] = cum_all[heads_at]
            cums[rows, :SLOTS] = turned[:, heads_at]
            cums[rows, SLOTS:] = turned[:, scales_at]
            tail = turned[BLOCK - 1 : BLOCK, heads_at]
            for buffer, value in ((logs, before), (tails, tail)):
                buffer[i] = jnp.concatenate(
                    [spread(value, head_list_a, dim_a), spread(value, head_list_b, dim_b)], axis=1
                )
            before = before + tail
        final_log = jnp.concatenate(
            [spread(before, head_list_a, dim_a), spread(before, head_list_b, dim_b)], axis=1
        )
        total[...] = final_log
    state[...] = jnp.zeros_like(state)

    with scope("conv_loads"):
        for copy in conv_loads:
            copy.wait()
    def convolve(g, at):
        for first_lane in range(0, xin.shape[2], LANES):
            here = pl.ds(g * xin.shape[2] + first_lane, LANES)
            extended = xin[g, pl.ds(at, BLOCK + HALO), pl.ds(first_lane, LANES)].astype(F32)
            summed = None
            for k in range(kernel_len):
                first = HALO - kernel_len + 1 + k
                term = taps[k : k + 1, here] * extended[first : first + BLOCK]
                summed = term if summed is None else summed + term
            conv[pl.ds(at, BLOCK), here] = silu(summed).astype(BF16)

    def convolve_pair(g, at):
        span = 2 * BLOCK
        rows = pl.ds(pl.multiple_of(2 * at, span), span + 2 * HALO)
        extended = kin[g, rows].astype(F32)
        summed = None
        for k in range(kernel_len):
            first = 2 * (HALO - kernel_len + 1 + k)
            window = extended[first : first + span].reshape(span // SLOTS, SLOTS, LANES)
            term = window * pattern[g, k][None]
            summed = term if summed is None else summed + term
        woven[...] = silu(summed).reshape(span, LANES)
        for j in range(2):
            column = width + (2 * g + j) * state_len
            conv[pl.ds(at, BLOCK), column : column + LANES] = woven[
                pl.ds(j, BLOCK, stride=2), :
            ].astype(BF16)

    def convolve_three(i, carry):
        at = pl.multiple_of(i * BLOCK, BLOCK)
        convolve(0, at)
        convolve(1, at)
        convolve_pair(0, at)
        return carry

    def states(i, carry):
        at = pl.multiple_of(i * BLOCK, BLOCK)
        rows = pl.ds(at, BLOCK)
        scale = cums[rows, SLOTS:]
        kept = jnp.exp(tails[i])
        for which, (head_list, dim, wide, offset) in enumerate(groups):
            key_at = width + which * state_len
            columns = slice(offset, offset + wide)
            heads_here = list(range(len(head_list)))
            shifted = scale[:, head_list[0] : head_list[-1] + 1]
            xv = conv[rows, columns].astype(F32)
            u = (xv * spread(shifted, heads_here, dim)).astype(BF16)
            k = conv[rows, key_at : key_at + state_len]
            fresh = lax.dot_general(k, u, (((0,), (0,)), ((), ())), preferred_element_type=F32)
            old = state[:, columns]
            starts[i, :, columns] = old
            state[:, columns] = old * kept[:, columns] + fresh
        return carry

    run("conv1", 1, blocks, convolve_three)
    wait_all(halo, "halo")
    for g in range(2):
        for buffer, size in ((xin, HALO), (kin, 2 * HALO)):
            edge = buffer[g, :size].astype(F32)
            buffer[g, :size] = jnp.where(sp == 0, 0.0, edge).astype(BF16)
    run("conv0", 0, 1, convolve_three)
    run("states", 0, blocks, states)

    half = width // 2

    def half_of(core):
        return pl.ds(pl.multiple_of(core * half, half), half)

    pack(packet, None, state[...], total[...])
    swapped = post(packet.at[:, half_of(1 - c)], from_partner, from_partner, partner)

    def queries(i, carry):
        convolve_pair(1, pl.multiple_of(i * BLOCK, BLOCK))
        return carry

    def mix_inside(i, carry):
        at = pl.multiple_of(i * BLOCK, BLOCK)
        rows = pl.ds(at, BLOCK)
        causal = row_id >= col_id
        dt_across = dt_rows[:, rows]
        cum = cums[rows]
        cum_across = cum_rows[:, rows]
        lane = lax.broadcasted_iota(jnp.int32, (BLOCK, LANES), 1)
        for which, (head_list, dim, wide, offset) in enumerate(groups):
            key_at = width + which * state_len
            query_at = key_at + 2 * state_len
            k = conv[rows, key_at : key_at + state_len]
            q = conv[rows, query_at : query_at + state_len]
            scores = lax.dot_general(q, k, (((1,), (1,)), ((), ())), preferred_element_type=F32)
            span = max(dim, LANES)
            per = span // dim
            for first in range(0, len(head_list), per):
                columns = slice(offset + first * dim, offset + first * dim + span)
                x_part = conv[rows, columns]
                part = None
                for j in range(per):
                    h = head_list[first + j]
                    gap = cum[:, h : h + 1] - cum_across[h : h + 1]
                    decays = jnp.exp(jnp.where(causal, gap, FAR))
                    weight = (scores * decays * dt_across[h : h + 1]).astype(BF16)
                    got = jnp.dot(weight, x_part, preferred_element_type=F32)
                    part = got if part is None else jnp.where(lane >= j * dim, got, part)
                inside[rows, columns] = part
        return carry

    def send_along(buffer, targets):
        arrivals = []
        for d, slot in ((1, 1), (-1, 3), (2, 2)):
            landing = buffer.at[slot]
            arrivals.append(post(buffer.at[0], landing, landing, targets[d]))
        return arrivals

    def fold(buffer, place, number):
        zero = jnp.zeros((state_len, half), F32)
        every, every_log = zero, jnp.zeros((1, half), F32)
        ahead, ahead_log = every, every_log
        for p in range(number):
            slot = turn(place, -p)
            one, log = opened(buffer[slot], state_len)
            counts = p < place
            ahead = jnp.where(counts, ahead * jnp.exp(log) + one, ahead)
            ahead_log = jnp.where(counts, ahead_log + log, ahead_log)
            every = every * jnp.exp(log) + one
            every_log = every_log + log
        return every, every_log, ahead, ahead_log

    wait_all(w_first[2:], "w_first_z")
    w_second_z = forward_over("w", True, hs=(1,))
    wait_all(o_entry, "o_entry")
    o_first_z = spread_over("o", True, (1,))
    run("queries", 0, blocks, queries)
    wait_all([swapped], "swap_wait")
    mine, mine_log = opened(packet[:, half_of(c)], state_len)
    theirs, theirs_log = opened(from_partner[...], state_len)
    even = c == 0
    a_state = jnp.where(even, mine, theirs)
    a_log = jnp.where(even, mine_log, theirs_log)
    b_state = jnp.where(even, theirs, mine)
    b_log = jnp.where(even, theirs_log, mine_log)
    first_state[...] = a_state
    first_log[...] = a_log
    pack(along_y, 0, a_state * jnp.exp(b_log) + b_state, a_log + b_log)
    y_arrivals = send_along(along_y, ys)
    wait_all(w_first[:2], "w_first_y")
    w_second_y = forward_over("w", True, hs=(0,))
    o_first_y = spread_over("o", True, (0,))
    run("mix0", 0, 4, mix_inside)
    wait_all(o_first_z, "o_first_z")
    o_second_z = forward_over("o", True, hs=(1,))
    wait_all(y_arrivals, "y_wait")
    row_all, row_all_log, row_ahead, row_ahead_log = fold(along_y, y, SIDE)
    row_state[...] = row_ahead
    row_log[...] = row_ahead_log
    pack(along_z, 0, row_all, row_all_log)
    z_arrivals = send_along(along_z, zs)
    wait_all(o_second_z, "o_second_z")
    o_third = spread_over("o", False, (1,))
    run("mix4", 4, 6, mix_inside)
    wait_all(o_first_y, "o_first_y")
    o_second_y = forward_over("o", True, hs=(0,))
    wait_all(w_second_z, "w_second_z")
    w_third = {0: spread_over("w", False, (1,), 0)}
    wait_all(w_second_y, "w_second_y")
    w_third[0] += spread_over("w", False, (0,), 0)
    run("mix6", 6, blocks, mix_inside)
    wait_all(z_arrivals, "z_wait")
    _, _, plane_ahead, _ = fold(along_z, z, SIDE - 1)
    chip = plane_ahead * jnp.exp(row_log[...]) + row_state[...]
    second = chip * jnp.exp(first_log[...]) + first_state[...]
    entering[:, half_of(c)] = jnp.where(even, chip, second)
    for_partner[...] = jnp.where(even, second, chip)
    entered = post(
        for_partner, entering.at[:, half_of(c)], entering.at[:, half_of(1 - c)], partner
    )
    wait_all(o_second_y, "o_second_y")
    o_third += spread_over("o", False, (0,))
    w_third[1] = spread_over("w", False, (1,), 1)
    w_mirrored = {m: mirror_over("w", (0,), m) for m in range(3)}
    o_mirrored = mirror_over("o", (0,))

    sub = length // (SIDE * SIDE)
    lane = lax.broadcasted_iota(jnp.int32, (BLOCK, LANES), 1)

    def carry_block(n, carry):
        stage = n // SIDE
        d = lax.rem(n, SIDE)
        i = 2 * d + stage
        rows = pl.ds(pl.multiple_of(i * BLOCK, BLOCK), BLOCK)
        grown = jnp.exp(cums[rows])
        for which, (head_list, dim, wide, offset) in enumerate(groups):
            columns = slice(offset, offset + wide)
            query_at = width + (2 + which) * state_len
            q = conv[rows, query_at : query_at + state_len]
            old = starts[i, :, columns] + entering[:, columns] * jnp.exp(logs[i, :, columns])
            carried = jnp.dot(q, old.astype(BF16), preferred_element_type=F32)
            mixed = inside[rows, columns] + carried * spread(grown, head_list, dim)
            gated = mixed * silu(gates[which, rows].astype(F32))
            squares = gated * gated
            span = max(dim, LANES)
            per = span // dim
            normed = []
            for first in range(0, len(head_list), per):
                at = first * dim
                part = squares[:, at : at + span]
                means = None
                for j in range(per):
                    if per == 1:
                        means = jnp.sum(part, axis=1, keepdims=True)
                    else:
                        ours = (lane >= j * dim) & (lane < (j + 1) * dim)
                        one = jnp.sum(jnp.where(ours, part, 0.0), axis=1, keepdims=True)
                        means = one if means is None else jnp.where(lane >= j * dim, one, means)
                normed.append(gated[:, at : at + span] * lax.rsqrt(means * (1.0 / dim) + EPS))
            normed = (jnp.concatenate(normed, axis=1) * gain[:, columns]).astype(BF16)
            place = pl.ds(pl.multiple_of(x * width + offset, LANES), wide)
            spot = pl.ds(pl.multiple_of(d * sub, sub), sub)
            heads[2 * stage, spot, place] = normed[:sub]
            heads[2 * stage + 1, spot, place] = normed[sub:]
        return carry

    def hcols(offset):
        return pl.ds(pl.multiple_of(turn(x, offset) * width, LANES), width)

    step_rows = heads.shape[1]
    g1 = {d: counter.take(SIDE) for d in (1, -1)}
    g2 = {d: counter.take(SIDE) for d in (1, -1)}

    def heads_out(k, d):
        src = heads.at[k, :, hcols(0)]
        return message(src, src, xs[d], g1[d] + k)

    def heads_in(k, d):
        landing = heads.at[k, :, hcols(-d)]
        return message(landing, landing, xs[d], g1[d] + k)

    def far_rows(d):
        return pl.ds(0 if d == 1 else step_rows // 2, step_rows // 2)

    def heads_on(k, d):
        src = heads.at[k, far_rows(d), hcols(-d)]
        return message(src, src, xs[d], g2[d] + k)

    def heads_far(k, d):
        landing = heads.at[k, far_rows(d), hcols(-2 * d)]
        return message(landing, landing, xs[d], g2[d] + k)

    def start_heads(k):
        for d in (1, -1):
            heads_out(k, d).start()

    def forward_heads(k):
        with scope("heads_in"):
            for d in (1, -1):
                heads_in(k, d).wait_recv()
        for d in (1, -1):
            heads_on(k, d).start()

    features = res.shape[3]
    hid = hidden.shape[2]
    side_half = features // 2
    r1 = {d: counter.take(SIDE) for d in (1, -1)}
    r2 = {d: counter.take(SIDE) for d in (1, -1)}

    def prow(offset):
        return pl.ds(pl.multiple_of(turn(x, offset) * sub, sub), sub)

    def project(k):
        with scope("heads_far"):
            for d in (1, -1):
                heads_far(k, d).wait_recv()
        with scope("out_dot"):
            left = heads[k]
            for first, size in tile_list(features, 512):
                mixbuf[:, first : first + size] = jnp.dot(
                    left,
                    o[..., first : first + size].reshape(SIDE * width, size),
                    preferred_element_type=F32,
                )
        with scope("norms"):
            outer = mixer_gain[...].astype(F32).reshape(1, features)
            inner = in_gain[...].astype(F32).reshape(1, features)
            for d in range(SIDE):
                rows = slice(d * sub, (d + 1) * sub)
                mixed = res[k, d].astype(F32) + unit_rms(mixbuf[rows]) * outer
                mixbuf[rows] = mixed
                ninbuf[k, rows] = (unit_rms(mixed) * inner).astype(BF16)
            for j in range(SIDE):
                spot = slice((j % 2) * sub, (j % 2 + 1) * sub)
                cols = slice(j * width, (j + 1) * width)
                starts[2 * k + j // 2, spot] = mixbuf[prow(0), cols]

    w_fourth = {}

    def pass_weights(m):
        wait_all(w_third[m], "w_third")
        w_fourth[m] = forward_over("w", False, m)
        w_mirrored[m] += mirror_over("w", (1, -1), m)

    def settle_weights(m):
        wait_all(w_fourth[m], "w_fourth")
        w_mirrored[m] += mirror_over("w", (2,), m)

    wait_all([entered], "enter_wait")
    for copy in gate_loads:
        copy.wait()
    run("carry1", 0, SIDE, carry_block)
    start_heads(0)
    start_heads(1)
    run("carry2", SIDE, 2 * SIDE, carry_block)
    wait_all(o_near, "o_near")
    for d in (1, -1):
        o_mirrored.append(post(orows(d, c), orows(d, c), orows(d, 1 - c), partner))
    wait_all(o_third, "o_third")
    o_fourth = forward_over("o", False)
    o_mirrored += mirror_over("o", (1, -1))
    w_third[1] += spread_over("w", False, (0,), 1)
    pass_weights(0)
    w_third[2] = spread_over("w", False, (1, 0), 2)
    forward_heads(0)
    start_heads(2)
    wait_all(o_fourth, "o_fourth")
    o_mirrored += mirror_over("o", (2,))
    forward_heads(1)
    start_heads(3)
    for copy in res_loads:
        copy.wait()
    wait_all(o_mirrored, "o_mirrored")
    project(0)
    pass_weights(1)
    settle_weights(0)
    forward_heads(2)
    project(1)
    pass_weights(2)
    forward_heads(3)
    settle_weights(1)
    wait_all(w_mirrored[0] + w_mirrored[1], "w_mirrored")

    def far_out(k, d):
        lanes = pl.ds(0 if d == 1 else side_half, side_half)
        landing = (ra if d == 1 else rb).at[k]
        return message(parts.at[k, prow(2), lanes], landing, xs[d], r1[d] + k)

    def near_out(k, d):
        landing = (rc if d == 1 else rd).at[k]
        return message(parts.at[k, prow(d)], landing, xs[d], r2[d] + k)

    def pass_on(k):
        for d in (1, -1):
            with scope("far_wait"):
                far_out(k, d).wait_recv()
            lanes = slice(0, side_half) if d == 1 else slice(side_half, features)
            extra = (ra if d == 1 else rb)[k].astype(F32)
            mine = parts[k, prow(d), lanes].astype(F32)
            parts[k, prow(d), lanes] = (mine + extra).astype(BF16)
            near_out(k, d).start()

    def gate_up(k, between=None):
        with scope("gate_up"):
            nin = ninbuf[k]
            for first, size in tile_list(hid, 512):
                if between is not None and first == 1024:
                    between()
                wg = w[0, :, :, :, :, first : first + size].reshape(features, size)
                wu = w[1, :, :, :, :, first : first + size].reshape(features, size)
                gate = jnp.dot(nin, wg, preferred_element_type=F32)
                up = jnp.dot(nin, wu, preferred_element_type=F32)
                hidden[lax.rem(k, 2), :, first : first + size] = (silu(gate) * up).astype(BF16)

    def down(k):
        with scope("down"):
            hv = hidden[lax.rem(k, 2)]
            tile = features // SIDE
            for n in range(SIDE):
                wd = w[2, n].reshape(tile, hid)
                got = lax.dot_general(hv, wd, (((1,), (1,)), ((), ())), preferred_element_type=F32)
                parts[k, :, n * tile : (n + 1) * tile] = got.astype(BF16)
            for d in (1, -1):
                far_out(k, d).start()

    def down_pair(k, carry):
        down(k)
        return carry

    def channel_mix(k, carry):
        project(k)

        @pl.when(k == 2)
        def _():
            pass_on(0)

        gate_up(k)

        @pl.when(k == 2)
        def _():
            pass_on(1)

        down(k)
        return carry

    gate_up(0, lambda: settle_weights(2))
    gate_up(1)
    wait_all(w_mirrored[2], "w_mirrored2")
    lax.fori_loop(0, 2, down_pair, 0)
    lax.fori_loop(2, SIDE, channel_mix, 0)
    outer = 0.5 * out_gain[...].astype(F32).reshape(1, features)

    def finish(k):
        with scope("near_wait"):
            for d in (1, -1):
                near_out(k, d).wait_recv()
        ffn = parts[k, prow(0)].astype(F32) + rc[k].astype(F32) + rd[k].astype(F32)
        kept = [
            starts[2 * k + j // 2, (j % 2) * sub : (j % 2 + 1) * sub] for j in range(SIDE)
        ]
        updated = jnp.concatenate(kept, axis=1) + unit_rms(ffn) * outer
        out[k * sub : (k + 1) * sub] = updated.astype(BF16)

    pass_on(SIDE - 2)
    finish(0)
    finish(1)
    pass_on(SIDE - 1)
    finish(2)
    finish(SIDE - 1)

    with scope("drain"):
        for copy in issued:
            copy.wait_send()

    def drain(k, carry):
        for d in (1, -1):
            heads_out(k, d).wait_send()
            heads_on(k, d).wait_send()
            far_out(k, d).wait_send()
            near_out(k, d).wait_send()
        return carry

    lax.fori_loop(0, SIDE, drain, 0)


def local_program(
    residual,
    small_heads,
    large_heads,
    state_keys,
    state_queries,
    small_gate,
    large_gate,
    small_step,
    large_step,
    small_taps,
    large_taps,
    key_taps,
    query_taps,
    small_decay,
    large_decay,
    small_gain,
    large_gain,
    small_out,
    large_out,
    mixer_gain,
    ffn_in_gain,
    gate_proj,
    up_proj,
    down_proj,
    ffn_out_gain,
):
    length, features = residual.shape
    state_len = state_keys.shape[-1]
    key_rows = state_keys.reshape(-1, state_len)
    query_rows = state_queries.reshape(-1, state_len)
    heads_a = small_step.shape[1]
    heads_b = large_step.shape[1]
    heads = heads_a + heads_b
    width_a = small_heads.shape[1]
    width_b = large_heads.shape[1]
    width = width_a + width_b
    everything = width + 2 * state_len * state_keys.shape[1]
    blocks = length // BLOCK
    sizes = ((heads_a, width_a // heads_a), (heads_b, width_b // heads_b), state_len, blocks)
    kernel_len = small_taps.shape[0]
    sub = length // (SIDE * SIDE)
    step_rows = SIDE * sub
    wrows, hid = gate_proj.shape
    orow = width // (2 * SIDE * SIDE)
    out_shape = (SIDE // 2, SIDE, 2, orow, features)
    half = width // 2
    packet_rows = state_len + TAIL
    any_space = pl.BlockSpec(memory_space=pl.ANY)
    vmem = pl.BlockSpec(memory_space=pltpu.VMEM)
    smem = pl.BlockSpec(memory_space=pltpu.SMEM)
    messages = 160

    return pl.pallas_call(
        functools.partial(whole_kernel, sizes),
        in_specs=[any_space] * 7
        + [vmem] * 2
        + [smem] * 2
        + [vmem] * 6
        + [any_space] * 2
        + [vmem] * 3
        + [any_space] * 3,
        out_specs=vmem,
        out_shape=jax.ShapeDtypeStruct((length // SIDE, features), BF16),
        scratch_shapes=[
            pltpu.VMEM((2, HALO + length, width_a), BF16),
            pltpu.VMEM((2, 2 * (HALO + length), state_len), BF16),
            pltpu.VMEM((2, length, width_a), BF16),
            pltpu.VMEM((2 * BLOCK, state_len), F32),
            pltpu.VMEM((length, everything), BF16),
            pltpu.VMEM((kernel_len, width), F32),
            pltpu.VMEM((2, kernel_len, SLOTS, state_len), F32),
            pltpu.VMEM((1, width), F32),
            pltpu.VMEM((SLOTS, length), F32),
            pltpu.VMEM((SLOTS, length), F32),
            pltpu.VMEM((length, 2 * SLOTS), F32),
            pltpu.VMEM((blocks, 1, width), F32),
            pltpu.VMEM((blocks, 1, width), F32),
            pltpu.VMEM((blocks, state_len, width), F32),
            pltpu.VMEM((length, width), F32),
            pltpu.VMEM((state_len, width), F32),
            pltpu.VMEM((1, width), F32),
            pltpu.VMEM((packet_rows, width), BF16),
            pltpu.VMEM((packet_rows, half), BF16),
            pltpu.VMEM((state_len, half), F32),
            pltpu.VMEM((1, half), F32),
            pltpu.VMEM((SIDE, packet_rows, half), BF16),
            pltpu.VMEM((SIDE, packet_rows, half), BF16),
            pltpu.VMEM((state_len, half), F32),
            pltpu.VMEM((1, half), F32),
            pltpu.VMEM((state_len, width), F32),
            pltpu.VMEM((state_len, half), F32),
            pltpu.VMEM((3, SIDE, SIDE, 2, wrows, hid), BF16),
            pltpu.VMEM((SIDE, SIDE, SIDE, 2, orow, features), BF16),
            pltpu.VMEM((SIDE, step_rows, SIDE * width), BF16),
            pltpu.VMEM((SIDE, SIDE, sub, features), BF16),
            pltpu.VMEM((step_rows, features), F32),
            pltpu.VMEM((SIDE, step_rows, features), BF16),
            pltpu.VMEM((2, step_rows, hid), BF16),
            pltpu.VMEM((SIDE, step_rows, features), BF16),
            pltpu.VMEM((SIDE, sub, features // 2), BF16),
            pltpu.VMEM((SIDE, sub, features // 2), BF16),
            pltpu.VMEM((SIDE, sub, features), BF16),
            pltpu.VMEM((SIDE, sub, features), BF16),
            pltpu.SemaphoreType.DMA((messages,)),
            pltpu.SemaphoreType.DMA((messages,)),
            pltpu.SemaphoreType.DMA((16,)),
        ],
        compiler_params=pltpu.CompilerParams(
            collective_id=0, has_side_effects=True, vmem_limit_bytes=VMEM_LIMIT
        ),
        cost_estimate=pl.CostEstimate(
            flops=40_000_000_000, bytes_accessed=60_000_000, transcendentals=0
        ),
        name="layer",
    )(
        residual.reshape(SIDE, SIDE, sub, features),
        small_heads,
        large_heads,
        key_rows,
        query_rows,
        small_gate,
        large_gate,
        small_step.T,
        large_step.T,
        small_decay,
        large_decay,
        small_taps,
        large_taps,
        key_taps,
        query_taps,
        small_gain,
        large_gain,
        small_out.reshape(out_shape),
        large_out.reshape(out_shape),
        mixer_gain,
        ffn_in_gain,
        ffn_out_gain,
        gate_proj,
        up_proj,
        down_proj,
    )


def solution(mesh):
    placed = (
        P("sp", None),
        P("sp", "tp"),
        P("sp", "tp"),
        P("sp", "tp", None),
        P("sp", "tp", None),
        P("sp", "tp"),
        P("sp", "tp"),
        P("sp", "tp"),
        P("sp", "tp"),
        P(None, "tp"),
        P(None, "tp"),
        P(None, "tp", None),
        P(None, "tp", None),
        P("tp"),
        P("tp"),
        P("tp"),
        P("tp"),
        P("tp", None),
        P("tp", None),
        P(),
        P(),
        P("sp", "tp"),
        P("sp", "tp"),
        P("sp", "tp"),
        P(),
    )
    return jax.shard_map(
        local_program, mesh=mesh, in_specs=placed, out_specs=P(("sp", "tp"), None), check_vma=False
    )
```

```python
import functools

import jax
import jax.numpy as jnp
from jax import lax
from jax.experimental import pallas as pl
from jax.experimental.pallas import tpu as pltpu
from jax.sharding import PartitionSpec as P

BLOCK = 128
HALO = 16
LANES = 128
SLOTS = 8
TAIL = 16
SIDE = 4

EPS = 1e-06
FAR = -1e30
F32 = jnp.float32
BF16 = jnp.bfloat16
MESH = pl.DeviceIdType.MESH
scope = jax.named_scope
VMEM_LIMIT = 66_000_000


def silu(x):
    return x / (1.0 + jnp.exp(-x))


def softplus(x):
    return jnp.maximum(x, 0.0) + jnp.log1p(jnp.exp(-jnp.abs(x)))


def exact_dot(a, b, dims=(((1,), (0,)), ((), ()))):
    return lax.dot_general(a, b, dims, precision=lax.Precision.HIGHEST, preferred_element_type=F32)


def lower(n):
    rows = lax.broadcasted_iota(jnp.int32, (n, n), 0)
    return rows >= lax.broadcasted_iota(jnp.int32, (n, n), 1)


def spread(columns, heads, dim):
    rows = columns.shape[0]
    parts = []
    if dim >= LANES:
        for h in heads:
            parts.append(jnp.broadcast_to(columns[:, h : h + 1], (rows, dim)))
    else:
        per = LANES // dim
        lane = lax.broadcasted_iota(jnp.int32, (rows, LANES), 1)
        for first in range(0, len(heads), per):
            part = jnp.broadcast_to(columns[:, heads[first] : heads[first] + 1], (rows, LANES))
            for j in range(1, per):
                h = heads[first + j]
                part = jnp.where(lane >= j * dim, columns[:, h : h + 1], part)
            parts.append(part)
    return jnp.concatenate(parts, axis=1)


def unit_rms(values):
    return values * lax.rsqrt(jnp.mean(values * values, axis=-1, keepdims=True) + EPS)


def pack(ref, slot, state, log):
    rows = state.shape[0]
    high = log.astype(BF16).astype(F32)
    row = lax.broadcasted_iota(jnp.int32, (TAIL, log.shape[1]), 0)
    both = jnp.where(row == 0, high, jnp.where(row == 1, log - high, 0.0))
    if slot is None:
        ref[:rows] = state.astype(BF16)
        ref[rows:] = both.astype(BF16)
    else:
        ref[slot, :rows] = state.astype(BF16)
        ref[slot, rows:] = both.astype(BF16)


def opened(packet, rows):
    log = packet[rows : rows + TAIL].astype(F32)
    return packet[:rows].astype(F32), log[0:1] + log[1:2]


class Counter:
    def __init__(self):
        self.n = 0

    def take(self, count=1):
        first = self.n
        self.n += count
        return first


def tile_list(width, tile):
    return [(s, min(tile, width - s)) for s in range(0, width, tile)]


def whole_kernel(
    sizes,
    res_in,
    small_in,
    large_in,
    key_in,
    query_in,
    small_gate_in,
    large_gate_in,
    small_step,
    large_step,
    small_decay,
    large_decay,
    small_taps,
    large_taps,
    key_taps,
    query_taps,
    small_gain,
    large_gain,
    small_out,
    large_out,
    mixer_gain,
    in_gain,
    out_gain,
    gate_in,
    up_in,
    down_in,
    out,
    xin,
    kin,
    gates,
    woven,
    conv,
    taps,
    pattern,
    gain,
    dt_rows,
    cum_rows,
    cums,
    logs,
    tails,
    starts,
    inside,
    state,
    total,
    packet,
    from_partner,
    first_state,
    first_log,
    along_y,
    along_z,
    row_state,
    row_log,
    entering,
    for_partner,
    w,
    o,
    heads,
    res,
    ninbuf,
    hidden,
    parts,
    ra,
    rb,
    rc,
    rd,
    send,
    recv,
    local,
):
    (heads_a, dim_a), (heads_b, dim_b), state_len, blocks = sizes
    head_list_a = list(range(heads_a))
    head_list_b = list(range(heads_a, heads_a + heads_b))
    width_a = heads_a * dim_a
    width_b = heads_b * dim_b
    width = width_a + width_b
    groups = (
        (head_list_a, dim_a, width_a, 0),
        (head_list_b, dim_b, width_b, width_a),
    )

    sp = lax.axis_index("sp")
    x = lax.axis_index("tp")
    c = lax.rem(sp, 2)
    y = lax.rem(sp // 2, SIDE)
    z = sp // (2 * SIDE)
    zy = sp // 2
    count_sp = lax.axis_size("sp")

    def turn(v, d):
        return lax.rem(v + d + SIDE, SIDE)

    def at_chip(zz, yy):
        return ((zz * SIDE + yy) * 2 + c, x)

    partner = (sp + 1 - 2 * c, x)
    xs = {d: (sp, turn(x, d)) for d in (1, -1, 2)}
    ys = {d: at_chip(z, turn(y, d)) for d in (1, -1, 2)}
    zs = {d: at_chip(turn(z, d), y) for d in (1, -1, 2)}
    after = (lax.rem(sp + 1, count_sp), x)
    prior = (lax.rem(sp + count_sp - 1, count_sp), x)

    barrier = pltpu.get_barrier_semaphore()
    greeted = [partner, after, prior] + [v[d] for v in (xs, ys, zs) for d in (1, -1, 2)]
    for peer in greeted:
        pl.semaphore_signal(barrier, inc=1, device_id=peer, device_id_type=MESH)

    counter = Counter()
    issued = []

    def message(src, dst, target, index):
        return pltpu.make_async_remote_copy(
            src_ref=src,
            dst_ref=dst,
            send_sem=send.at[index],
            recv_sem=recv.at[index],
            device_id=target,
            device_id_type=MESH,
        )

    def post(src, dst, landing, target):
        index = counter.take()
        copy = message(src, dst, target, index)
        copy.start()
        issued.append(copy)
        return message(landing, landing, target, index)

    def wait_all(arrivals, name="wait"):
        with scope(name):
            for arrival in arrivals:
                arrival.wait_recv()

    def run(name, first, last, body):
        with scope(name):
            lax.fori_loop(first, last, body, 0)

    loads = []

    def load(src, dst):
        copy = pltpu.make_async_copy(src, dst, local.at[len(loads)])
        copy.start()
        loads.append(copy)
        return copy

    length = small_in.shape[0]
    weight_loads = [
        load(ref, w.at[m, z, y, c]) for m, ref in enumerate((gate_in, up_in, down_in))
    ]
    conv_loads = [
        load(ref, xin.at[g, pl.ds(HALO, length)]) for g, ref in enumerate((small_in, large_in))
    ]
    conv_loads += [
        load(ref, kin.at[g, pl.ds(2 * HALO, 2 * length)])
        for g, ref in enumerate((key_in, query_in))
    ]
    out_loads = [
        load(ref, o.at[x, pl.ds(first, SIDE // 2)])
        for ref, first in ((small_out, 0), (large_out, SIDE // 2))
    ]
    kernel_len = small_taps.shape[0]
    taps[:, :width_a] = small_taps[...].astype(F32)
    taps[:, width_a:width] = large_taps[...].astype(F32)
    pair_row = lax.broadcasted_iota(jnp.int32, (SLOTS, LANES), 0)
    for g, ref in enumerate((key_taps, query_taps)):
        for k in range(kernel_len):
            pattern[g, k] = jnp.where(
                pair_row % 2 == 0, ref[k, 0:1].astype(F32), ref[k, 1:2].astype(F32)
            )
    gain[:, :width_a] = small_gain[...].astype(F32).reshape(1, width_a)
    gain[:, width_a:] = large_gain[...].astype(F32).reshape(1, width_b)
    dt_rows[...] = jnp.zeros_like(dt_rows)
    dt_rows[:heads_a] = softplus(small_step[...])
    dt_rows[heads_a : heads_a + heads_b] = softplus(large_step[...])
    head_row = lax.broadcasted_iota(jnp.int32, (SLOTS, BLOCK), 0)
    rate = jnp.zeros((SLOTS, BLOCK), F32)
    for h in range(heads_a + heads_b):
        value = small_decay[h] if h < heads_a else large_decay[h - heads_a]
        rate = jnp.where(head_row == h, value, rate)
    rate = jnp.exp(rate)
    row_id = lax.broadcasted_iota(jnp.int32, (BLOCK, BLOCK), 0)
    col_id = lax.broadcasted_iota(jnp.int32, (BLOCK, BLOCK), 1)
    with scope("decays"):
        pieces = [dt_rows[:, i * BLOCK : (i + 1) * BLOCK] for i in range(blocks)]
        dt_all = jnp.concatenate(pieces, axis=0)
        rate_all = jnp.concatenate([rate] * blocks, axis=0)
        cum_all = exact_dot(-dt_all * rate_all, (row_id <= col_id).astype(F32))
        scale_all = dt_all * jnp.exp(cum_all[:, BLOCK - 1 : BLOCK] - cum_all)
        eye = (row_id == col_id).astype(F32)
        turned = exact_dot(
            eye, jnp.concatenate([cum_all, scale_all], axis=0), (((1,), (1,)), ((), ()))
        )
        before = jnp.zeros((1, SLOTS), F32)
        for i in range(blocks):
            rows = slice(i * BLOCK, (i + 1) * BLOCK)
            heads_at = slice(i * SLOTS, (i + 1) * SLOTS)
            scales_at = slice((blocks + i) * SLOTS, (blocks + i + 1) * SLOTS)
            cum_rows[:, rows] = cum_all[heads_at]
            cums[rows, :SLOTS] = turned[:, heads_at]
            cums[rows, SLOTS:] = turned[:, scales_at]
            tail = turned[BLOCK - 1 : BLOCK, heads_at]
            for buffer, value in ((logs, before), (tails, tail)):
                buffer[i] = jnp.concatenate(
                    [spread(value, head_list_a, dim_a), spread(value, head_list_b, dim_b)], axis=1
                )
            before = before + tail
        final_log = jnp.concatenate(
            [spread(before, head_list_a, dim_a), spread(before, head_list_b, dim_b)], axis=1
        )
        total[...] = final_log
    with scope("barrier"):
        pl.semaphore_wait(barrier, len(greeted))

    halo = []
    for g, ref in enumerate((small_in, large_in)):
        first = xin.at[g, pl.ds(0, HALO)]
        halo.append(post(ref.at[pl.ds(length - HALO, HALO)], first, first, after))
    for g, ref in enumerate((key_in, query_in)):
        first = kin.at[g, pl.ds(0, 2 * HALO)]
        halo.append(post(ref.at[pl.ds(2 * (length - HALO), 2 * HALO)], first, first, after))

    near_cols = w.shape[5] // LANES // 2 * LANES

    def cell(kind, h, first_axis, offset, q=None, m=None, core=c):
        if first_axis:
            zz, yy = (z, turn(y, offset)) if h == 0 else (turn(z, offset), y)
        else:
            zz, yy = (turn(z, offset), slice(None)) if h == 0 else (slice(None), turn(y, offset))
        if kind == "o":
            extent = o.shape[5] // 2 if q is None else o.shape[5] // 4
            part = pl.ds(h * (o.shape[5] // 2) + (0 if q is None else q) * extent, extent)
            return o.at[turn(x, 2), zz, yy, core, slice(None), part]
        extent = w.shape[4] if q is None else w.shape[4] // 2
        rows = pl.ds((0 if q is None else q) * extent, extent)
        cols = pl.ds(0, near_cols) if h == 0 else pl.ds(near_cols, w.shape[5] - near_cols)
        return w.at[slice(None) if m is None else m, zz, yy, core, rows, cols]

    def target_of(h, first_axis, d):
        return (ys if (h == 0) == first_axis else zs)[d]

    def spread_over(kind, first_axis, hs=(0, 1), m=None, q=None):
        arrivals = []
        for h in hs:
            for d in (1, -1):
                src = cell(kind, h, first_axis, 0, q, m)
                landing = cell(kind, h, first_axis, -d, q, m)
                arrivals.append(post(src, src, landing, target_of(h, first_axis, d)))
        return arrivals

    def forward_over(kind, first_axis, m=None, hs=(0, 1)):
        arrivals = []
        for h in hs:
            for d, q in ((1, 0), (-1, 1)):
                src = cell(kind, h, first_axis, -d, q, m)
                landing = cell(kind, h, first_axis, -2 * d, q, m)
                arrivals.append(post(src, src, landing, target_of(h, first_axis, d)))
        return arrivals

    def mirror_over(kind, offsets, m=None):
        arrivals = []
        for h in (0, 1):
            for offset in offsets:
                src = cell(kind, h, False, offset, m=m)
                landing = cell(kind, h, False, offset, m=m, core=1 - c)
                arrivals.append(post(src, src, landing, partner))
        return arrivals

    with scope("loads"):
        for copy in weight_loads + out_loads:
            copy.wait()
    mine_out = o.at[x, z, y, c]
    o_entry = [post(mine_out, mine_out, o.at[turn(x, 2), z, y, c], xs[2])]
    w_first = spread_over("w", True)

    def orows(offset, core):
        return o.at[turn(x, offset), pl.ds(core * (SIDE // 2), SIDE // 2)]

    o_near = [post(orows(0, c), orows(0, c), orows(-d, c), xs[d]) for d in (1, -1)]

    gate_loads = [
        load(ref, gates.at[g]) for g, ref in enumerate((small_gate_in, large_gate_in))
    ]
    res_loads = [load(res_in.at[:, k], res.at[k]) for k in range(SIDE)]
    state[...] = jnp.zeros_like(state)

    with scope("conv_loads"):
        for copy in conv_loads:
            copy.wait()
    def convolve(g, at):
        for first_lane in range(0, xin.shape[2], LANES):
            here = pl.ds(g * xin.shape[2] + first_lane, LANES)
            extended = xin[g, pl.ds(at, BLOCK + HALO), pl.ds(first_lane, LANES)].astype(F32)
            summed = None
            for k in range(kernel_len):
                first = HALO - kernel_len + 1 + k
                term = taps[k : k + 1, here] * extended[first : first + BLOCK]
                summed = term if summed is None else summed + term
            conv[pl.ds(at, BLOCK), here] = silu(summed).astype(BF16)

    def convolve_pair(g, at):
        span = 2 * BLOCK
        rows = pl.ds(pl.multiple_of(2 * at, span), span + 2 * HALO)
        extended = kin[g, rows].astype(F32)
        summed = None
        for k in range(kernel_len):
            first = 2 * (HALO - kernel_len + 1 + k)
            window = extended[first : first + span].reshape(span // SLOTS, SLOTS, LANES)
            term = window * pattern[g, k][None]
            summed = term if summed is None else summed + term
        woven[...] = silu(summed).reshape(span, LANES)
        for j in range(2):
            column = width + (2 * g + j) * state_len
            conv[pl.ds(at, BLOCK), column : column + LANES] = woven[
                pl.ds(j, BLOCK, stride=2), :
            ].astype(BF16)

    def convolve_three(i, carry):
        at = pl.multiple_of(i * BLOCK, BLOCK)
        convolve(0, at)
        convolve(1, at)
        convolve_pair(0, at)
        return carry

    def states(i, carry):
        at = pl.multiple_of(i * BLOCK, BLOCK)
        rows = pl.ds(at, BLOCK)
        scale = cums[rows, SLOTS:]
        kept = jnp.exp(tails[i])
        for which, (head_list, dim, wide, offset) in enumerate(groups):
            key_at = width + which * state_len
            columns = slice(offset, offset + wide)
            heads_here = list(range(len(head_list)))
            shifted = scale[:, head_list[0] : head_list[-1] + 1]
            xv = conv[rows, columns].astype(F32)
            u = (xv * spread(shifted, heads_here, dim)).astype(BF16)
            k = conv[rows, key_at : key_at + state_len]
            fresh = lax.dot_general(k, u, (((0,), (0,)), ((), ())), preferred_element_type=F32)
            old = state[:, columns]
            starts[i, :, columns] = old
            state[:, columns] = old * kept[:, columns] + fresh
        return carry

    run("conv1", 1, blocks, convolve_three)
    wait_all(halo, "halo")
    for g in range(2):
        for buffer, size in ((xin, HALO), (kin, 2 * HALO)):
            edge = buffer[g, :size].astype(F32)
            buffer[g, :size] = jnp.where(sp == 0, 0.0, edge).astype(BF16)
    run("conv0", 0, 1, convolve_three)
    run("states", 0, blocks, states)

    half = width // 2

    def half_of(core):
        return pl.ds(pl.multiple_of(core * half, half), half)

    pack(packet, None, state[...], total[...])
    swapped = post(packet.at[:, half_of(1 - c)], from_partner, from_partner, partner)

    def queries(i, carry):
        convolve_pair(1, pl.multiple_of(i * BLOCK, BLOCK))
        return carry

    def mix_inside(i, carry):
        at = pl.multiple_of(i * BLOCK, BLOCK)
        rows = pl.ds(at, BLOCK)
        causal = row_id >= col_id
        dt_across = dt_rows[:, rows]
        cum = cums[rows]
        cum_across = cum_rows[:, rows]
        lane = lax.broadcasted_iota(jnp.int32, (BLOCK, LANES), 1)
        for which, (head_list, dim, wide, offset) in enumerate(groups):
            key_at = width + which * state_len
            query_at = key_at + 2 * state_len
            k = conv[rows, key_at : key_at + state_len]
            q = conv[rows, query_at : query_at + state_len]
            scores = lax.dot_general(q, k, (((1,), (1,)), ((), ())), preferred_element_type=F32)
            span = max(dim, LANES)
            per = span // dim
            for first in range(0, len(head_list), per):
                columns = slice(offset + first * dim, offset + first * dim + span)
                x_part = conv[rows, columns]
                part = None
                for j in range(per):
                    h = head_list[first + j]
                    gap = cum[:, h : h + 1] - cum_across[h : h + 1]
                    decays = jnp.exp(jnp.where(causal, gap, FAR))
                    weight = (scores * decays * dt_across[h : h + 1]).astype(BF16)
                    got = jnp.dot(weight, x_part, preferred_element_type=F32)
                    part = got if part is None else jnp.where(lane >= j * dim, got, part)
                inside[rows, columns] = part
        return carry

    def send_along(buffer, targets):
        arrivals = []
        for d, slot in ((1, 1), (-1, 3), (2, 2)):
            landing = buffer.at[slot]
            arrivals.append(post(buffer.at[0], landing, landing, targets[d]))
        return arrivals

    def fold(buffer, place, number):
        zero = jnp.zeros((state_len, half), F32)
        every, every_log = zero, jnp.zeros((1, half), F32)
        ahead, ahead_log = every, every_log
        for p in range(number):
            slot = turn(place, -p)
            one, log = opened(buffer[slot], state_len)
            counts = p < place
            ahead = jnp.where(counts, ahead * jnp.exp(log) + one, ahead)
            ahead_log = jnp.where(counts, ahead_log + log, ahead_log)
            every = every * jnp.exp(log) + one
            every_log = every_log + log
        return every, every_log, ahead, ahead_log

    wait_all(w_first[2:], "w_first_z")
    w_second_z = forward_over("w", True, hs=(1,))
    wait_all(o_entry, "o_entry")
    o_first_z = spread_over("o", True, (1,))
    run("queries", 0, blocks, queries)
    wait_all([swapped], "swap_wait")
    mine, mine_log = opened(packet[:, half_of(c)], state_len)
    theirs, theirs_log = opened(from_partner[...], state_len)
    even = c == 0
    a_state = jnp.where(even, mine, theirs)
    a_log = jnp.where(even, mine_log, theirs_log)
    b_state = jnp.where(even, theirs, mine)
    b_log = jnp.where(even, theirs_log, mine_log)
    first_state[...] = a_state
    first_log[...] = a_log
    pack(along_y, 0, a_state * jnp.exp(b_log) + b_state, a_log + b_log)
    y_arrivals = send_along(along_y, ys)
    wait_all(w_first[:2], "w_first_y")
    w_second_y = forward_over("w", True, hs=(0,))
    o_first_y = spread_over("o", True, (0,))
    run("mix0", 0, 4, mix_inside)
    wait_all(o_first_z, "o_first_z")
    o_second_z = forward_over("o", True, hs=(1,))
    wait_all(y_arrivals, "y_wait")
    row_all, row_all_log, row_ahead, row_ahead_log = fold(along_y, y, SIDE)
    row_state[...] = row_ahead
    row_log[...] = row_ahead_log
    pack(along_z, 0, row_all, row_all_log)
    z_arrivals = send_along(along_z, zs)
    wait_all(o_second_z, "o_second_z")
    o_third = spread_over("o", False, (1,))
    run("mix4", 4, 6, mix_inside)
    wait_all(o_first_y, "o_first_y")
    o_second_y = forward_over("o", True, hs=(0,))
    wait_all(w_second_z, "w_second_z")
    w_third = {0: spread_over("w", False, (1,), 0)}
    wait_all(w_second_y, "w_second_y")
    w_third[0] += spread_over("w", False, (0,), 0)
    run("mix6", 6, blocks, mix_inside)
    wait_all(z_arrivals, "z_wait")
    _, _, plane_ahead, _ = fold(along_z, z, SIDE - 1)
    chip = plane_ahead * jnp.exp(row_log[...]) + row_state[...]
    second = chip * jnp.exp(first_log[...]) + first_state[...]
    entering[:, half_of(c)] = jnp.where(even, chip, second)
    for_partner[...] = jnp.where(even, second, chip)
    entered = post(
        for_partner, entering.at[:, half_of(c)], entering.at[:, half_of(1 - c)], partner
    )
    wait_all(o_second_y, "o_second_y")
    o_third += spread_over("o", False, (0,))
    w_third[1] = spread_over("w", False, (1,), 1)
    w_mirrored = {m: mirror_over("w", (0,), m) for m in range(3)}
    o_mirrored = mirror_over("o", (0,))

    sub = length // (SIDE * SIDE)
    lane = lax.broadcasted_iota(jnp.int32, (BLOCK, LANES), 1)

    def carry_block(n, carry):
        stage = n // SIDE
        d = lax.rem(n, SIDE)
        i = 2 * d + stage
        rows = pl.ds(pl.multiple_of(i * BLOCK, BLOCK), BLOCK)
        grown = jnp.exp(cums[rows])
        for which, (head_list, dim, wide, offset) in enumerate(groups):
            columns = slice(offset, offset + wide)
            query_at = width + (2 + which) * state_len
            q = conv[rows, query_at : query_at + state_len]
            old = starts[i, :, columns] + entering[:, columns] * jnp.exp(logs[i, :, columns])
            carried = jnp.dot(q, old.astype(BF16), preferred_element_type=F32)
            mixed = inside[rows, columns] + carried * spread(grown, head_list, dim)
            gated = mixed * silu(gates[which, rows].astype(F32))
            squares = gated * gated
            span = max(dim, LANES)
            per = span // dim
            normed = []
            for first in range(0, len(head_list), per):
                at = first * dim
                part = squares[:, at : at + span]
                means = None
                for j in range(per):
                    if per == 1:
                        means = jnp.sum(part, axis=1, keepdims=True)
                    else:
                        ours = (lane >= j * dim) & (lane < (j + 1) * dim)
                        one = jnp.sum(jnp.where(ours, part, 0.0), axis=1, keepdims=True)
                        means = one if means is None else jnp.where(lane >= j * dim, one, means)
                normed.append(gated[:, at : at + span] * lax.rsqrt(means * (1.0 / dim) + EPS))
            normed = (jnp.concatenate(normed, axis=1) * gain[:, columns]).astype(BF16)
            place = pl.ds(pl.multiple_of(x * width + offset, LANES), wide)
            spot = pl.ds(pl.multiple_of(d * sub, sub), sub)
            heads[2 * stage, spot, place] = normed[:sub]
            heads[2 * stage + 1, spot, place] = normed[sub:]
        return carry

    def hcols(offset):
        return pl.ds(pl.multiple_of(turn(x, offset) * width, LANES), width)

    step_rows = heads.shape[1]
    g1 = {d: counter.take(SIDE) for d in (1, -1)}
    g2 = {d: counter.take(SIDE) for d in (1, -1)}

    def heads_out(k, d):
        src = heads.at[k, :, hcols(0)]
        return message(src, src, xs[d], g1[d] + k)

    def heads_in(k, d):
        landing = heads.at[k, :, hcols(-d)]
        return message(landing, landing, xs[d], g1[d] + k)

    def far_rows(d):
        return pl.ds(0 if d == 1 else step_rows // 2, step_rows // 2)

    def heads_on(k, d):
        src = heads.at[k, far_rows(d), hcols(-d)]
        return message(src, src, xs[d], g2[d] + k)

    def heads_far(k, d):
        landing = heads.at[k, far_rows(d), hcols(-2 * d)]
        return message(landing, landing, xs[d], g2[d] + k)

    def start_heads(k):
        for d in (1, -1):
            heads_out(k, d).start()

    def forward_heads(k):
        with scope("heads_in"):
            for d in (1, -1):
                heads_in(k, d).wait_recv()
        for d in (1, -1):
            heads_on(k, d).start()

    features = res.shape[3]
    hid = hidden.shape[2]
    side_half = features // 2
    r1 = {d: counter.take(SIDE) for d in (1, -1)}
    r2 = {d: counter.take(SIDE) for d in (1, -1)}

    def prow(offset):
        return pl.ds(pl.multiple_of(turn(x, offset) * sub, sub), sub)

    def project(k):
        with scope("heads_far"):
            for d in (1, -1):
                heads_far(k, d).wait_recv()
        with scope("out_dot"):
            left = heads[k]
            for n, (first, size) in enumerate(tile_list(features, width)):
                inside[n * step_rows : (n + 1) * step_rows] = jnp.dot(
                    left,
                    o[..., first : first + size].reshape(SIDE * width, size),
                    preferred_element_type=F32,
                )
        with scope("norms"):
            outer = mixer_gain[...].astype(F32).reshape(1, features)
            inner = in_gain[...].astype(F32).reshape(1, features)
            for d in range(SIDE):
                tiles = [
                    slice(n * step_rows + d * sub, n * step_rows + (d + 1) * sub)
                    for n in range(SIDE)
                ]
                mix = jnp.concatenate([inside[t] for t in tiles], axis=1)
                mixed = res[k, d].astype(F32) + unit_rms(mix) * outer
                for n, t in enumerate(tiles):
                    inside[t] = mixed[:, n * width : (n + 1) * width]
                ninbuf[k, d * sub : (d + 1) * sub] = (unit_rms(mixed) * inner).astype(BF16)
            for j in range(SIDE):
                spot = slice((j % 2) * sub, (j % 2 + 1) * sub)
                own = pl.ds(pl.multiple_of(j * step_rows + x * sub, sub), sub)
                starts[2 * k + j // 2, spot] = inside[own]

    w_fourth = {}

    def pass_weights(m):
        wait_all(w_third[m], "w_third")
        w_fourth[m] = forward_over("w", False, m)
        w_mirrored[m] += mirror_over("w", (1, -1), m)

    def settle_weights(m):
        wait_all(w_fourth[m], "w_fourth")
        w_mirrored[m] += mirror_over("w", (2,), m)

    wait_all([entered], "enter_wait")
    for copy in gate_loads:
        copy.wait()
    run("carry1", 0, SIDE, carry_block)
    start_heads(0)
    start_heads(1)
    run("carry2", SIDE, 2 * SIDE, carry_block)
    wait_all(o_near, "o_near")
    for d in (1, -1):
        o_mirrored.append(post(orows(d, c), orows(d, c), orows(d, 1 - c), partner))
    wait_all(o_third, "o_third")
    o_fourth = forward_over("o", False)
    o_mirrored += mirror_over("o", (1, -1))
    w_third[1] += spread_over("w", False, (0,), 1)
    pass_weights(0)
    w_third[2] = spread_over("w", False, (1, 0), 2)
    forward_heads(0)
    start_heads(2)
    wait_all(o_fourth, "o_fourth")
    o_mirrored += mirror_over("o", (2,))
    forward_heads(1)
    start_heads(3)
    for copy in res_loads:
        copy.wait()
    wait_all(o_mirrored, "o_mirrored")
    def gate_only(k):
        with scope("gate"):
            nin = ninbuf[k]
            for first, size in tile_list(hid, 512):
                wg = w[0, :, :, :, :, first : first + size].reshape(features, size)
                gate = jnp.dot(nin, wg, preferred_element_type=F32)
                hidden[k % 2, :, first : first + size] = silu(gate).astype(BF16)

    def up_only(k, between=None):
        with scope("up"):
            nin = ninbuf[k]
            for first, size in tile_list(hid, 512):
                if between is not None and first == 1024:
                    between()
                wu = w[1, :, :, :, :, first : first + size].reshape(features, size)
                up = jnp.dot(nin, wu, preferred_element_type=F32)
                gated = hidden[k % 2, :, first : first + size].astype(F32)
                hidden[k % 2, :, first : first + size] = (gated * up).astype(BF16)

    project(0)
    pass_weights(1)
    settle_weights(0)
    forward_heads(2)
    wait_all(w_mirrored[0], "w_mirrored0")
    gate_only(0)
    project(1)
    pass_weights(2)
    gate_only(1)
    forward_heads(3)
    settle_weights(1)
    wait_all(w_mirrored[1], "w_mirrored1")

    def far_out(k, d):
        lanes = pl.ds(0 if d == 1 else side_half, side_half)
        landing = (ra if d == 1 else rb).at[k]
        return message(parts.at[k, prow(2), lanes], landing, xs[d], r1[d] + k)

    def near_out(k, d):
        landing = (rc if d == 1 else rd).at[k]
        return message(parts.at[k, prow(d)], landing, xs[d], r2[d] + k)

    def pass_on(k):
        for d in (1, -1):
            with scope("far_wait"):
                far_out(k, d).wait_recv()
            lanes = slice(0, side_half) if d == 1 else slice(side_half, features)
            extra = (ra if d == 1 else rb)[k].astype(F32)
            mine = parts[k, prow(d), lanes].astype(F32)
            parts[k, prow(d), lanes] = (mine + extra).astype(BF16)
            near_out(k, d).start()

    def gate_up(k):
        with scope("gate_up"):
            nin = ninbuf[k]
            for first, size in tile_list(hid, 512):
                wg = w[0, :, :, :, :, first : first + size].reshape(features, size)
                wu = w[1, :, :, :, :, first : first + size].reshape(features, size)
                gate = jnp.dot(nin, wg, preferred_element_type=F32)
                up = jnp.dot(nin, wu, preferred_element_type=F32)
                hidden[lax.rem(k, 2), :, first : first + size] = (silu(gate) * up).astype(BF16)

    def down(k):
        with scope("down"):
            hv = hidden[lax.rem(k, 2)]
            tile = features // SIDE
            for n in range(SIDE):
                wd = w[2, n].reshape(tile, hid)
                got = lax.dot_general(hv, wd, (((1,), (1,)), ((), ())), preferred_element_type=F32)
                parts[k, :, n * tile : (n + 1) * tile] = got.astype(BF16)
            for d in (1, -1):
                far_out(k, d).start()

    def down_pair(k, carry):
        down(k)
        return carry

    def channel_mix(k, carry):
        project(k)

        @pl.when(k == 2)
        def _():
            pass_on(0)

        gate_up(k)

        @pl.when(k == 2)
        def _():
            pass_on(1)

        down(k)
        return carry

    up_only(0, lambda: settle_weights(2))
    up_only(1)
    wait_all(w_mirrored[2], "w_mirrored2")
    lax.fori_loop(0, 2, down_pair, 0)
    lax.fori_loop(2, SIDE, channel_mix, 0)
    outer = 0.5 * out_gain[...].astype(F32).reshape(1, features)

    def finish(k):
        with scope("near_wait"):
            for d in (1, -1):
                near_out(k, d).wait_recv()
        ffn = parts[k, prow(0)].astype(F32) + rc[k].astype(F32) + rd[k].astype(F32)
        kept = [
            starts[2 * k + j // 2, (j % 2) * sub : (j % 2 + 1) * sub] for j in range(SIDE)
        ]
        updated = jnp.concatenate(kept, axis=1) + unit_rms(ffn) * outer
        out[k * sub : (k + 1) * sub] = updated.astype(BF16)

    pass_on(SIDE - 2)
    finish(0)
    finish(1)
    pass_on(SIDE - 1)
    finish(2)
    finish(SIDE - 1)

    with scope("drain"):
        for copy in issued:
            copy.wait_send()

    def drain(k, carry):
        for d in (1, -1):
            heads_out(k, d).wait_send()
            heads_on(k, d).wait_send()
            far_out(k, d).wait_send()
            near_out(k, d).wait_send()
        return carry

    lax.fori_loop(0, SIDE, drain, 0)


def local_program(
    residual,
    small_heads,
    large_heads,
    state_keys,
    state_queries,
    small_gate,
    large_gate,
    small_step,
    large_step,
    small_taps,
    large_taps,
    key_taps,
    query_taps,
    small_decay,
    large_decay,
    small_gain,
    large_gain,
    small_out,
    large_out,
    mixer_gain,
    ffn_in_gain,
    gate_proj,
    up_proj,
    down_proj,
    ffn_out_gain,
):
    length, features = residual.shape
    state_len = state_keys.shape[-1]
    key_rows = state_keys.reshape(-1, state_len)
    query_rows = state_queries.reshape(-1, state_len)
    heads_a = small_step.shape[1]
    heads_b = large_step.shape[1]
    heads = heads_a + heads_b
    width_a = small_heads.shape[1]
    width_b = large_heads.shape[1]
    width = width_a + width_b
    everything = width + 2 * state_len * state_keys.shape[1]
    blocks = length // BLOCK
    sizes = ((heads_a, width_a // heads_a), (heads_b, width_b // heads_b), state_len, blocks)
    kernel_len = small_taps.shape[0]
    sub = length // (SIDE * SIDE)
    step_rows = SIDE * sub
    wrows, hid = gate_proj.shape
    orow = width // (2 * SIDE * SIDE)
    out_shape = (SIDE // 2, SIDE, 2, orow, features)
    half = width // 2
    packet_rows = state_len + TAIL
    any_space = pl.BlockSpec(memory_space=pl.ANY)
    vmem = pl.BlockSpec(memory_space=pltpu.VMEM)
    smem = pl.BlockSpec(memory_space=pltpu.SMEM)
    messages = 160

    return pl.pallas_call(
        functools.partial(whole_kernel, sizes),
        in_specs=[any_space] * 7
        + [vmem] * 2
        + [smem] * 2
        + [vmem] * 6
        + [any_space] * 2
        + [vmem] * 3
        + [any_space] * 3,
        out_specs=vmem,
        out_shape=jax.ShapeDtypeStruct((length // SIDE, features), BF16),
        scratch_shapes=[
            pltpu.VMEM((2, HALO + length, width_a), BF16),
            pltpu.VMEM((2, 2 * (HALO + length), state_len), BF16),
            pltpu.VMEM((2, length, width_a), BF16),
            pltpu.VMEM((2 * BLOCK, state_len), F32),
            pltpu.VMEM((length, everything), BF16),
            pltpu.VMEM((kernel_len, width), F32),
            pltpu.VMEM((2, kernel_len, SLOTS, state_len), F32),
            pltpu.VMEM((1, width), F32),
            pltpu.VMEM((SLOTS, length), F32),
            pltpu.VMEM((SLOTS, length), F32),
            pltpu.VMEM((length, 2 * SLOTS), F32),
            pltpu.VMEM((blocks, 1, width), F32),
            pltpu.VMEM((blocks, 1, width), F32),
            pltpu.VMEM((blocks, state_len, width), F32),
            pltpu.VMEM((length, width), F32),
            pltpu.VMEM((state_len, width), F32),
            pltpu.VMEM((1, width), F32),
            pltpu.VMEM((packet_rows, width), BF16),
            pltpu.VMEM((packet_rows, half), BF16),
            pltpu.VMEM((state_len, half), F32),
            pltpu.VMEM((1, half), F32),
            pltpu.VMEM((SIDE, packet_rows, half), BF16),
            pltpu.VMEM((SIDE, packet_rows, half), BF16),
            pltpu.VMEM((state_len, half), F32),
            pltpu.VMEM((1, half), F32),
            pltpu.VMEM((state_len, width), F32),
            pltpu.VMEM((state_len, half), F32),
            pltpu.VMEM((3, SIDE, SIDE, 2, wrows, hid), BF16),
            pltpu.VMEM((SIDE, SIDE, SIDE, 2, orow, features), BF16),
            pltpu.VMEM((SIDE, step_rows, SIDE * width), BF16),
            pltpu.VMEM((SIDE, SIDE, sub, features), BF16),
            pltpu.VMEM((SIDE, step_rows, features), BF16),
            pltpu.VMEM((2, step_rows, hid), BF16),
            pltpu.VMEM((SIDE, step_rows, features), BF16),
            pltpu.VMEM((SIDE, sub, features // 2), BF16),
            pltpu.VMEM((SIDE, sub, features // 2), BF16),
            pltpu.VMEM((SIDE, sub, features), BF16),
            pltpu.VMEM((SIDE, sub, features), BF16),
            pltpu.SemaphoreType.DMA((messages,)),
            pltpu.SemaphoreType.DMA((messages,)),
            pltpu.SemaphoreType.DMA((16,)),
        ],
        compiler_params=pltpu.CompilerParams(
            collective_id=0, has_side_effects=True, vmem_limit_bytes=VMEM_LIMIT
        ),
        cost_estimate=pl.CostEstimate(
            flops=40_000_000_000, bytes_accessed=60_000_000, transcendentals=0
        ),
        name="layer",
    )(
        residual.reshape(SIDE, SIDE, sub, features),
        small_heads,
        large_heads,
        key_rows,
        query_rows,
        small_gate,
        large_gate,
        small_step.T,
        large_step.T,
        small_decay,
        large_decay,
        small_taps,
        large_taps,
        key_taps,
        query_taps,
        small_gain,
        large_gain,
        small_out.reshape(out_shape),
        large_out.reshape(out_shape),
        mixer_gain,
        ffn_in_gain,
        ffn_out_gain,
        gate_proj,
        up_proj,
        down_proj,
    )


def solution(mesh):
    placed = (
        P("sp", None),
        P("sp", "tp"),
        P("sp", "tp"),
        P("sp", "tp", None),
        P("sp", "tp", None),
        P("sp", "tp"),
        P("sp", "tp"),
        P("sp", "tp"),
        P("sp", "tp"),
        P(None, "tp"),
        P(None, "tp"),
        P(None, "tp", None),
        P(None, "tp", None),
        P("tp"),
        P("tp"),
        P("tp"),
        P("tp"),
        P("tp", None),
        P("tp", None),
        P(),
        P(),
        P("sp", "tp"),
        P("sp", "tp"),
        P("sp", "tp"),
        P(),
    )
    return jax.shard_map(
        local_program, mesh=mesh, in_specs=placed, out_specs=P(("sp", "tp"), None), check_vma=False
    )
```

```python
import functools

import jax
import jax.numpy as jnp
from jax import lax
from jax.experimental import pallas as pl
from jax.experimental.pallas import tpu as pltpu
from jax.sharding import PartitionSpec as P

BLOCK = 128
HALO = 16
LANES = 128
SLOTS = 8
TAIL = 16
SIDE = 4

EPS = 1e-06
FAR = -1e30
F32 = jnp.float32
BF16 = jnp.bfloat16
MESH = pl.DeviceIdType.MESH
scope = jax.named_scope
VMEM_LIMIT = 66_000_000


def silu(x):
    return x / (1.0 + jnp.exp(-x))


def softplus(x):
    return jnp.maximum(x, 0.0) + jnp.log1p(jnp.exp(-jnp.abs(x)))


def exact_dot(a, b, dims=(((1,), (0,)), ((), ()))):
    return lax.dot_general(a, b, dims, precision=lax.Precision.HIGHEST, preferred_element_type=F32)


def lower(n):
    rows = lax.broadcasted_iota(jnp.int32, (n, n), 0)
    return rows >= lax.broadcasted_iota(jnp.int32, (n, n), 1)


def spread(columns, heads, dim):
    rows = columns.shape[0]
    parts = []
    if dim >= LANES:
        for h in heads:
            parts.append(jnp.broadcast_to(columns[:, h : h + 1], (rows, dim)))
    else:
        per = LANES // dim
        lane = lax.broadcasted_iota(jnp.int32, (rows, LANES), 1)
        for first in range(0, len(heads), per):
            part = jnp.broadcast_to(columns[:, heads[first] : heads[first] + 1], (rows, LANES))
            for j in range(1, per):
                h = heads[first + j]
                part = jnp.where(lane >= j * dim, columns[:, h : h + 1], part)
            parts.append(part)
    return jnp.concatenate(parts, axis=1)


def unit_rms(values):
    return values * lax.rsqrt(jnp.mean(values * values, axis=-1, keepdims=True) + EPS)


def pack(ref, slot, state, log):
    rows = state.shape[0]
    high = log.astype(BF16).astype(F32)
    row = lax.broadcasted_iota(jnp.int32, (TAIL, log.shape[1]), 0)
    both = jnp.where(row == 0, high, jnp.where(row == 1, log - high, 0.0))
    if slot is None:
        ref[:rows] = state.astype(BF16)
        ref[rows:] = both.astype(BF16)
    else:
        ref[slot, :rows] = state.astype(BF16)
        ref[slot, rows:] = both.astype(BF16)


def opened(packet, rows):
    log = packet[rows : rows + TAIL].astype(F32)
    return packet[:rows].astype(F32), log[0:1] + log[1:2]


class Counter:
    def __init__(self):
        self.n = 0

    def take(self, count=1):
        first = self.n
        self.n += count
        return first


def tile_list(width, tile):
    return [(s, min(tile, width - s)) for s in range(0, width, tile)]


def whole_kernel(
    sizes,
    res_in,
    small_in,
    large_in,
    key_in,
    query_in,
    small_gate_in,
    large_gate_in,
    small_step,
    large_step,
    small_decay,
    large_decay,
    small_taps,
    large_taps,
    key_taps,
    query_taps,
    small_gain,
    large_gain,
    small_out,
    large_out,
    mixer_gain,
    in_gain,
    out_gain,
    gate_in,
    up_in,
    down_in,
    out,
    xin,
    kin,
    gates,
    woven,
    conv,
    taps,
    pattern,
    gain,
    dt_rows,
    cum_rows,
    cums,
    logs,
    tails,
    starts,
    inside,
    state,
    total,
    packet,
    from_partner,
    first_state,
    first_log,
    along_y,
    along_z,
    row_state,
    row_log,
    entering,
    for_partner,
    w,
    o,
    heads,
    res,
    ninbuf,
    hidden,
    parts,
    ra,
    rb,
    rc,
    rd,
    send,
    recv,
    local,
):
    (heads_a, dim_a), (heads_b, dim_b), state_len, blocks = sizes
    head_list_a = list(range(heads_a))
    head_list_b = list(range(heads_a, heads_a + heads_b))
    width_a = heads_a * dim_a
    width_b = heads_b * dim_b
    width = width_a + width_b
    groups = (
        (head_list_a, dim_a, width_a, 0),
        (head_list_b, dim_b, width_b, width_a),
    )

    sp = lax.axis_index("sp")
    x = lax.axis_index("tp")
    c = lax.rem(sp, 2)
    y = lax.rem(sp // 2, SIDE)
    z = sp // (2 * SIDE)
    zy = sp // 2
    count_sp = lax.axis_size("sp")

    def turn(v, d):
        return lax.rem(v + d + SIDE, SIDE)

    def at_chip(zz, yy):
        return ((zz * SIDE + yy) * 2 + c, x)

    partner = (sp + 1 - 2 * c, x)
    xs = {d: (sp, turn(x, d)) for d in (1, -1, 2)}
    ys = {d: at_chip(z, turn(y, d)) for d in (1, -1, 2)}
    zs = {d: at_chip(turn(z, d), y) for d in (1, -1, 2)}
    after = (lax.rem(sp + 1, count_sp), x)
    prior = (lax.rem(sp + count_sp - 1, count_sp), x)

    barrier = pltpu.get_barrier_semaphore()
    greeted = [partner, after, prior] + [v[d] for v in (xs, ys, zs) for d in (1, -1, 2)]
    for peer in greeted:
        pl.semaphore_signal(barrier, inc=1, device_id=peer, device_id_type=MESH)

    counter = Counter()
    issued = []

    def message(src, dst, target, index):
        return pltpu.make_async_remote_copy(
            src_ref=src,
            dst_ref=dst,
            send_sem=send.at[index],
            recv_sem=recv.at[index],
            device_id=target,
            device_id_type=MESH,
        )

    def post(src, dst, landing, target):
        index = counter.take()
        copy = message(src, dst, target, index)
        copy.start()
        issued.append(copy)
        return message(landing, landing, target, index)

    def wait_all(arrivals, name="wait"):
        with scope(name):
            for arrival in arrivals:
                arrival.wait_recv()

    def run(name, first, last, body):
        with scope(name):
            lax.fori_loop(first, last, body, 0)

    loads = []

    def load(src, dst):
        copy = pltpu.make_async_copy(src, dst, local.at[len(loads)])
        copy.start()
        loads.append(copy)
        return copy

    length = small_in.shape[0]
    weight_loads = [
        load(ref, w.at[m, z, y, c]) for m, ref in enumerate((gate_in, up_in, down_in))
    ]
    conv_loads = [
        load(ref, xin.at[g, pl.ds(HALO, length)]) for g, ref in enumerate((small_in, large_in))
    ]
    conv_loads += [
        load(ref, kin.at[g, pl.ds(2 * HALO, 2 * length)])
        for g, ref in enumerate((key_in, query_in))
    ]
    out_loads = [
        load(ref, o.at[x, pl.ds(first, SIDE // 2)])
        for ref, first in ((small_out, 0), (large_out, SIDE // 2))
    ]
    kernel_len = small_taps.shape[0]
    taps[:, :width_a] = small_taps[...].astype(F32)
    taps[:, width_a:width] = large_taps[...].astype(F32)
    pair_row = lax.broadcasted_iota(jnp.int32, (SLOTS, LANES), 0)
    for g, ref in enumerate((key_taps, query_taps)):
        for k in range(kernel_len):
            pattern[g, k] = jnp.where(
                pair_row % 2 == 0, ref[k, 0:1].astype(F32), ref[k, 1:2].astype(F32)
            )
    gain[:, :width_a] = small_gain[...].astype(F32).reshape(1, width_a)
    gain[:, width_a:] = large_gain[...].astype(F32).reshape(1, width_b)
    dt_rows[...] = jnp.zeros_like(dt_rows)
    dt_rows[:heads_a] = softplus(small_step[...])
    dt_rows[heads_a : heads_a + heads_b] = softplus(large_step[...])
    head_row = lax.broadcasted_iota(jnp.int32, (SLOTS, BLOCK), 0)
    rate = jnp.zeros((SLOTS, BLOCK), F32)
    for h in range(heads_a + heads_b):
        value = small_decay[h] if h < heads_a else large_decay[h - heads_a]
        rate = jnp.where(head_row == h, value, rate)
    rate = jnp.exp(rate)
    row_id = lax.broadcasted_iota(jnp.int32, (BLOCK, BLOCK), 0)
    col_id = lax.broadcasted_iota(jnp.int32, (BLOCK, BLOCK), 1)
    with scope("decays"):
        pieces = [dt_rows[:, i * BLOCK : (i + 1) * BLOCK] for i in range(blocks)]
        dt_all = jnp.concatenate(pieces, axis=0)
        rate_all = jnp.concatenate([rate] * blocks, axis=0)
        cum_all = exact_dot(-dt_all * rate_all, (row_id <= col_id).astype(F32))
        scale_all = dt_all * jnp.exp(cum_all[:, BLOCK - 1 : BLOCK] - cum_all)
        eye = (row_id == col_id).astype(F32)
        turned = exact_dot(
            eye, jnp.concatenate([cum_all, scale_all], axis=0), (((1,), (1,)), ((), ()))
        )
        before = jnp.zeros((1, SLOTS), F32)
        for i in range(blocks):
            rows = slice(i * BLOCK, (i + 1) * BLOCK)
            heads_at = slice(i * SLOTS, (i + 1) * SLOTS)
            scales_at = slice((blocks + i) * SLOTS, (blocks + i + 1) * SLOTS)
            cum_rows[:, rows] = cum_all[heads_at]
            cums[rows, :SLOTS] = turned[:, heads_at]
            cums[rows, SLOTS:] = turned[:, scales_at]
            tail = turned[BLOCK - 1 : BLOCK, heads_at]
            for buffer, value in ((logs, before), (tails, tail)):
                buffer[i] = jnp.concatenate(
                    [spread(value, head_list_a, dim_a), spread(value, head_list_b, dim_b)], axis=1
                )
            before = before + tail
        final_log = jnp.concatenate(
            [spread(before, head_list_a, dim_a), spread(before, head_list_b, dim_b)], axis=1
        )
        total[...] = final_log
    with scope("barrier"):
        pl.semaphore_wait(barrier, len(greeted))

    halo = []
    for g, ref in enumerate((small_in, large_in)):
        first = xin.at[g, pl.ds(0, HALO)]
        halo.append(post(ref.at[pl.ds(length - HALO, HALO)], first, first, after))
    for g, ref in enumerate((key_in, query_in)):
        first = kin.at[g, pl.ds(0, 2 * HALO)]
        halo.append(post(ref.at[pl.ds(2 * (length - HALO), 2 * HALO)], first, first, after))

    near_cols = w.shape[5] // LANES // 2 * LANES

    def cell(kind, h, first_axis, offset, q=None, m=None, core=c):
        if first_axis:
            zz, yy = (z, turn(y, offset)) if h == 0 else (turn(z, offset), y)
        else:
            zz, yy = (turn(z, offset), slice(None)) if h == 0 else (slice(None), turn(y, offset))
        if kind == "o":
            extent = o.shape[5] // 2 if q is None else o.shape[5] // 4
            part = pl.ds(h * (o.shape[5] // 2) + (0 if q is None else q) * extent, extent)
            return o.at[turn(x, 2), zz, yy, core, slice(None), part]
        extent = w.shape[4] if q is None else w.shape[4] // 2
        rows = pl.ds((0 if q is None else q) * extent, extent)
        cols = pl.ds(0, near_cols) if h == 0 else pl.ds(near_cols, w.shape[5] - near_cols)
        return w.at[slice(None) if m is None else m, zz, yy, core, rows, cols]

    def target_of(h, first_axis, d):
        return (ys if (h == 0) == first_axis else zs)[d]

    def spread_over(kind, first_axis, hs=(0, 1), m=None, q=None):
        arrivals = []
        for h in hs:
            for d in (1, -1):
                src = cell(kind, h, first_axis, 0, q, m)
                landing = cell(kind, h, first_axis, -d, q, m)
                arrivals.append(post(src, src, landing, target_of(h, first_axis, d)))
        return arrivals

    def forward_over(kind, first_axis, m=None, hs=(0, 1)):
        arrivals = []
        for h in hs:
            for d, q in ((1, 0), (-1, 1)):
                src = cell(kind, h, first_axis, -d, q, m)
                landing = cell(kind, h, first_axis, -2 * d, q, m)
                arrivals.append(post(src, src, landing, target_of(h, first_axis, d)))
        return arrivals

    def mirror_over(kind, offsets, m=None):
        arrivals = []
        for h in (0, 1):
            for offset in offsets:
                src = cell(kind, h, False, offset, m=m)
                landing = cell(kind, h, False, offset, m=m, core=1 - c)
                arrivals.append(post(src, src, landing, partner))
        return arrivals

    with scope("loads"):
        for copy in weight_loads + out_loads:
            copy.wait()
    mine_out = o.at[x, z, y, c]
    o_entry = [post(mine_out, mine_out, o.at[turn(x, 2), z, y, c], xs[2])]
    w_first = spread_over("w", True)

    def orows(offset, core):
        return o.at[turn(x, offset), pl.ds(core * (SIDE // 2), SIDE // 2)]

    o_near = [post(orows(0, c), orows(0, c), orows(-d, c), xs[d]) for d in (1, -1)]

    gate_loads = [
        load(ref, gates.at[g]) for g, ref in enumerate((small_gate_in, large_gate_in))
    ]
    res_loads = [load(res_in.at[:, k], res.at[k]) for k in range(SIDE)]
    state[...] = jnp.zeros_like(state)

    with scope("conv_loads"):
        for copy in conv_loads:
            copy.wait()
    def convolve(g, at):
        for first_lane in range(0, xin.shape[2], LANES):
            here = pl.ds(g * xin.shape[2] + first_lane, LANES)
            extended = xin[g, pl.ds(at, BLOCK + HALO), pl.ds(first_lane, LANES)].astype(F32)
            summed = None
            for k in range(kernel_len):
                first = HALO - kernel_len + 1 + k
                term = taps[k : k + 1, here] * extended[first : first + BLOCK]
                summed = term if summed is None else summed + term
            conv[pl.ds(at, BLOCK), here] = silu(summed).astype(BF16)

    def convolve_pair(g, at):
        span = 2 * BLOCK
        rows = pl.ds(pl.multiple_of(2 * at, span), span + 2 * HALO)
        extended = kin[g, rows].astype(F32)
        summed = None
        for k in range(kernel_len):
            first = 2 * (HALO - kernel_len + 1 + k)
            window = extended[first : first + span].reshape(span // SLOTS, SLOTS, LANES)
            term = window * pattern[g, k][None]
            summed = term if summed is None else summed + term
        woven[...] = silu(summed).reshape(span, LANES)
        for j in range(2):
            column = width + (2 * g + j) * state_len
            conv[pl.ds(at, BLOCK), column : column + LANES] = woven[
                pl.ds(j, BLOCK, stride=2), :
            ].astype(BF16)

    def convolve_three(i, carry):
        at = pl.multiple_of(i * BLOCK, BLOCK)
        convolve(0, at)
        convolve(1, at)
        convolve_pair(0, at)
        return carry

    def states(i, carry):
        at = pl.multiple_of(i * BLOCK, BLOCK)
        rows = pl.ds(at, BLOCK)
        scale = cums[rows, SLOTS:]
        kept = jnp.exp(tails[i])
        for which, (head_list, dim, wide, offset) in enumerate(groups):
            key_at = width + which * state_len
            columns = slice(offset, offset + wide)
            heads_here = list(range(len(head_list)))
            shifted = scale[:, head_list[0] : head_list[-1] + 1]
            xv = conv[rows, columns].astype(F32)
            u = (xv * spread(shifted, heads_here, dim)).astype(BF16)
            k = conv[rows, key_at : key_at + state_len]
            fresh = lax.dot_general(k, u, (((0,), (0,)), ((), ())), preferred_element_type=F32)
            old = state[:, columns]
            starts[i, :, columns] = old
            state[:, columns] = old * kept[:, columns] + fresh
        return carry

    run("conv1", 1, blocks, convolve_three)
    wait_all(halo, "halo")
    for g in range(2):
        for buffer, size in ((xin, HALO), (kin, 2 * HALO)):
            edge = buffer[g, :size].astype(F32)
            buffer[g, :size] = jnp.where(sp == 0, 0.0, edge).astype(BF16)
    run("conv0", 0, 1, convolve_three)
    run("states", 0, blocks, states)

    half = width // 2

    def half_of(core):
        return pl.ds(pl.multiple_of(core * half, half), half)

    pack(packet, None, state[...], total[...])
    swapped = post(packet.at[:, half_of(1 - c)], from_partner, from_partner, partner)

    def queries(i, carry):
        convolve_pair(1, pl.multiple_of(i * BLOCK, BLOCK))
        return carry

    def mix_inside(i, carry):
        at = pl.multiple_of(i * BLOCK, BLOCK)
        rows = pl.ds(at, BLOCK)
        causal = row_id >= col_id
        dt_across = dt_rows[:, rows]
        cum = cums[rows]
        cum_across = cum_rows[:, rows]
        lane = lax.broadcasted_iota(jnp.int32, (BLOCK, LANES), 1)
        for which, (head_list, dim, wide, offset) in enumerate(groups):
            key_at = width + which * state_len
            query_at = key_at + 2 * state_len
            k = conv[rows, key_at : key_at + state_len]
            q = conv[rows, query_at : query_at + state_len]
            scores = lax.dot_general(q, k, (((1,), (1,)), ((), ())), preferred_element_type=F32)
            span = max(dim, LANES)
            per = span // dim
            for first in range(0, len(head_list), per):
                columns = slice(offset + first * dim, offset + first * dim + span)
                x_part = conv[rows, columns]
                part = None
                for j in range(per):
                    h = head_list[first + j]
                    gap = cum[:, h : h + 1] - cum_across[h : h + 1]
                    decays = jnp.exp(jnp.where(causal, gap, FAR))
                    weight = (scores * decays * dt_across[h : h + 1]).astype(BF16)
                    got = jnp.dot(weight, x_part, preferred_element_type=F32)
                    part = got if part is None else jnp.where(lane >= j * dim, got, part)
                inside[rows, columns] = part
        return carry

    def send_along(buffer, targets):
        arrivals = []
        for d, slot in ((1, 1), (-1, 3), (2, 2)):
            landing = buffer.at[slot]
            arrivals.append(post(buffer.at[0], landing, landing, targets[d]))
        return arrivals

    def fold(buffer, place, number):
        zero = jnp.zeros((state_len, half), F32)
        every, every_log = zero, jnp.zeros((1, half), F32)
        ahead, ahead_log = every, every_log
        for p in range(number):
            slot = turn(place, -p)
            one, log = opened(buffer[slot], state_len)
            counts = p < place
            ahead = jnp.where(counts, ahead * jnp.exp(log) + one, ahead)
            ahead_log = jnp.where(counts, ahead_log + log, ahead_log)
            every = every * jnp.exp(log) + one
            every_log = every_log + log
        return every, every_log, ahead, ahead_log

    wait_all(w_first[2:], "w_first_z")
    w_second_z = forward_over("w", True, hs=(1,))
    wait_all(o_entry, "o_entry")
    o_first_z = spread_over("o", True, (1,))
    run("queries", 0, blocks, queries)
    wait_all([swapped], "swap_wait")
    mine, mine_log = opened(packet[:, half_of(c)], state_len)
    theirs, theirs_log = opened(from_partner[...], state_len)
    even = c == 0
    a_state = jnp.where(even, mine, theirs)
    a_log = jnp.where(even, mine_log, theirs_log)
    b_state = jnp.where(even, theirs, mine)
    b_log = jnp.where(even, theirs_log, mine_log)
    first_state[...] = a_state
    first_log[...] = a_log
    pack(along_y, 0, a_state * jnp.exp(b_log) + b_state, a_log + b_log)
    y_arrivals = send_along(along_y, ys)
    wait_all(w_first[:2], "w_first_y")
    w_second_y = forward_over("w", True, hs=(0,))
    o_first_y = spread_over("o", True, (0,))
    run("mix0", 0, 4, mix_inside)
    wait_all(o_first_z, "o_first_z")
    o_second_z = forward_over("o", True, hs=(1,))
    wait_all(y_arrivals, "y_wait")
    row_all, row_all_log, row_ahead, row_ahead_log = fold(along_y, y, SIDE)
    row_state[...] = row_ahead
    row_log[...] = row_ahead_log
    pack(along_z, 0, row_all, row_all_log)
    z_arrivals = send_along(along_z, zs)
    wait_all(o_second_z, "o_second_z")
    o_third = spread_over("o", False, (1,))
    run("mix4", 4, 6, mix_inside)
    wait_all(o_first_y, "o_first_y")
    o_second_y = forward_over("o", True, hs=(0,))
    wait_all(w_second_z, "w_second_z")
    w_third = {0: spread_over("w", False, (1,), 0)}
    wait_all(w_second_y, "w_second_y")
    w_third[0] += spread_over("w", False, (0,), 0)
    run("mix6", 6, blocks, mix_inside)
    wait_all(z_arrivals, "z_wait")
    _, _, plane_ahead, _ = fold(along_z, z, SIDE - 1)
    chip = plane_ahead * jnp.exp(row_log[...]) + row_state[...]
    second = chip * jnp.exp(first_log[...]) + first_state[...]
    entering[:, half_of(c)] = jnp.where(even, chip, second)
    for_partner[...] = jnp.where(even, second, chip)
    entered = post(
        for_partner, entering.at[:, half_of(c)], entering.at[:, half_of(1 - c)], partner
    )
    wait_all(o_second_y, "o_second_y")
    o_third += spread_over("o", False, (0,))
    w_third[1] = spread_over("w", False, (1,), 1)
    w_mirrored = {m: mirror_over("w", (0,), m) for m in range(3)}
    o_mirrored = mirror_over("o", (0,))

    sub = length // (SIDE * SIDE)
    lane = lax.broadcasted_iota(jnp.int32, (BLOCK, LANES), 1)

    def carry_block(n, carry):
        stage = n // SIDE
        d = lax.rem(n, SIDE)
        i = 2 * d + stage
        rows = pl.ds(pl.multiple_of(i * BLOCK, BLOCK), BLOCK)
        grown = jnp.exp(cums[rows])
        for which, (head_list, dim, wide, offset) in enumerate(groups):
            columns = slice(offset, offset + wide)
            query_at = width + (2 + which) * state_len
            q = conv[rows, query_at : query_at + state_len]
            old = starts[i, :, columns] + entering[:, columns] * jnp.exp(logs[i, :, columns])
            carried = jnp.dot(q, old.astype(BF16), preferred_element_type=F32)
            mixed = inside[rows, columns] + carried * spread(grown, head_list, dim)
            gated = mixed * silu(gates[which, rows].astype(F32))
            squares = gated * gated
            span = max(dim, LANES)
            per = span // dim
            normed = []
            for first in range(0, len(head_list), per):
                at = first * dim
                part = squares[:, at : at + span]
                means = None
                for j in range(per):
                    if per == 1:
                        means = jnp.sum(part, axis=1, keepdims=True)
                    else:
                        ours = (lane >= j * dim) & (lane < (j + 1) * dim)
                        one = jnp.sum(jnp.where(ours, part, 0.0), axis=1, keepdims=True)
                        means = one if means is None else jnp.where(lane >= j * dim, one, means)
                normed.append(gated[:, at : at + span] * lax.rsqrt(means * (1.0 / dim) + EPS))
            normed = (jnp.concatenate(normed, axis=1) * gain[:, columns]).astype(BF16)
            place = pl.ds(pl.multiple_of(x * width + offset, LANES), wide)
            spot = pl.ds(pl.multiple_of(d * sub, sub), sub)
            heads[2 * stage, spot, place] = normed[:sub]
            heads[2 * stage + 1, spot, place] = normed[sub:]
        return carry

    def hcols(offset):
        return pl.ds(pl.multiple_of(turn(x, offset) * width, LANES), width)

    step_rows = heads.shape[1]
    g1 = {d: counter.take(SIDE) for d in (1, -1)}
    g2 = {d: counter.take(SIDE) for d in (1, -1)}

    def heads_out(k, d):
        src = heads.at[k, :, hcols(0)]
        return message(src, src, xs[d], g1[d] + k)

    def heads_in(k, d):
        landing = heads.at[k, :, hcols(-d)]
        return message(landing, landing, xs[d], g1[d] + k)

    def far_rows(d):
        return pl.ds(0 if d == 1 else step_rows // 2, step_rows // 2)

    def heads_on(k, d):
        src = heads.at[k, far_rows(d), hcols(-d)]
        return message(src, src, xs[d], g2[d] + k)

    def heads_far(k, d):
        landing = heads.at[k, far_rows(d), hcols(-2 * d)]
        return message(landing, landing, xs[d], g2[d] + k)

    def start_heads(k):
        for d in (1, -1):
            heads_out(k, d).start()

    def forward_heads(k):
        with scope("heads_in"):
            for d in (1, -1):
                heads_in(k, d).wait_recv()
        for d in (1, -1):
            heads_on(k, d).start()

    features = res.shape[3]
    hid = hidden.shape[2]
    side_half = features // 2
    r1 = {d: counter.take(SIDE) for d in (1, -1)}
    r2 = {d: counter.take(SIDE) for d in (1, -1)}

    def prow(offset):
        return pl.ds(pl.multiple_of(turn(x, offset) * sub, sub), sub)

    def project(k):
        with scope("heads_far"):
            for d in (1, -1):
                heads_far(k, d).wait_recv()
        with scope("out_dot"):
            left = heads[k]
            for n, (first, size) in enumerate(tile_list(features, width)):
                inside[n * step_rows : (n + 1) * step_rows] = jnp.dot(
                    left,
                    o[..., first : first + size].reshape(SIDE * width, size),
                    preferred_element_type=F32,
                )
        with scope("norms"):
            outer = mixer_gain[...].astype(F32).reshape(1, features)
            inner = in_gain[...].astype(F32).reshape(1, features)
            for d in range(SIDE):
                tiles = [
                    slice(n * step_rows + d * sub, n * step_rows + (d + 1) * sub)
                    for n in range(SIDE)
                ]
                mix = jnp.concatenate([inside[t] for t in tiles], axis=1)
                mixed = res[k, d].astype(F32) + unit_rms(mix) * outer
                for n, t in enumerate(tiles):
                    inside[t] = mixed[:, n * width : (n + 1) * width]
                ninbuf[k, d * sub : (d + 1) * sub] = (unit_rms(mixed) * inner).astype(BF16)
            for j in range(SIDE):
                spot = slice((j % 2) * sub, (j % 2 + 1) * sub)
                own = pl.ds(pl.multiple_of(j * step_rows + x * sub, sub), sub)
                starts[2 * k + j // 2, spot] = inside[own]

    w_fourth = {}

    def pass_weights(m):
        wait_all(w_third[m], "w_third")
        w_fourth[m] = forward_over("w", False, m)
        w_mirrored[m] += mirror_over("w", (1, -1), m)

    def settle_weights(m):
        wait_all(w_fourth[m], "w_fourth")
        w_mirrored[m] += mirror_over("w", (2,), m)

    wait_all([entered], "enter_wait")
    for copy in gate_loads:
        copy.wait()
    run("carry1", 0, SIDE, carry_block)
    start_heads(0)
    start_heads(1)
    run("carry2", SIDE, 2 * SIDE, carry_block)
    wait_all(o_near, "o_near")
    for d in (1, -1):
        o_mirrored.append(post(orows(d, c), orows(d, c), orows(d, 1 - c), partner))
    wait_all(o_third, "o_third")
    o_fourth = forward_over("o", False)
    o_mirrored += mirror_over("o", (1, -1))
    w_third[1] += spread_over("w", False, (0,), 1)
    pass_weights(0)
    w_third[2] = spread_over("w", False, (1, 0), 2)
    forward_heads(0)
    start_heads(2)
    wait_all(o_fourth, "o_fourth")
    o_mirrored += mirror_over("o", (2,))
    forward_heads(1)
    start_heads(3)
    for copy in res_loads:
        copy.wait()
    wait_all(o_mirrored, "o_mirrored")
    def gate_only(k):
        with scope("gate"):
            nin = ninbuf[k]
            for first, size in tile_list(hid, 512):
                wg = w[0, :, :, :, :, first : first + size].reshape(features, size)
                gate = jnp.dot(nin, wg, preferred_element_type=F32)
                hidden[k % 2, :, first : first + size] = silu(gate).astype(BF16)

    def up_only(k):
        with scope("up"):
            nin = ninbuf[k]
            for first, size in tile_list(hid, 512):
                wu = w[1, :, :, :, :, first : first + size].reshape(features, size)
                up = jnp.dot(nin, wu, preferred_element_type=F32)
                gated = hidden[k % 2, :, first : first + size].astype(F32)
                hidden[k % 2, :, first : first + size] = (gated * up).astype(BF16)

    project(0)
    pass_weights(1)
    settle_weights(0)
    forward_heads(2)
    wait_all(w_mirrored[0], "w_mirrored0")
    gate_only(0)
    project(1)
    pass_weights(2)
    settle_weights(1)
    gate_only(1)
    forward_heads(3)
    wait_all(w_mirrored[1], "w_mirrored1")

    def far_out(k, d):
        lanes = pl.ds(0 if d == 1 else side_half, side_half)
        landing = (ra if d == 1 else rb).at[k]
        return message(parts.at[k, prow(2), lanes], landing, xs[d], r1[d] + k)

    def near_out(k, d):
        landing = (rc if d == 1 else rd).at[k]
        return message(parts.at[k, prow(d)], landing, xs[d], r2[d] + k)

    def pass_on(k):
        for d in (1, -1):
            with scope("far_wait"):
                far_out(k, d).wait_recv()
            lanes = slice(0, side_half) if d == 1 else slice(side_half, features)
            extra = (ra if d == 1 else rb)[k].astype(F32)
            mine = parts[k, prow(d), lanes].astype(F32)
            parts[k, prow(d), lanes] = (mine + extra).astype(BF16)
            near_out(k, d).start()

    def gate_up(k):
        with scope("gate_up"):
            nin = ninbuf[k]
            for first, size in tile_list(hid, 512):
                wg = w[0, :, :, :, :, first : first + size].reshape(features, size)
                wu = w[1, :, :, :, :, first : first + size].reshape(features, size)
                gate = jnp.dot(nin, wg, preferred_element_type=F32)
                up = jnp.dot(nin, wu, preferred_element_type=F32)
                hidden[lax.rem(k, 2), :, first : first + size] = (silu(gate) * up).astype(BF16)

    def down(k):
        with scope("down"):
            hv = hidden[lax.rem(k, 2)]
            tile = features // SIDE
            for n in range(SIDE):
                wd = w[2, n].reshape(tile, hid)
                got = lax.dot_general(hv, wd, (((1,), (1,)), ((), ())), preferred_element_type=F32)
                parts[k, :, n * tile : (n + 1) * tile] = got.astype(BF16)
            for d in (1, -1):
                far_out(k, d).start()

    def down_pair(k, carry):
        down(k)
        return carry

    def channel_mix(k, carry):
        project(k)

        @pl.when(k == 2)
        def _():
            pass_on(0)

        gate_up(k)

        @pl.when(k == 2)
        def _():
            pass_on(1)

        down(k)
        return carry

    up_only(0)
    settle_weights(2)
    up_only(1)
    wait_all(w_mirrored[2], "w_mirrored2")
    lax.fori_loop(0, 2, down_pair, 0)
    lax.fori_loop(2, SIDE, channel_mix, 0)
    outer = 0.5 * out_gain[...].astype(F32).reshape(1, features)

    def finish(k):
        with scope("near_wait"):
            for d in (1, -1):
                near_out(k, d).wait_recv()
        ffn = parts[k, prow(0)].astype(F32) + rc[k].astype(F32) + rd[k].astype(F32)
        kept = [
            starts[2 * k + j // 2, (j % 2) * sub : (j % 2 + 1) * sub] for j in range(SIDE)
        ]
        updated = jnp.concatenate(kept, axis=1) + unit_rms(ffn) * outer
        out[k * sub : (k + 1) * sub] = updated.astype(BF16)

    pass_on(SIDE - 2)
    finish(0)
    finish(1)
    pass_on(SIDE - 1)
    finish(2)
    finish(SIDE - 1)

    with scope("drain"):
        for copy in issued:
            copy.wait_send()

    def drain(k, carry):
        for d in (1, -1):
            heads_out(k, d).wait_send()
            heads_on(k, d).wait_send()
            far_out(k, d).wait_send()
            near_out(k, d).wait_send()
        return carry

    lax.fori_loop(0, SIDE, drain, 0)


def local_program(
    residual,
    small_heads,
    large_heads,
    state_keys,
    state_queries,
    small_gate,
    large_gate,
    small_step,
    large_step,
    small_taps,
    large_taps,
    key_taps,
    query_taps,
    small_decay,
    large_decay,
    small_gain,
    large_gain,
    small_out,
    large_out,
    mixer_gain,
    ffn_in_gain,
    gate_proj,
    up_proj,
    down_proj,
    ffn_out_gain,
):
    length, features = residual.shape
    state_len = state_keys.shape[-1]
    key_rows = state_keys.reshape(-1, state_len)
    query_rows = state_queries.reshape(-1, state_len)
    heads_a = small_step.shape[1]
    heads_b = large_step.shape[1]
    heads = heads_a + heads_b
    width_a = small_heads.shape[1]
    width_b = large_heads.shape[1]
    width = width_a + width_b
    everything = width + 2 * state_len * state_keys.shape[1]
    blocks = length // BLOCK
    sizes = ((heads_a, width_a // heads_a), (heads_b, width_b // heads_b), state_len, blocks)
    kernel_len = small_taps.shape[0]
    sub = length // (SIDE * SIDE)
    step_rows = SIDE * sub
    wrows, hid = gate_proj.shape
    orow = width // (2 * SIDE * SIDE)
    out_shape = (SIDE // 2, SIDE, 2, orow, features)
    half = width // 2
    packet_rows = state_len + TAIL
    any_space = pl.BlockSpec(memory_space=pl.ANY)
    vmem = pl.BlockSpec(memory_space=pltpu.VMEM)
    smem = pl.BlockSpec(memory_space=pltpu.SMEM)
    messages = 160

    return pl.pallas_call(
        functools.partial(whole_kernel, sizes),
        in_specs=[any_space] * 7
        + [vmem] * 2
        + [smem] * 2
        + [vmem] * 6
        + [any_space] * 2
        + [vmem] * 3
        + [any_space] * 3,
        out_specs=vmem,
        out_shape=jax.ShapeDtypeStruct((length // SIDE, features), BF16),
        scratch_shapes=[
            pltpu.VMEM((2, HALO + length, width_a), BF16),
            pltpu.VMEM((2, 2 * (HALO + length), state_len), BF16),
            pltpu.VMEM((2, length, width_a), BF16),
            pltpu.VMEM((2 * BLOCK, state_len), F32),
            pltpu.VMEM((length, everything), BF16),
            pltpu.VMEM((kernel_len, width), F32),
            pltpu.VMEM((2, kernel_len, SLOTS, state_len), F32),
            pltpu.VMEM((1, width), F32),
            pltpu.VMEM((SLOTS, length), F32),
            pltpu.VMEM((SLOTS, length), F32),
            pltpu.VMEM((length, 2 * SLOTS), F32),
            pltpu.VMEM((blocks, 1, width), F32),
            pltpu.VMEM((blocks, 1, width), F32),
            pltpu.VMEM((blocks, state_len, width), F32),
            pltpu.VMEM((length, width), F32),
            pltpu.VMEM((state_len, width), F32),
            pltpu.VMEM((1, width), F32),
            pltpu.VMEM((packet_rows, width), BF16),
            pltpu.VMEM((packet_rows, half), BF16),
            pltpu.VMEM((state_len, half), F32),
            pltpu.VMEM((1, half), F32),
            pltpu.VMEM((SIDE, packet_rows, half), BF16),
            pltpu.VMEM((SIDE, packet_rows, half), BF16),
            pltpu.VMEM((state_len, half), F32),
            pltpu.VMEM((1, half), F32),
            pltpu.VMEM((state_len, width), F32),
            pltpu.VMEM((state_len, half), F32),
            pltpu.VMEM((3, SIDE, SIDE, 2, wrows, hid), BF16),
            pltpu.VMEM((SIDE, SIDE, SIDE, 2, orow, features), BF16),
            pltpu.VMEM((SIDE, step_rows, SIDE * width), BF16),
            pltpu.VMEM((SIDE, SIDE, sub, features), BF16),
            pltpu.VMEM((SIDE, step_rows, features), BF16),
            pltpu.VMEM((2, step_rows, hid), BF16),
            pltpu.VMEM((SIDE, step_rows, features), BF16),
            pltpu.VMEM((SIDE, sub, features // 2), BF16),
            pltpu.VMEM((SIDE, sub, features // 2), BF16),
            pltpu.VMEM((SIDE, sub, features), BF16),
            pltpu.VMEM((SIDE, sub, features), BF16),
            pltpu.SemaphoreType.DMA((messages,)),
            pltpu.SemaphoreType.DMA((messages,)),
            pltpu.SemaphoreType.DMA((16,)),
        ],
        compiler_params=pltpu.CompilerParams(
            collective_id=0, has_side_effects=True, vmem_limit_bytes=VMEM_LIMIT
        ),
        cost_estimate=pl.CostEstimate(
            flops=40_000_000_000, bytes_accessed=60_000_000, transcendentals=0
        ),
        name="layer",
    )(
        residual.reshape(SIDE, SIDE, sub, features),
        small_heads,
        large_heads,
        key_rows,
        query_rows,
        small_gate,
        large_gate,
        small_step.T,
        large_step.T,
        small_decay,
        large_decay,
        small_taps,
        large_taps,
        key_taps,
        query_taps,
        small_gain,
        large_gain,
        small_out.reshape(out_shape),
        large_out.reshape(out_shape),
        mixer_gain,
        ffn_in_gain,
        ffn_out_gain,
        gate_proj,
        up_proj,
        down_proj,
    )


def solution(mesh):
    placed = (
        P("sp", None),
        P("sp", "tp"),
        P("sp", "tp"),
        P("sp", "tp", None),
        P("sp", "tp", None),
        P("sp", "tp"),
        P("sp", "tp"),
        P("sp", "tp"),
        P("sp", "tp"),
        P(None, "tp"),
        P(None, "tp"),
        P(None, "tp", None),
        P(None, "tp", None),
        P("tp"),
        P("tp"),
        P("tp"),
        P("tp"),
        P("tp", None),
        P("tp", None),
        P(),
        P(),
        P("sp", "tp"),
        P("sp", "tp"),
        P("sp", "tp"),
        P(),
    )
    return jax.shard_map(
        local_program, mesh=mesh, in_specs=placed, out_specs=P(("sp", "tp"), None), check_vma=False
    )
```
